256 devices in a mesh: sp: 64 (over z, y, core), tp: 4 (over x).
Axes of the slice: x: 4, y: 4, z: 8, core: 2. Of those that a mesh axis runs over, the one named last changes fastest.
Arguments:
- layer_grad: bfloat16 [12288, 2048], P('sp'), may hold values from -16 to 16
- routes: int32 [12288, 2], P('sp'), may hold values from 0 to 63, as said below
- route_weight: float32 [12288, 2], P('sp'), may hold values from 0.1 to 0.9
- slot_tokens: bfloat16 [64, 576, 2048], P('sp'), may hold values from -6 to 6
- gate_proj: bfloat16 [64, 2048, 1024], P('sp', None, 'tp'), may hold values from -0.125 to 0.125
- up_proj: bfloat16 [64, 2048, 1024], P('sp', None, 'tp'), may hold values from -0.125 to 0.125
- down_proj: bfloat16 [64, 1024, 2048], P('sp', 'tp'), may hold values from -0.1875 to 0.1875
- out_proj: bfloat16 [2048, 1024], P(None, 'tp'), may hold values from -0.1875 to 0.1875
- queries: bfloat16 [12288, 512], P('sp', 'tp'), may hold values from -6 to 6
- keys: bfloat16 [12288, 512], P('sp', 'tp'), may hold values from -6 to 6
- values: bfloat16 [12288, 1024], P('sp', 'tp'), may hold values from -6 to 6
- fwd_decay: float32 [12288, 512], P('sp', 'tp'), may hold values from -2 to 0
- bwd_decay: float32 [12288, 512], P('sp', 'tp'), may hold values from -2 to 0
Outputs:
- gate_grad: bfloat16 [64, 2048, 1024], P('sp', None, 'tp')
- up_grad: bfloat16 [64, 2048, 1024], P('sp', None, 'tp')
- down_grad: bfloat16 [64, 1024, 2048], P('sp', 'tp')
- proj_grad: float32 [2048, 1024], P('sp', 'tp')
- query_grad: bfloat16 [12288, 512], P('sp', 'tp')
- key_grad: bfloat16 [12288, 512], P('sp', 'tp')
- value_grad: bfloat16 [12288, 1024], P('sp', 'tp')
The draws below stay inside these ranges and needn't reach their ends.
Inputs may be any that keep to these rules, and one draw needn't show every extreme that they name: `routes`: each row names two different experts of one group of 8 consecutive experts. In every aligned block of 192 rows one expert is named by 9 rows or more.
All inputs are finite; a program needn't handle non-finite values.
Results may differ from the reference program's by a relative error of at most 0.015.
Values may be sent and summed in bfloat16 or wider, within the bound.
A program may use at most 128 MiB of HBM per device.

```python
import functools
import jax
import jax.numpy as jnp
from jax import lax

D = 2048
ATTENTION_HEADS = 8
KEY_CHANNELS = 64
DV = 128
FF = 1024
EXP_GROUP = 8
BLOCK = 64
TOK_DEV = 192
EXPERTS = 64
CAP = 9
SLOTS = 576
SEQUENCE_TOKENS = 12288
N_SP = 64
N_TP = 4


def draw_routes(key, part):
    random_subkeys = jax.random.split(jax.random.fold_in(key, 11), 6)
    blocks = SEQUENCE_TOKENS // TOK_DEV
    group_count = EXPERTS // EXP_GROUP
    chosen_group = jax.random.randint(random_subkeys[0], (SEQUENCE_TOKENS,), 0, group_count)
    primary = jax.random.randint(random_subkeys[1], (SEQUENCE_TOKENS,), 0, EXP_GROUP)
    offsets = jax.random.randint(random_subkeys[2], (SEQUENCE_TOKENS,), 1, EXP_GROUP)
    hottest = jax.random.randint(random_subkeys[3], (), 0, EXPERTS)
    orders = jax.vmap(jax.random.permutation, in_axes=(0, None))(jax.random.split(random_subkeys[4], blocks), TOK_DEV)
    forced = (orders < CAP).reshape(SEQUENCE_TOKENS)
    chosen_group = jnp.where(forced, hottest // EXP_GROUP, chosen_group)
    primary = jnp.where(forced, hottest % EXP_GROUP, primary)
    secondary = (primary + offsets) % EXP_GROUP
    flipped = jax.random.randint(random_subkeys[5], (SEQUENCE_TOKENS,), 0, 2)
    first_id = chosen_group * EXP_GROUP + primary
    second_id = chosen_group * EXP_GROUP + secondary
    leading = jnp.where(flipped == 1, second_id, first_id)
    trailing = jnp.where(flipped == 1, first_id, second_id)
    return jnp.stack([leading, trailing], axis=1).astype(jnp.int32)


def decay_law(key, salt):
    random_subkeys = jax.random.split(jax.random.fold_in(key, salt), 12)
    blocks = SEQUENCE_TOKENS // TOK_DEV
    head_chance = 0.5
    block_chance = 0.5
    heads_index = jnp.arange(ATTENTION_HEADS)
    forced_head = jax.random.randint(random_subkeys[0], (), 0, ATTENTION_HEADS)
    steady_head = (forced_head + jax.random.randint(random_subkeys[1], (), 1, ATTENTION_HEADS)) % ATTENTION_HEADS
    mixed_head = jax.random.uniform(random_subkeys[2], (ATTENTION_HEADS,)) < head_chance
    mixed_head = jnp.logical_and(jnp.logical_or(mixed_head, heads_index == forced_head), heads_index != steady_head)
    fast_block = jax.random.uniform(random_subkeys[3], (blocks, ATTENTION_HEADS)) < block_chance
    turning = jax.random.randint(random_subkeys[4], (), 1, blocks)
    block_index = jnp.arange(blocks)[:, None]
    at_forced = (heads_index == forced_head)[None, :]
    fast_block = jnp.where(jnp.logical_and(block_index == turning, at_forced), True, fast_block)
    fast_block = jnp.where(jnp.logical_and(block_index == turning - 1, at_forced), False, fast_block)
    speedy = jnp.logical_and(fast_block, mixed_head[None, :])
    quick_rate = jax.random.uniform(random_subkeys[5], (ATTENTION_HEADS, KEY_CHANNELS), minval=0.02, maxval=0.035)
    slow_rate = jnp.exp(jax.random.uniform(random_subkeys[6], (ATTENTION_HEADS, KEY_CHANNELS), minval=-1.6, maxval=0.0)) / SEQUENCE_TOKENS
    rate_table = jnp.where(speedy[:, None, :, None], quick_rate[None, None], slow_rate[None, None])
    device_factor = jnp.exp(jax.random.uniform(random_subkeys[7], (blocks, 1, 1, 1), minval=-0.69, maxval=0.69))
    jitter = jax.random.uniform(random_subkeys[8], (blocks, TOK_DEV, ATTENTION_HEADS, KEY_CHANNELS), minval=0.4, maxval=1.6)
    steady_decay = -(rate_table * device_factor * jitter).reshape(SEQUENCE_TOKENS, ATTENTION_HEADS, KEY_CHANNELS)
    start_spike = jax.random.randint(random_subkeys[9], (ATTENTION_HEADS, 1), 0, blocks) * TOK_DEV
    free_spike = jax.random.randint(random_subkeys[10], (ATTENTION_HEADS, 1), 0, SEQUENCE_TOKENS)
    spike_position = jnp.concatenate([start_spike, free_spike], axis=1)
    spike_length = jax.random.uniform(random_subkeys[11], (ATTENTION_HEADS, 2), minval=0.22, maxval=0.5)
    spike_hits = (jnp.arange(SEQUENCE_TOKENS)[:, None, None] == spike_position[None]).astype(jnp.float32)
    spike_events = -jnp.sum(spike_hits * spike_length[None], axis=2)
    return (steady_decay + spike_events[:, :, None]).reshape(SEQUENCE_TOKENS, ATTENTION_HEADS * KEY_CHANNELS).astype(jnp.float32)


def draw_fwd_decay(key, part):
    return decay_law(key, 23)


def draw_bwd_decay(key, part):
    return decay_law(key, 37)


def strengthened(values, rng, source, target, blocks, factor):
    def block_of(dim):
        return (jnp.arange(values.shape[dim]) // (values.shape[dim] // blocks)).reshape((-1,) + (1,) * (values.ndim - 1 - dim))

    near = jax.random.permutation(rng, blocks)[block_of(target)]
    second = (block_of(target) + blocks // 2) % blocks
    return jnp.where((block_of(source) == near) | (block_of(source) == second), factor * values, values)


def shard_levels(rng, extent, cuts, least, largest):
    def one(axis_at, parts):
        heights = jax.random.uniform(jax.random.fold_in(jax.random.fold_in(rng, 6), axis_at), (parts,), jnp.float32, least / len(cuts), largest / len(cuts))
        return jnp.repeat(jnp.exp(heights), extent[axis_at] // parts).reshape((-1,) + (1,) * (len(extent) - axis_at - 1))

    gain = one(*cuts[0])
    for cut in cuts[1:]:
        gain = gain * one(*cut)
    return gain


def gaussian(stream_key, extent, deviation, limit, cuts=(), kind=jnp.bfloat16):
    result = jax.random.normal(stream_key, extent, jnp.float32) * deviation
    if len(cuts) > 0:
        result = shard_levels(stream_key, extent, cuts, -0.22, 0.18) * result
    return jnp.clip(result, min=-limit, max=limit).astype(kind)


def gaussian_with(own_key, shape, width, bound, cuts, heavy, kind=jnp.bfloat16):
    values = width * jax.random.normal(own_key, shape, jnp.float32)
    if cuts:
        values = values * shard_levels(own_key, shape, cuts, -0.22, 0.18)
    return jnp.clip(strengthened(values, jax.random.fold_in(own_key, 3), *heavy), -bound, bound).astype(kind)


def setup_inputs(seed: int = 0) -> dict:
    key_list = jax.random.split(jax.random.key(seed), 14)
    layer_grad = gaussian_with(key_list[0], (SEQUENCE_TOKENS, D), 1.0, 16.0, ((0, 64),), (0, 1, 64, 4.0))
    routes = draw_routes(jax.random.fold_in(key_list[13], 71), 0)
    route_weight = jnp.clip(0.1 + 0.79999997 * jax.random.uniform(key_list[2], (SEQUENCE_TOKENS, 2), jnp.float32) ** shard_levels(key_list[2], (SEQUENCE_TOKENS, 2), ((0, 64),), -0.2, 0.2), 0.1, 0.9)
    slot_tokens = gaussian(key_list[3], (EXPERTS, SLOTS, D), 1.0, 6.0, ((0, 64),))
    gate_proj = gaussian(key_list[4], (EXPERTS, D, FF), D ** -0.5, 0.125, ((0, 64), (2, 4)))
    up_proj = gaussian(key_list[5], (EXPERTS, D, FF), D ** -0.5, 0.125, ((0, 64), (2, 4)))
    down_proj = gaussian(key_list[6], (EXPERTS, FF, D), FF ** -0.5, 0.1875, ((0, 64), (1, 4)))
    out_proj = gaussian(key_list[7], (D, ATTENTION_HEADS * DV), (ATTENTION_HEADS * DV) ** -0.5, 0.1875, ((1, 4),))
    queries = gaussian(key_list[8], (SEQUENCE_TOKENS, ATTENTION_HEADS * KEY_CHANNELS), 1.0, 6.0, ((0, 64), (1, 4)))
    keys = gaussian(key_list[9], (SEQUENCE_TOKENS, ATTENTION_HEADS * KEY_CHANNELS), 1.0, 6.0, ((0, 64), (1, 4)))
    values = gaussian(key_list[10], (SEQUENCE_TOKENS, ATTENTION_HEADS * DV), 1.0, 6.0, ((0, 64), (1, 4)))
    fwd_decay = draw_fwd_decay(jax.random.fold_in(key_list[13], 71), 0)
    bwd_decay = draw_bwd_decay(jax.random.fold_in(key_list[13], 71), 0)
    return {"layer_grad": layer_grad, "routes": routes, "route_weight": route_weight, "slot_tokens": slot_tokens, "gate_proj": gate_proj, "up_proj": up_proj, "down_proj": down_proj, "out_proj": out_proj, "queries": queries, "keys": keys, "values": values, "fwd_decay": fwd_decay, "bwd_decay": bwd_decay}


EPSILON = 1e-06

def sweep(query_rows, keyrows, valrows, log_decay, strict):
    nheads, length, kwidth = query_rows.shape
    vwidth = valrows.shape[-1]
    number = length // BLOCK
    offset = -1 if strict else 0
    causal = jnp.tril(jnp.ones((BLOCK, BLOCK), jnp.float32), offset)

    def split(array):
        return jnp.moveaxis(array.reshape(nheads, number, BLOCK, array.shape[-1]), 1, 0)

    def advance(carried_state, pieces):
        query_block, key_block, value_block, gblock = pieces
        running_total = jnp.cumsum(gblock, axis=1)
        middle = running_total[:, BLOCK // 2 - 1:BLOCK // 2, :]
        scores = jnp.einsum('hik,hjk->hij', query_block * jnp.exp(running_total - middle), key_block * jnp.exp(middle - running_total), precision=lax.Precision.HIGHEST) * causal
        inner = jnp.einsum('hij,hjv->hiv', scores, value_block, precision=lax.Precision.HIGHEST)
        outer_product = jnp.einsum('zuw,zwo->zuo', query_block * jnp.exp(running_total), carried_state, precision=lax.Precision.HIGHEST)
        final_row = running_total[:, -1:, :]
        fresh_state = jnp.einsum('xor,xot->xrt', key_block * jnp.exp(final_row - running_total), value_block, precision=lax.Precision.HIGHEST)
        return (jnp.exp(final_row[:, 0, :])[:, :, None] * carried_state + fresh_state, inner + outer_product)
    start_state = jnp.zeros((nheads, kwidth, vwidth), jnp.float32)
    final, outputs = lax.scan(advance, start_state, (split(query_rows), split(keyrows), split(valrows), split(log_decay)))
    return (jnp.moveaxis(outputs, 0, 1).reshape(nheads, length, vwidth), final)

def slot_ranks(expert_ids, experts):
    members = (expert_ids[:, None] == jnp.arange(experts, dtype=jnp.int32)[None, :]).astype(jnp.int32)
    before = jnp.cumsum(members, axis=0) - members
    return lax.optimization_barrier(jnp.sum(before * members, axis=1))

def mixer_forward(query_rows, keyrows, valrows, fwd_log, bwd_log):
    forward_out, forward_end = sweep(query_rows, keyrows, valrows, fwd_log, False)
    backward_out, backward_end = sweep(jnp.flip(query_rows, 1), jnp.flip(keyrows, 1), jnp.flip(valrows, 1), jnp.flip(bwd_log, 1), True)
    mixed = forward_out + jnp.flip(backward_out, 1)
    return mixed * lax.rsqrt(lax.optimization_barrier(jnp.mean(mixed * mixed, axis=-1, keepdims=True)) + EPSILON)

def expert_back(pieces):
    inputs, inbound, w_gate, w_up, w_down = pieces
    gate = jnp.dot(inputs, w_gate, preferred_element_type=jnp.float32)
    upper = jnp.dot(inputs, w_up, preferred_element_type=jnp.float32)
    sigma = jax.nn.sigmoid(gate)
    act = (gate * sigma * upper).astype(jnp.bfloat16)
    grad_down = lax.dot_general(act, inbound, (((0,), (0,)), ((), ())), preferred_element_type=jnp.float32)
    act_grad = lax.dot_general(inbound, w_down, (((1,), (1,)), ((), ())), preferred_element_type=jnp.float32)
    up_delta = (act_grad * gate * sigma).astype(jnp.bfloat16)
    gate_delta = (act_grad * upper * sigma * (1.0 + gate * (1.0 - sigma))).astype(jnp.bfloat16)
    grad_gate = lax.dot_general(inputs, gate_delta, (((0,), (0,)), ((), ())), preferred_element_type=jnp.float32)
    grad_up = lax.dot_general(inputs, up_delta, (((0,), (0,)), ((), ())), preferred_element_type=jnp.float32)
    share = w_gate.shape[1] // N_TP
    total = jnp.zeros((inputs.shape[0], inputs.shape[1]), jnp.float32)
    for portion in range(N_TP):
        lower_col = portion * share
        partial_sum = lax.dot_general(gate_delta[:, lower_col:lower_col + share], w_gate[:, lower_col:lower_col + share], (((1,), (1,)), ((), ())), preferred_element_type=jnp.float32)
        partial_sum = partial_sum + lax.dot_general(up_delta[:, lower_col:lower_col + share], w_up[:, lower_col:lower_col + share], (((1,), (1,)), ((), ())), preferred_element_type=jnp.float32)
        total = total + lax.optimization_barrier(partial_sum.astype(jnp.bfloat16)).astype(jnp.float32)
    return (grad_gate.astype(jnp.bfloat16), grad_up.astype(jnp.bfloat16), grad_down.astype(jnp.bfloat16), total.astype(jnp.bfloat16))

def reference(layer_grad, routes, route_weight, slot_tokens, gate_proj, up_proj, down_proj, out_proj, queries, keys, values, fwd_decay, bwd_decay):
    per_block = routes.reshape(N_SP, TOK_DEV * 2).astype(jnp.int32)
    ranks = jax.vmap(functools.partial(slot_ranks, experts=EXPERTS))(per_block)
    source = jnp.arange(N_SP, dtype=jnp.int32)[:, None]
    kept = ranks < CAP
    target = jnp.where(kept, per_block * SLOTS + source * CAP + ranks, EXPERTS * SLOTS).reshape(-1).astype(jnp.int32)
    weighted = (layer_grad.astype(jnp.float32)[:, None, :] * route_weight[:, :, None]).astype(jnp.bfloat16).reshape(SEQUENCE_TOKENS * 2, D)
    inbound = jnp.zeros((EXPERTS * SLOTS + 1, D), jnp.bfloat16).at[target].set(weighted)[:EXPERTS * SLOTS].reshape(EXPERTS, SLOTS, D)
    grad_gate, grad_up, grad_down, slot_grad = lax.map(expert_back, (slot_tokens, inbound, gate_proj, up_proj, down_proj))
    picked = slot_grad.reshape(EXPERTS * SLOTS, D)[jnp.minimum(target, EXPERTS * SLOTS - 1)]
    picked = picked.astype(jnp.float32) * kept.reshape(-1, 1).astype(jnp.float32)
    moe_grad = lax.optimization_barrier(jnp.sum(picked.reshape(SEQUENCE_TOKENS, 2, D), axis=1))
    stream_grad = (layer_grad.astype(jnp.float32) + moe_grad).astype(jnp.bfloat16)
    scale = KEY_CHANNELS ** (-0.5)

    def split_heads(array, size):
        return array.astype(jnp.float32).reshape(SEQUENCE_TOKENS, ATTENTION_HEADS, size).transpose(1, 0, 2)

    def merge_heads(array):
        return array.transpose(1, 0, 2).reshape(SEQUENCE_TOKENS, -1)
    mixed, pullback = jax.vjp(mixer_forward, split_heads(queries, KEY_CHANNELS) * scale, split_heads(keys, KEY_CHANNELS), split_heads(values, DV), split_heads(fwd_decay, KEY_CHANNELS), split_heads(bwd_decay, KEY_CHANNELS))
    mixed_rows = merge_heads(mixed).astype(jnp.bfloat16)
    proj_grad = lax.dot_general(stream_grad, mixed_rows, (((0,), (0,)), ((), ())), preferred_element_type=jnp.float32)
    mixed_grad = jnp.dot(stream_grad, out_proj, preferred_element_type=jnp.float32)
    query_part, key_part, value_part, fwd_part, bwd_part = pullback(split_heads(mixed_grad, DV))
    return (grad_gate, grad_up, grad_down, proj_grad, (merge_heads(query_part) * scale).astype(jnp.bfloat16), merge_heads(key_part).astype(jnp.bfloat16), merge_heads(value_part).astype(jnp.bfloat16))
```

```python
import functools

import jax
import jax.numpy as jnp
from jax import lax
from jax.experimental import pallas as pl
from jax.experimental.pallas import tpu as pltpu
from jax.sharding import Mesh
from jax.sharding import PartitionSpec as P

KEY_CHANNELS = 64
DV = 128
BLOCK = 64
SP = ("sp_0", "sp_1", "sp_2")
EPSILON = 1e-06
CAP = 9
F32 = jnp.float32
BF16 = jnp.bfloat16
PIECE = 16
ROWS = PIECE + 8


def dot(a, b, contract=((1,), (0,))):
    return lax.dot_general(
        a.astype(BF16), b.astype(BF16), (contract, ((), ())), preferred_element_type=F32
    )


def dot_exact(a, b):
    return lax.dot_general(
        a,
        b,
        (((1,), (0,)), ((), ())),
        precision=lax.Precision.HIGHEST,
        preferred_element_type=F32,
    )


NT = ((1,), (1,))
TN = ((0,), (0,))


def iota(shape, dim):
    return lax.broadcasted_iota(jnp.int32, shape, dim)


def stacked(x):
    low = iota(x.shape, 1) < KEY_CHANNELS
    zero = jnp.zeros_like(x)
    return jnp.concatenate([jnp.where(low, x, zero), jnp.where(low, zero, x)], axis=0)


def doubled(x):
    return jnp.concatenate([x, x], axis=0)


def folded(x):
    half = x.shape[0] // 2
    return x[:half] + x[half:]


def heads_on_rows(x):
    return jnp.concatenate([x[:, :DV], x[:, DV:]], axis=0)


def heads_on_lanes(x):
    half = x.shape[0] // 2
    return jnp.concatenate([x[:half], x[half:]], axis=1)


def masks():
    shape = (2 * BLOCK, 2 * BLOCK)
    i, j = iota(shape, 0), iota(shape, 1)
    same = (i // BLOCK) == (j // BLOCK)
    return same & (i >= j), same & (i < j)


class Piece:
    def __init__(self, b, q_ref, k_ref, v_ref, fd_ref, bd_ref):
        rows = pl.ds(b * BLOCK, BLOCK)
        shape = (BLOCK, BLOCK)
        lower = (iota(shape, 0) >= iota(shape, 1)).astype(F32)
        upper = (iota(shape, 0) <= iota(shape, 1)).astype(F32)
        self.q = q_ref[rows, :].astype(F32) * KEY_CHANNELS**-0.5
        self.k = k_ref[rows, :].astype(F32)
        self.vs = heads_on_rows(v_ref[rows, :])
        self.g = dot_exact(lower, fd_ref[rows, :])
        self.h = dot_exact(upper, bd_ref[rows, :])
        self.last = self.g[BLOCK - 1 :, :]
        self.first = self.h[:1, :]
        self.mid_g = self.g[BLOCK // 2 - 1 : BLOCK // 2, :]
        self.mid_h = self.h[BLOCK // 2 : BLOCK // 2 + 1, :]

    def ends(self):
        self.eg_end = jnp.exp(self.last - self.g)
        self.eh_end = jnp.exp(self.first - self.h)
        self.kg_end = stacked(self.k * self.eg_end).astype(BF16)
        self.kh_end = stacked(self.k * self.eh_end).astype(BF16)
        self.fresh_f = dot(self.vs, self.kg_end, TN)
        self.fresh_b = dot(self.vs, self.kh_end, TN)

    def entries(self):
        self.eg = jnp.exp(self.g)
        self.eh = jnp.exp(self.h)
        self.qg = stacked(self.q * self.eg).astype(BF16)
        self.qh = stacked(self.q * self.eh).astype(BF16)

    def scores(self, inclusive, strict):
        self.up_g = jnp.exp(self.g - self.mid_g)
        self.dn_g = jnp.exp(self.mid_g - self.g)
        self.up_h = jnp.exp(self.h - self.mid_h)
        self.dn_h = jnp.exp(self.mid_h - self.h)
        self.q_up_g = stacked(self.q * self.up_g).astype(BF16)
        self.k_dn_g = stacked(self.k * self.dn_g).astype(BF16)
        self.q_up_h = stacked(self.q * self.up_h).astype(BF16)
        self.k_dn_h = stacked(self.k * self.dn_h).astype(BF16)
        a_f = jnp.where(inclusive, dot(self.q_up_g, self.k_dn_g, NT), 0.0)
        a_b = jnp.where(strict, dot(self.q_up_h, self.k_dn_h, NT), 0.0)
        return (a_f + a_b).astype(BF16)


def both_states(pieces, forward_entry, backward_entry):
    s, before = forward_entry, []
    for piece in pieces:
        before.append(s)
        s = jnp.exp(piece.last) * s + piece.fresh_f
    r, after = backward_entry, [None] * len(pieces)
    for b in reversed(range(len(pieces))):
        after[b] = r
        r = jnp.exp(pieces[b].first) * r + pieces[b].fresh_b
    return before, after, s, r


def position():
    z, y, c = (lax.axis_index(a) for a in SP)
    return z, y, c, y * 2 + c


def plane_peer(p, d, planes):
    other = lax.rem(p + d, planes)
    return other, {"sp_1": other // 2, "sp_2": lax.rem(other, 2)}


def greet(planes, depth):
    z, _, _, p = position()
    barrier = pltpu.get_barrier_semaphore()
    for d in range(1, planes):
        _, device = plane_peer(p, d, planes)
        pl.semaphore_signal(barrier, 1, device_id=device, device_id_type=pl.DeviceIdType.MESH)
    for d in range(1, depth):
        device = {"sp_0": lax.rem(z + d, depth)}
        pl.semaphore_signal(barrier, 1, device_id=device, device_id_type=pl.DeviceIdType.MESH)
    return barrier, planes + depth - 2


class Carry:
    SCRATCH_PLANES, SCRATCH_DEPTH = 8, 8

    @classmethod
    def scratch(cls):
        n, m = cls.SCRATCH_PLANES, cls.SCRATCH_DEPTH
        return [
            pltpu.VMEM((n, 2, ROWS, 128), F32),
            pltpu.VMEM((n, 2, ROWS, 128), F32),
            pltpu.VMEM((2, ROWS, 128), F32),
            pltpu.VMEM((m, ROWS, 128), F32),
            pltpu.VMEM((n, 2, PIECE, 128), F32),
            pltpu.VMEM((n, 2, PIECE, 128), F32),
            pltpu.SemaphoreType.DMA((n,)),
            pltpu.SemaphoreType.DMA((n,)),
            pltpu.SemaphoreType.DMA((m,)),
            pltpu.SemaphoreType.DMA((m,)),
            pltpu.SemaphoreType.DMA((n,)),
            pltpu.SemaphoreType.DMA((n,)),
        ]

    def __init__(self, refs):
        (
            self.out1,
            self.in1,
            self.out2,
            self.in2,
            self.out3,
            self.in3,
            self.s1,
            self.r1,
            self.s2,
            self.r2,
            self.s3,
            self.r3,
        ) = refs
        self.n, self.m = self.SCRATCH_PLANES, self.SCRATCH_DEPTH
        self.z, _, _, self.p = position()

    def plane_copy(self, out, into, send, recv, d, arriving=False):
        other, device = plane_peer(self.p, d, self.n)
        at = other if arriving else self.p
        return pltpu.make_async_remote_copy(
            src_ref=out.at[other],
            dst_ref=into.at[at],
            send_sem=send.at[other],
            recv_sem=recv.at[at],
            device_id=device,
            device_id_type=pl.DeviceIdType.MESH,
        )

    def start(self, terms, logs):
        for dim in range(2):
            decay = jnp.broadcast_to(logs[dim], (8, 128))
            for j in range(self.n):
                self.out1[j, dim, :PIECE, :] = terms[dim][j * PIECE : (j + 1) * PIECE, :]
                self.out1[j, dim, PIECE:, :] = decay
        for d in range(1, self.n):
            self.plane_copy(self.out1, self.in1, self.s1, self.r1, d).start()
        self.in1[self.p] = self.out1[self.p]

    def middle(self):
        for d in range(1, self.n):
            self.plane_copy(self.out1, self.in1, self.s1, self.r1, d, True).wait_recv()
        zero = jnp.zeros((PIECE, 128), F32)
        none = jnp.zeros((1, 128), F32)
        self.before = [[None] * self.n, [None] * self.n]
        for dim in range(2):
            total, log = zero, none
            for i in range(self.n) if dim == 0 else reversed(range(self.n)):
                self.before[dim][i] = (total, log)
                step = self.in1[i, dim, PIECE : PIECE + 1, :]
                total = total * jnp.exp(step) + self.in1[i, dim, :PIECE, :]
                log = log + step
            self.out2[dim, :PIECE, :] = total
            self.out2[dim, PIECE:, :] = jnp.broadcast_to(log, (8, 128))
        for d in range(1, self.m):
            self.depth_copy(d).start()

    def depth_copy(self, d, arriving=False):
        other = lax.rem(self.z + d, self.m)
        dim = jnp.where(other > self.z, 0, 1)
        at = other if arriving else self.z
        return pltpu.make_async_remote_copy(
            src_ref=self.out2.at[dim],
            dst_ref=self.in2.at[at],
            send_sem=self.s2.at[other],
            recv_sem=self.r2.at[at],
            device_id={"sp_0": other},
            device_id_type=pl.DeviceIdType.MESH,
        )

    def last(self):
        self.in2[self.z] = jnp.zeros((ROWS, 128), F32)
        for d in range(1, self.m):
            self.depth_copy(d, True).wait_recv()
        entry = []
        for dim in range(2):
            total = jnp.zeros((PIECE, 128), F32)
            for i in range(self.m) if dim == 0 else reversed(range(self.m)):
                passed = (i < self.z) if dim == 0 else (i > self.z)
                step = self.in2[i, PIECE : PIECE + 1, :]
                total = jnp.where(passed, total * jnp.exp(step) + self.in2[i, :PIECE, :], total)
            entry.append(total)
        for i in range(self.n):
            for dim in range(2):
                inside, log = self.before[dim][i]
                self.out3[i, dim] = inside + jnp.exp(log) * entry[dim]
        for d in range(1, self.n):
            self.plane_copy(self.out3, self.in3, self.s3, self.r3, d).start()
        self.in3[self.p] = self.out3[self.p]

    def finish(self):
        for d in range(1, self.n):
            self.plane_copy(self.out3, self.in3, self.s3, self.r3, d, True).wait_recv()
        for d in range(1, self.n):
            self.plane_copy(self.out1, self.in1, self.s1, self.r1, d).wait_send()
            self.plane_copy(self.out3, self.in3, self.s3, self.r3, d).wait_send()
        for d in range(1, self.m):
            self.depth_copy(d).wait_send()
        return [self.in3[:, dim].reshape(128, 128) for dim in range(2)]


def forward_kernel(q, k, v, fd, bd, o_ref, rows_ref, entry_ref, *scratch):
    barrier, count = greet(8, 8)
    pieces = [Piece(b, q, k, v, fd, bd) for b in range(3)]
    for piece in pieces:
        piece.ends()
    zero = jnp.zeros((DV, 128), F32)
    _, _, forward_end, backward_end = both_states(pieces, zero, zero)
    log_f = sum(piece.last for piece in pieces)
    log_b = sum(piece.first for piece in pieces)
    pl.semaphore_wait(barrier, count)
    carry = Carry(scratch)
    carry.start((forward_end, backward_end), (log_f, log_b))
    inclusive, strict = masks()
    inner = []
    for piece in pieces:
        inner.append(dot(piece.scores(inclusive, strict), piece.vs))
        piece.entries()
    carry.middle()
    carry.last()
    forward_entry, backward_entry = carry.finish()
    entry_ref[0] = forward_entry
    entry_ref[1] = backward_entry
    before, after, _, _ = both_states(pieces, forward_entry, backward_entry)
    for b, piece in enumerate(pieces):
        left = jnp.concatenate([piece.qg, piece.qh], axis=1)
        right = jnp.concatenate([before[b], after[b]], axis=1)
        o = inner[b] + dot(left, right, NT)
        o_ref[b] = o
        mixed = o * lax.rsqrt(jnp.mean(o * o, axis=1, keepdims=True) + EPSILON)
        rows_ref[pl.ds(b * BLOCK, BLOCK), :] = heads_on_lanes(mixed).astype(BF16)


def backward_kernel(
    stream, out_proj, q, k, v, fd, bd, o_ref, entry_ref, dq_ref, dk_ref, dv_ref, *scratch
):
    barrier, count = greet(8, 8)
    pieces = [Piece(b, q, k, v, fd, bd) for b in range(3)]
    mixed_grad = jnp.dot(stream[...], out_proj[...], preferred_element_type=F32)
    c, d = jnp.zeros((DV, 128), F32), jnp.zeros((DV, 128), F32)
    for b, piece in enumerate(pieces):
        o = o_ref[b]
        inv = lax.rsqrt(jnp.mean(o * o, axis=1, keepdims=True) + EPSILON)
        mixed = o * inv
        mg = heads_on_rows(mixed_grad[b * BLOCK : (b + 1) * BLOCK, :])
        piece.do = (inv * (mg - mixed * jnp.mean(mg * mixed, axis=1, keepdims=True))).astype(BF16)
        piece.entries()
        piece.back_f = dot(piece.do, piece.qg, TN)
        piece.back_b = dot(piece.do, piece.qh, TN)
    for piece in pieces:
        c = c * jnp.exp(piece.first) + piece.back_b
    for piece in reversed(pieces):
        d = d * jnp.exp(piece.last) + piece.back_f
    log_f = sum(piece.last for piece in pieces)
    log_b = sum(piece.first for piece in pieces)
    pl.semaphore_wait(barrier, count)
    carry = Carry(scratch)
    carry.start((c, d), (log_b, log_f))
    inclusive, strict = masks()
    for piece in pieces:
        a = piece.scores(inclusive, strict)
        da = dot(piece.do, piece.vs, NT)
        da_f = jnp.where(inclusive, da, 0.0).astype(BF16)
        da_b = jnp.where(strict, da, 0.0).astype(BF16)
        piece.dv = dot(a, piece.do, TN)
        piece.dq = dot(da_f, piece.k_dn_g) * doubled(piece.up_g) + dot(
            da_b, piece.k_dn_h
        ) * doubled(piece.up_h)
        piece.dk = dot(da_f, piece.q_up_g, TN) * doubled(piece.dn_g) + dot(
            da_b, piece.q_up_h, TN
        ) * doubled(piece.dn_h)
    carry.middle()
    for piece in pieces:
        piece.ends()
    before, after, _, _ = both_states(pieces, entry_ref[0], entry_ref[1])
    for b, piece in enumerate(pieces):
        dq = dot(piece.do, jnp.concatenate([before[b], after[b]], axis=1))
        piece.dq = piece.dq + dq[:, :128] * stacked(piece.eg) + dq[:, 128:] * stacked(piece.eh)
        dq_ref[pl.ds(b * BLOCK, BLOCK), :] = (folded(piece.dq) * KEY_CHANNELS**-0.5).astype(BF16)
    carry.last()
    c, d = carry.finish()
    late, early = [None] * 3, [None] * 3
    for b, piece in enumerate(pieces):
        early[b] = c
        c = c * jnp.exp(piece.first) + piece.back_b
    for b in reversed(range(3)):
        late[b] = d
        d = d * jnp.exp(pieces[b].last) + pieces[b].back_f
    for b, piece in enumerate(pieces):
        states = jnp.concatenate([late[b], early[b]], axis=1).astype(BF16)
        dk = dot(piece.vs, states)
        dk = piece.dk + dk[:, :128] * stacked(piece.eg_end) + dk[:, 128:] * stacked(piece.eh_end)
        dv = piece.dv + dot(jnp.concatenate([piece.kg_end, piece.kh_end], axis=1), states, NT)
        rows = pl.ds(b * BLOCK, BLOCK)
        dk_ref[rows, :] = folded(dk).astype(BF16)
        dv_ref[rows, :] = heads_on_lanes(dv).astype(BF16)


def vmem(n):
    return [pl.BlockSpec(memory_space=pltpu.VMEM)] * n


def attention_forward(q, k, v, fd, bd):
    tokens = q.shape[0]
    return pl.pallas_call(
        forward_kernel,
        out_shape=(
            jax.ShapeDtypeStruct((3, 128, DV), F32),
            jax.ShapeDtypeStruct((tokens, 2 * DV), BF16),
            jax.ShapeDtypeStruct((2, DV, 128), F32),
        ),
        in_specs=vmem(5),
        out_specs=tuple(vmem(3)),
        scratch_shapes=Carry.scratch(),
        compiler_params=pltpu.CompilerParams(collective_id=0, has_side_effects=True),
        cost_estimate=pl.CostEstimate(
            flops=10**9, bytes_accessed=2**20, transcendentals=0
        ),
        name="attention_forward",
    )(q, k, v, fd, bd)


def attention_backward(stream, out_proj, q, k, v, fd, bd, o, entry):
    tokens = q.shape[0]
    return pl.pallas_call(
        backward_kernel,
        out_shape=(
            jax.ShapeDtypeStruct((tokens, 128), BF16),
            jax.ShapeDtypeStruct((tokens, 128), BF16),
            jax.ShapeDtypeStruct((tokens, 2 * DV), BF16),
        ),
        in_specs=vmem(9),
        out_specs=tuple(vmem(3)),
        scratch_shapes=Carry.scratch(),
        compiler_params=pltpu.CompilerParams(collective_id=1, has_side_effects=True),
        cost_estimate=pl.CostEstimate(
            flops=10**9, bytes_accessed=2**21, transcendentals=0
        ),
        name="attention_backward",
    )(stream, out_proj, q, k, v, fd, bd, o, entry)


def copy_for_each(array, axis):
    devices = lax.axis_size(axis)
    return lax.all_to_all(
        jnp.broadcast_to(array[None], (devices, *array.shape)), axis, 0, 0, tiled=True
    )


def in_order(pieces, dim):
    shape = list(pieces.shape[1:])
    shape[dim] *= pieces.shape[0]
    return jnp.moveaxis(pieces, 0, dim).reshape(shape)


def slot_choice(routes, weights, experts, slots):
    tokens = routes.shape[0]
    ids = routes.reshape(-1)
    members = (ids[:, None] == jnp.arange(experts, dtype=jnp.int32)[None, :]).astype(BF16)
    earlier = jnp.tril(jnp.ones((2 * tokens, 2 * tokens), BF16), -1)
    before = jnp.dot(earlier, members, preferred_element_type=F32)
    ranks = jnp.sum(before * members.astype(F32), axis=1).astype(jnp.int32)
    target = jnp.where(ranks < CAP, ids * CAP + ranks, -1).reshape(tokens, 2)
    slot = jnp.arange(slots, dtype=jnp.int32)[:, None]
    first = slot == target[:, 0][None, :]
    second = slot == target[:, 1][None, :]
    chosen = (first | second).astype(BF16)
    weight = jnp.sum(
        jnp.where(first, weights[:, 0][None, :], 0.0)
        + jnp.where(second, weights[:, 1][None, :], 0.0),
        axis=1,
        keepdims=True,
    )
    return chosen, weight


def on_device(
    layer_grad,
    routes,
    route_weight,
    slot_tokens,
    gate_proj,
    up_proj,
    down_proj,
    out_proj,
    queries,
    keys,
    values,
    fwd_decay,
    bwd_decay,
):
    devices = lax.axis_size(SP)
    width = layer_grad.shape[1]
    slots = slot_tokens.shape[1]
    capacity = slots // devices
    quarter = width // lax.axis_size("tp")
    chosen, weight = slot_choice(routes, route_weight, devices, slots)
    own_columns = lax.dynamic_slice_in_dim(layer_grad, lax.axis_index("tp") * quarter, quarter, 1)
    outgoing = (jnp.dot(chosen, own_columns, preferred_element_type=F32) * weight).astype(BF16)
    arrived = lax.all_to_all(
        outgoing.reshape(devices, capacity, quarter), SP, split_axis=0, concat_axis=0, tiled=True
    ).reshape(slots, quarter)
    o, mixed_rows, entry = attention_forward(queries, keys, values, fwd_decay, bwd_decay)
    inbound = in_order(copy_for_each(arrived, "tp"), 1)
    inputs = slot_tokens[0]
    w_gate = gate_proj[0]
    w_upper = up_proj[0]
    w_down = down_proj[0]
    gate = jnp.dot(inputs, w_gate, preferred_element_type=F32)
    upper = jnp.dot(inputs, w_upper, preferred_element_type=F32)
    sigma = jax.nn.sigmoid(gate)
    act = (gate * sigma * upper).astype(BF16)
    grad_down = lax.dot_general(act, inbound, (TN, ((), ())), preferred_element_type=F32)
    act_grad = lax.dot_general(inbound, w_down, (NT, ((), ())), preferred_element_type=F32)
    up_delta = (act_grad * gate * sigma).astype(BF16)
    gate_delta = (act_grad * upper * sigma * (1.0 + gate * (1.0 - sigma))).astype(BF16)
    slot_part = lax.dot_general(gate_delta, w_gate, (NT, ((), ())), preferred_element_type=F32)
    slot_part = slot_part + lax.dot_general(
        up_delta, w_upper, (NT, ((), ())), preferred_element_type=F32
    )
    summed = lax.psum_scatter(slot_part.astype(BF16), "tp", scatter_dimension=1, tiled=True)
    grad_gate = lax.dot_general(inputs, gate_delta, (TN, ((), ())), preferred_element_type=F32)
    grad_up = lax.dot_general(inputs, up_delta, (TN, ((), ())), preferred_element_type=F32)
    backrows = lax.all_to_all(
        summed.reshape(devices, capacity, quarter), SP, split_axis=0, concat_axis=0, tiled=True
    ).reshape(slots, quarter)
    moe_grad = lax.dot_general(chosen, backrows, (TN, ((), ())), preferred_element_type=F32)
    stream_part = (own_columns.astype(F32) + moe_grad).astype(BF16)
    stream_grad = lax.all_gather(stream_part, "tp", axis=1, tiled=True)
    terms = lax.dot_general(
        stream_grad, mixed_rows, (TN, ((), ())), preferred_element_type=F32
    ).astype(BF16)
    arrived_terms = lax.all_to_all(
        terms.reshape(devices, -1, terms.shape[1]), SP, split_axis=0, concat_axis=0, tiled=True
    )
    proj_grad = arrived_terms.astype(F32).sum(axis=0)
    query_grad, key_grad, value_grad = attention_backward(
        stream_grad, out_proj, queries, keys, values, fwd_decay, bwd_decay, o, entry
    )
    return (
        grad_gate.astype(BF16)[None],
        grad_up.astype(BF16)[None],
        grad_down.astype(BF16)[None],
        proj_grad,
        query_grad,
        key_grad,
        value_grad,
    )


def solution(mesh):
    torus = Mesh(mesh.devices.reshape(8, 4, 2, mesh.shape["tp"]), ("sp_0", "sp_1", "sp_2", "tp"))
    in_specs = (
        P(SP, None),
        P(SP, None),
        P(SP, None),
        P(SP, None, None),
        P(SP, None, "tp"),
        P(SP, None, "tp"),
        P(SP, "tp", None),
        P(None, "tp"),
        P(SP, "tp"),
        P(SP, "tp"),
        P(SP, "tp"),
        P(SP, "tp"),
        P(SP, "tp"),
    )
    out_specs = (
        P(SP, None, "tp"),
        P(SP, None, "tp"),
        P(SP, "tp", None),
        P(SP, "tp"),
        P(SP, "tp"),
        P(SP, "tp"),
        P(SP, "tp"),
    )
    return jax.shard_map(
        on_device, mesh=torus, in_specs=in_specs, out_specs=out_specs, check_vma=False
    )
```

```python
import jax
import jax.numpy as jnp
from jax import lax
from jax.experimental import pallas as pl
from jax.experimental.pallas import tpu as pltpu
from jax.sharding import Mesh
from jax.sharding import PartitionSpec as P

KEY_CHANNELS = 64
DV = 128
BLOCK = 64
SP = ("sp_0", "sp_1", "sp_2")
EPSILON = 1e-06
CAP = 9
F32 = jnp.float32
BF16 = jnp.bfloat16
PIECE = 16
ROWS = PIECE + 8


def dot(a, b, contract=((1,), (0,))):
    return lax.dot_general(
        a.astype(BF16), b.astype(BF16), (contract, ((), ())), preferred_element_type=F32
    )


def dot_exact(a, b):
    return lax.dot_general(
        a,
        b,
        (((1,), (0,)), ((), ())),
        precision=lax.Precision.HIGHEST,
        preferred_element_type=F32,
    )


NT = ((1,), (1,))
TN = ((0,), (0,))


def iota(shape, dim):
    return lax.broadcasted_iota(jnp.int32, shape, dim)


def stacked(x):
    low = iota(x.shape, 1) < KEY_CHANNELS
    zero = jnp.zeros_like(x)
    return jnp.concatenate([jnp.where(low, x, zero), jnp.where(low, zero, x)], axis=0)


def doubled(x):
    return jnp.concatenate([x, x], axis=0)


def folded(x):
    half = x.shape[0] // 2
    return x[:half] + x[half:]


def heads_on_rows(x):
    return jnp.concatenate([x[:, :DV], x[:, DV:]], axis=0)


def heads_on_lanes(x):
    half = x.shape[0] // 2
    return jnp.concatenate([x[:half], x[half:]], axis=1)


def masks():
    shape = (2 * BLOCK, 2 * BLOCK)
    i, j = iota(shape, 0), iota(shape, 1)
    same = (i // BLOCK) == (j // BLOCK)
    return same & (i >= j), same & (i < j)


class Piece:
    def __init__(self, b, q_ref, k_ref, v_ref, fd_ref, bd_ref):
        rows = pl.ds(b * BLOCK, BLOCK)
        shape = (BLOCK, BLOCK)
        lower = (iota(shape, 0) >= iota(shape, 1)).astype(F32)
        upper = (iota(shape, 0) <= iota(shape, 1)).astype(F32)
        self.q = q_ref[rows, :].astype(F32) * KEY_CHANNELS**-0.5
        self.k = k_ref[rows, :].astype(F32)
        self.vs = heads_on_rows(v_ref[rows, :])
        self.g = dot_exact(lower, fd_ref[rows, :])
        self.h = dot_exact(upper, bd_ref[rows, :])
        self.last = self.g[BLOCK - 1 :, :]
        self.first = self.h[:1, :]
        self.mid_g = self.g[BLOCK // 2 - 1 : BLOCK // 2, :]
        self.mid_h = self.h[BLOCK // 2 : BLOCK // 2 + 1, :]

    def ends(self):
        self.eg_end = jnp.exp(self.last - self.g)
        self.eh_end = jnp.exp(self.first - self.h)
        self.kg_end = stacked(self.k * self.eg_end).astype(BF16)
        self.kh_end = stacked(self.k * self.eh_end).astype(BF16)
        self.fresh_f = dot(self.vs, self.kg_end, TN)
        self.fresh_b = dot(self.vs, self.kh_end, TN)

    def entries(self):
        self.eg = jnp.exp(self.g)
        self.eh = jnp.exp(self.h)
        self.qg = stacked(self.q * self.eg).astype(BF16)
        self.qh = stacked(self.q * self.eh).astype(BF16)

    def scores(self, inclusive, strict):
        self.up_g = jnp.exp(self.g - self.mid_g)
        self.dn_g = jnp.exp(self.mid_g - self.g)
        self.up_h = jnp.exp(self.h - self.mid_h)
        self.dn_h = jnp.exp(self.mid_h - self.h)
        self.q_up_g = stacked(self.q * self.up_g).astype(BF16)
        self.k_dn_g = stacked(self.k * self.dn_g).astype(BF16)
        self.q_up_h = stacked(self.q * self.up_h).astype(BF16)
        self.k_dn_h = stacked(self.k * self.dn_h).astype(BF16)
        a_f = jnp.where(inclusive, dot(self.q_up_g, self.k_dn_g, NT), 0.0)
        a_b = jnp.where(strict, dot(self.q_up_h, self.k_dn_h, NT), 0.0)
        return (a_f + a_b).astype(BF16)


def both_states(pieces, forward_entry, backward_entry):
    s, before = forward_entry, []
    for piece in pieces:
        before.append(s)
        s = jnp.exp(piece.last) * s + piece.fresh_f
    r, after = backward_entry, [None] * len(pieces)
    for b in reversed(range(len(pieces))):
        after[b] = r
        r = jnp.exp(pieces[b].first) * r + pieces[b].fresh_b
    return before, after, s, r


def position():
    z, y, c = (lax.axis_index(a) for a in SP)
    return z, y, c, y * 2 + c


def plane_peer(p, d, planes):
    other = lax.rem(p + d, planes)
    return other, {"sp_1": other // 2, "sp_2": lax.rem(other, 2)}


def greet(planes, depth):
    z, _, _, p = position()
    barrier = pltpu.get_barrier_semaphore()
    for d in range(1, planes):
        _, device = plane_peer(p, d, planes)
        pl.semaphore_signal(barrier, 1, device_id=device, device_id_type=pl.DeviceIdType.MESH)
    for d in range(1, depth):
        device = {"sp_0": lax.rem(z + d, depth)}
        pl.semaphore_signal(barrier, 1, device_id=device, device_id_type=pl.DeviceIdType.MESH)
    return barrier, planes + depth - 2


class Carry:
    SCRATCH_PLANES, SCRATCH_DEPTH = 8, 8

    @classmethod
    def scratch(cls):
        n, m = cls.SCRATCH_PLANES, cls.SCRATCH_DEPTH
        return [
            pltpu.VMEM((n, 2, ROWS, 128), F32),
            pltpu.VMEM((n, 2, ROWS, 128), F32),
            pltpu.VMEM((2, ROWS, 128), F32),
            pltpu.VMEM((m, ROWS, 128), F32),
            pltpu.VMEM((n, 2, PIECE, 128), F32),
            pltpu.VMEM((n, 2, PIECE, 128), F32),
            pltpu.SemaphoreType.DMA((n,)),
            pltpu.SemaphoreType.DMA((n,)),
            pltpu.SemaphoreType.DMA((m,)),
            pltpu.SemaphoreType.DMA((m,)),
            pltpu.SemaphoreType.DMA((n,)),
            pltpu.SemaphoreType.DMA((n,)),
        ]

    def __init__(self, refs):
        (
            self.out1,
            self.in1,
            self.out2,
            self.in2,
            self.out3,
            self.in3,
            self.s1,
            self.r1,
            self.s2,
            self.r2,
            self.s3,
            self.r3,
        ) = refs
        self.n, self.m = self.SCRATCH_PLANES, self.SCRATCH_DEPTH
        self.z, _, _, self.p = position()

    def plane_copy(self, out, into, send, recv, d, arriving=False):
        other, device = plane_peer(self.p, d, self.n)
        at = other if arriving else self.p
        return pltpu.make_async_remote_copy(
            src_ref=out.at[other],
            dst_ref=into.at[at],
            send_sem=send.at[other],
            recv_sem=recv.at[at],
            device_id=device,
            device_id_type=pl.DeviceIdType.MESH,
        )

    def start(self, terms, logs):
        for dim in range(2):
            decay = jnp.broadcast_to(logs[dim], (8, 128))
            for j in range(self.n):
                self.out1[j, dim, :PIECE, :] = terms[dim][j * PIECE : (j + 1) * PIECE, :]
                self.out1[j, dim, PIECE:, :] = decay
        for d in range(1, self.n):
            self.plane_copy(self.out1, self.in1, self.s1, self.r1, d).start()
        self.in1[self.p] = self.out1[self.p]

    def middle(self):
        for d in range(1, self.n):
            self.plane_copy(self.out1, self.in1, self.s1, self.r1, d, True).wait_recv()
        zero = jnp.zeros((PIECE, 128), F32)
        none = jnp.zeros((1, 128), F32)
        self.before = [[None] * self.n, [None] * self.n]
        for dim in range(2):
            total, log = zero, none
            for i in range(self.n) if dim == 0 else reversed(range(self.n)):
                self.before[dim][i] = (total, log)
                step = self.in1[i, dim, PIECE : PIECE + 1, :]
                total = total * jnp.exp(step) + self.in1[i, dim, :PIECE, :]
                log = log + step
            self.out2[dim, :PIECE, :] = total
            self.out2[dim, PIECE:, :] = jnp.broadcast_to(log, (8, 128))
        for d in range(1, self.m):
            self.depth_copy(d).start()

    def depth_copy(self, d, arriving=False):
        other = lax.rem(self.z + d, self.m)
        dim = jnp.where(other > self.z, 0, 1)
        at = other if arriving else self.z
        return pltpu.make_async_remote_copy(
            src_ref=self.out2.at[dim],
            dst_ref=self.in2.at[at],
            send_sem=self.s2.at[other],
            recv_sem=self.r2.at[at],
            device_id={"sp_0": other},
            device_id_type=pl.DeviceIdType.MESH,
        )

    def last(self):
        self.in2[self.z] = jnp.zeros((ROWS, 128), F32)
        for d in range(1, self.m):
            self.depth_copy(d, True).wait_recv()
        entry = []
        for dim in range(2):
            total = jnp.zeros((PIECE, 128), F32)
            for i in range(self.m) if dim == 0 else reversed(range(self.m)):
                passed = (i < self.z) if dim == 0 else (i > self.z)
                step = self.in2[i, PIECE : PIECE + 1, :]
                total = jnp.where(passed, total * jnp.exp(step) + self.in2[i, :PIECE, :], total)
            entry.append(total)
        for i in range(self.n):
            for dim in range(2):
                inside, log = self.before[dim][i]
                self.out3[i, dim] = inside + jnp.exp(log) * entry[dim]
        for d in range(1, self.n):
            self.plane_copy(self.out3, self.in3, self.s3, self.r3, d).start()
        self.in3[self.p] = self.out3[self.p]

    def finish(self):
        for d in range(1, self.n):
            self.plane_copy(self.out3, self.in3, self.s3, self.r3, d, True).wait_recv()
        for d in range(1, self.n):
            self.plane_copy(self.out1, self.in1, self.s1, self.r1, d).wait_send()
            self.plane_copy(self.out3, self.in3, self.s3, self.r3, d).wait_send()
        for d in range(1, self.m):
            self.depth_copy(d).wait_send()
        return [self.in3[:, dim].reshape(128, 128) for dim in range(2)]


OFFSETS = (0, 1, 7, 2, 6, 3, 5, 4)
PLANE_ORDER = (2, 6, 3, 7, 4, 5, 1)
PLANES, DEPTH, RING = 8, 8, 4
CHUNK = PLANES * CAP
MESH = pl.DeviceIdType.MESH


def remote(src, dst, sems, device):
    return pltpu.make_async_remote_copy(
        src_ref=src,
        dst_ref=dst,
        send_sem=sems[0],
        recv_sem=sems[1],
        device_id=device,
        device_id_type=MESH,
    )


def swap_matrix(shape):
    i = iota((shape[0], 1), 0)
    a = (i * 911) >> 16
    rest = i - a * CHUNK
    b = (rest * 7282) >> 16
    source = b * CHUNK + a * CAP + (rest - b * CAP)
    return jnp.where(source == iota(shape, 1), 1.0, 0.0).astype(BF16)


def expert_kernel(
    chosen,
    weight,
    layer_grad,
    slot_tokens,
    gate_proj,
    up_proj,
    down_proj,
    q,
    k,
    v,
    fd,
    bd,
    stream_ref,
    gate_grad_ref,
    up_grad_ref,
    down_grad_ref,
    o_ref,
    rows_ref,
    entry_ref,
    own,
    x,
    w_cat,
    w_down,
    swap,
    act,
    silu,
    slope,
    delta,
    out_plane,
    in_plane,
    out_depth,
    inbound,
    part,
    hop,
    hopped,
    both,
    plain,
    ret_out,
    ret_in,
    back_out,
    back_in,
    stream,
    send,
    recv,
    load,
    *carry_refs,
):
    z, _, _, p = position()
    t = lax.axis_index("tp")
    right, left, across = lax.rem(t + 1, RING), lax.rem(t + 3, RING), lax.rem(t + 2, RING)
    quarter = own.shape[1]
    barrier, count = greet(PLANES, DEPTH)
    for other in (left, right):
        pl.semaphore_signal(barrier, 1, device_id={"tp": other}, device_id_type=MESH)

    columns = pl.ds(pl.multiple_of(t * quarter, quarter), quarter)
    hidden = w_down.shape[0]
    loads = [
        pltpu.make_async_copy(layer_grad.at[:, columns], own, load.at[0]),
        pltpu.make_async_copy(slot_tokens.at[0], x, load.at[1]),
        pltpu.make_async_copy(gate_proj.at[0], w_cat.at[:, pl.ds(0, hidden)], load.at[2]),
        pltpu.make_async_copy(up_proj.at[0], w_cat.at[:, pl.ds(hidden, hidden)], load.at[3]),
        pltpu.make_async_copy(down_proj.at[0], w_down, load.at[4]),
    ]
    for copy in loads:
        copy.start()

    def sems(kind, i):
        return send.at[kind, i], recv.at[kind, i]

    def plane_out(kind, out, into, d):
        other, device = plane_peer(p, d, PLANES)
        return remote(out.at[other], into.at[p], sems(kind, d), device)

    def plane_in(kind, out, into, d):
        other, device = plane_peer(p, PLANES - d, PLANES)
        return remote(out.at[other], into.at[other], sems(kind, d), device)

    loads[0].wait()
    picked = dot(chosen[...], own[...]) * weight[...]
    out_plane[...] = picked.astype(BF16).reshape(out_plane.shape)
    pl.semaphore_wait(barrier, count + 2)
    for d in PLANE_ORDER:
        plane_out(0, out_plane, in_plane, d).start()
    in_plane[p] = out_plane[p]

    pieces = [Piece(b, q, k, v, fd, bd) for b in range(3)]
    for piece in pieces:
        piece.ends()
    zero = jnp.zeros((DV, 128), F32)
    _, _, forward_end, backward_end = both_states(pieces, zero, zero)
    log_f = sum(piece.last for piece in pieces)
    log_b = sum(piece.first for piece in pieces)
    carry = Carry(carry_refs)
    carry.start((forward_end, backward_end), (log_f, log_b))
    swap[...] = swap_matrix(swap.shape)

    for d in PLANE_ORDER:
        plane_in(0, out_plane, in_plane, d).wait_recv()
    moved = dot(swap[...], in_plane[...].reshape(DEPTH * CHUNK, quarter)).astype(BF16)
    out_depth[...] = moved.reshape(out_depth.shape)
    carry.middle()

    def depth_out(i):
        other = lax.rem(z + DEPTH - OFFSETS[i], DEPTH)
        return remote(out_depth.at[other], inbound.at[t, z], sems(1, i), {"sp_0": other})

    for i in range(1, DEPTH):
        depth_out(i).start()
    inbound[t, z] = out_depth[z]

    for copy in loads[1:4]:
        copy.wait()
    half = x.shape[0] // 2
    for j in range(2):
        rows = pl.ds(j * half, half)
        chunks = pl.ds(j * (DEPTH // 2), DEPTH // 2)
        both_up = jnp.dot(x[rows, :], w_cat[...], preferred_element_type=F32)
        gate, up = both_up[:, :hidden], both_up[:, hidden:]
        sigma = jax.nn.sigmoid(gate)
        s = gate * sigma
        shape = (DEPTH // 2, CHUNK, hidden)
        silu[chunks] = s.reshape(shape)
        act[chunks] = (s * up).astype(BF16).reshape(shape)
        slope[chunks] = (up * sigma * (1.0 + gate * (1.0 - sigma))).reshape(shape)
    loads[4].wait()

    def chunk_of(i):
        return lax.rem(z + OFFSETS[i], DEPTH)

    def spread(i, arriving=False):
        at = chunk_of(i)
        a, b = (left, right) if arriving else (t, t)
        return (
            remote(inbound.at[a, at], inbound.at[a, at], sems(2, i), {"tp": right}),
            remote(inbound.at[b, at], inbound.at[b, at], sems(3, i), {"tp": left}),
        )

    def sides(i):
        return (left, right) if i % 2 == 0 else (right, left)

    def pass_on(i, arriving=False):
        source, to = sides(i)
        at, which = chunk_of(i), across if arriving else source
        return remote(inbound.at[which, at], inbound.at[which, at], sems(4, i), {"tp": to})

    def send_hop(i):
        _, to = sides(i)
        return remote(part.at[i, across], hop.at[i], sems(5, i), {"tp": to})

    def send_both(i):
        _, to = sides(i)
        return remote(hopped.at[i], both.at[i], sems(6, i), {"tp": to})

    def send_plain(i):
        to, _ = sides(i)
        return remote(part.at[i, to], plain.at[i], sems(7, i), {"tp": to})

    def send_back(i, arriving=False):
        at = lax.rem(z + DEPTH - OFFSETS[i], DEPTH) if arriving else z
        other = chunk_of(i)
        return remote(ret_out.at[other], ret_in.at[at], sems(8, i), {"sp_0": other})

    def stage_0(i):
        if i > 0:
            at = chunk_of(i)
            remote(out_depth.at[at], inbound.at[t, at], sems(1, i), {"sp_0": at}).wait_recv()
        for copy in spread(i):
            copy.start()

    def stage_1(i):
        for copy in spread(i, True):
            copy.wait_recv()
        pass_on(i).start()

    def stage_2(i):
        at = chunk_of(i)
        pass_on(i, True).wait_recv()
        total = jnp.zeros((CHUNK, hidden), F32)
        for n in range(RING):
            total = total + dot(inbound[n, at], w_down[:, n * quarter : (n + 1) * quarter], NT)
        up_delta = (total * silu[at]).astype(BF16)
        gate_delta = (total * slope[at]).astype(BF16)
        deltas = jnp.concatenate([gate_delta, up_delta], axis=1)
        delta[at] = deltas
        _, to = sides(i)
        for n, which in enumerate((across, sides(i)[0], to, t)):
            rows = pl.ds(pl.multiple_of(which * quarter, quarter), quarter)
            part[i, which] = dot(deltas, w_cat[rows, :], NT).astype(BF16)
            if n == 0:
                send_hop(i).start()
            if n == 1:
                send_plain(i).start()

    def stage_3(i):
        _, to = sides(i)
        send_hop(i).wait_recv()
        hopped[i] = (hop[i].astype(F32) + part[i, to].astype(F32)).astype(BF16)
        send_both(i).start()

    def stage_4(i):
        at = chunk_of(i)
        send_both(i).wait_recv()
        send_plain(i).wait_recv()
        total = part[i, t].astype(F32) + both[i].astype(F32) + plain[i].astype(F32)
        if i == 0:
            ret_in[z] = total.astype(BF16)
        else:
            ret_out[at] = total.astype(BF16)
            send_back(i).start()

    stages = (stage_0, stage_1, stage_2, stage_3, stage_4)
    for n in range(DEPTH + len(stages) - 1):
        for lag, stage in enumerate(stages):
            if 0 <= n - lag < DEPTH:
                stage(n - lag)
        if n == 0:
            carry.last()
        if n == 1:
            inclusive, strict = masks()
            inner = []
            for piece in pieces:
                inner.append(dot(piece.scores(inclusive, strict), piece.vs))
                piece.entries()
        if n == 3:
            forward_entry, backward_entry = carry.finish()
            entry_ref[0] = forward_entry
            entry_ref[1] = backward_entry
            before, after, _, _ = both_states(pieces, forward_entry, backward_entry)
            for b, piece in enumerate(pieces):
                across_state = jnp.concatenate([before[b], after[b]], axis=1)
                o = inner[b] + dot(
                    jnp.concatenate([piece.qg, piece.qh], axis=1), across_state, NT
                )
                o_ref[b] = o
                mixed = o * lax.rsqrt(jnp.mean(o * o, axis=1, keepdims=True) + EPSILON)
                rows_ref[pl.ds(b * BLOCK, BLOCK), :] = heads_on_lanes(mixed).astype(BF16)

    act_all = act[...].reshape(DEPTH * CHUNK, hidden)
    for n in range(RING):
        rows = inbound[n].reshape(DEPTH * CHUNK, quarter)
        down_grad_ref[:, n * quarter : (n + 1) * quarter] = dot(act_all, rows, TN).astype(BF16)

    for i in range(1, DEPTH):
        send_back(i, True).wait_recv()
    moved = dot(swap[...], ret_in[...].reshape(DEPTH * CHUNK, quarter)).astype(BF16)
    back_out[...] = moved.reshape(back_out.shape)
    for d in PLANE_ORDER:
        plane_out(9, back_out, back_in, d).start()
    back_in[p] = back_out[p]
    deltas = delta[...].reshape(DEPTH * CHUNK, 2 * hidden)
    for n in range(RING):
        both_grads = dot(x[:, n * quarter : (n + 1) * quarter], deltas, TN)
        rows = pl.ds(n * quarter, quarter)
        gate_grad_ref[rows, :] = both_grads[:, :hidden].astype(BF16)
        up_grad_ref[rows, :] = both_grads[:, hidden:].astype(BF16)
    for d in PLANE_ORDER:
        plane_in(9, back_out, back_in, d).wait_recv()
    moe_grad = dot(chosen[...], back_in[...].reshape(DEPTH * CHUNK, quarter), TN)
    stream[t] = (own[...].astype(F32) + moe_grad).astype(BF16)

    tokens = own.shape[0]

    def stream_spread(arriving=False):
        a, b = (left, right) if arriving else (t, t)
        return (
            remote(stream.at[a], stream.at[a], sems(0, 0), {"tp": right}),
            remote(stream.at[b], stream.at[b], sems(1, 0), {"tp": left}),
        )

    def stream_pass(arriving=False):
        top, low = pl.ds(0, tokens // 2), pl.ds(tokens // 2, tokens // 2)
        a, b = (across, across) if arriving else (left, right)
        return (
            remote(stream.at[a, top], stream.at[a, top], sems(8, 0), {"tp": right}),
            remote(stream.at[b, low], stream.at[b, low], sems(9, 0), {"tp": left}),
        )

    for copy in stream_spread():
        copy.start()
    for copy, onward in zip(stream_spread(True), stream_pass()):
        copy.wait_recv()
        onward.start()
    for copy in stream_pass(True):
        copy.wait_recv()
    for n in range(RING):
        stream_ref[:, n * quarter : (n + 1) * quarter] = stream[n]

    for d in PLANE_ORDER:
        plane_out(0, out_plane, in_plane, d).wait_send()
        plane_out(9, back_out, back_in, d).wait_send()
    for i in range(DEPTH):
        if i > 0:
            depth_out(i).wait_send()
            send_back(i).wait_send()
        for copy in (*spread(i), pass_on(i), send_hop(i), send_both(i), send_plain(i)):
            copy.wait_send()
    for copy in (*stream_spread(), *stream_pass()):
        copy.wait_send()


def backward_kernel(
    stream, out_proj, q, k, v, fd, bd, o_ref, entry_ref, dq_ref, dk_ref, dv_ref, *scratch
):
    barrier, count = greet(8, 8)
    pieces = [Piece(b, q, k, v, fd, bd) for b in range(3)]
    mixed_grad = jnp.dot(stream[...], out_proj[...], preferred_element_type=F32)
    c, d = jnp.zeros((DV, 128), F32), jnp.zeros((DV, 128), F32)
    for b, piece in enumerate(pieces):
        o = o_ref[b]
        inv = lax.rsqrt(jnp.mean(o * o, axis=1, keepdims=True) + EPSILON)
        mixed = o * inv
        mg = heads_on_rows(mixed_grad[b * BLOCK : (b + 1) * BLOCK, :])
        piece.do = (inv * (mg - mixed * jnp.mean(mg * mixed, axis=1, keepdims=True))).astype(BF16)
        piece.entries()
        piece.back_f = dot(piece.do, piece.qg, TN)
        piece.back_b = dot(piece.do, piece.qh, TN)
    for piece in pieces:
        c = c * jnp.exp(piece.first) + piece.back_b
    for piece in reversed(pieces):
        d = d * jnp.exp(piece.last) + piece.back_f
    log_f = sum(piece.last for piece in pieces)
    log_b = sum(piece.first for piece in pieces)
    pl.semaphore_wait(barrier, count)
    carry = Carry(scratch)
    carry.start((c, d), (log_b, log_f))
    inclusive, strict = masks()
    for piece in pieces:
        a = piece.scores(inclusive, strict)
        da = dot(piece.do, piece.vs, NT)
        da_f = jnp.where(inclusive, da, 0.0).astype(BF16)
        da_b = jnp.where(strict, da, 0.0).astype(BF16)
        piece.dv = dot(a, piece.do, TN)
        piece.dq = dot(da_f, piece.k_dn_g) * doubled(piece.up_g) + dot(
            da_b, piece.k_dn_h
        ) * doubled(piece.up_h)
        piece.dk = dot(da_f, piece.q_up_g, TN) * doubled(piece.dn_g) + dot(
            da_b, piece.q_up_h, TN
        ) * doubled(piece.dn_h)
    carry.middle()
    for piece in pieces:
        piece.ends()
    before, after, _, _ = both_states(pieces, entry_ref[0], entry_ref[1])
    for b, piece in enumerate(pieces):
        dq = dot(piece.do, jnp.concatenate([before[b], after[b]], axis=1))
        piece.dq = piece.dq + dq[:, :128] * stacked(piece.eg) + dq[:, 128:] * stacked(piece.eh)
        dq_ref[pl.ds(b * BLOCK, BLOCK), :] = (folded(piece.dq) * KEY_CHANNELS**-0.5).astype(BF16)
    carry.last()
    c, d = carry.finish()
    late, early = [None] * 3, [None] * 3
    for b, piece in enumerate(pieces):
        early[b] = c
        c = c * jnp.exp(piece.first) + piece.back_b
    for b in reversed(range(3)):
        late[b] = d
        d = d * jnp.exp(pieces[b].last) + pieces[b].back_f
    for b, piece in enumerate(pieces):
        states = jnp.concatenate([late[b], early[b]], axis=1).astype(BF16)
        dk = dot(piece.vs, states)
        dk = piece.dk + dk[:, :128] * stacked(piece.eg_end) + dk[:, 128:] * stacked(piece.eh_end)
        dv = piece.dv + dot(jnp.concatenate([piece.kg_end, piece.kh_end], axis=1), states, NT)
        rows = pl.ds(b * BLOCK, BLOCK)
        dk_ref[rows, :] = folded(dk).astype(BF16)
        dv_ref[rows, :] = heads_on_lanes(dv).astype(BF16)


def vmem(n):
    return [pl.BlockSpec(memory_space=pltpu.VMEM)] * n


def experts(chosen, weight, layer_grad, slot_tokens, gate, up, down, q, k, v, fd, bd):
    tokens, width = layer_grad.shape
    slots = slot_tokens.shape[1]
    quarter = width // RING
    hidden = gate.shape[2]
    rows = (DEPTH, CHUNK, quarter)
    anywhere = pl.BlockSpec(memory_space=pl.ANY)
    return pl.pallas_call(
        expert_kernel,
        out_shape=(
            jax.ShapeDtypeStruct((tokens, width), BF16),
            jax.ShapeDtypeStruct((width, hidden), BF16),
            jax.ShapeDtypeStruct((width, hidden), BF16),
            jax.ShapeDtypeStruct((hidden, width), BF16),
            jax.ShapeDtypeStruct((3, 128, DV), F32),
            jax.ShapeDtypeStruct((tokens, 2 * DV), BF16),
            jax.ShapeDtypeStruct((2, DV, 128), F32),
        ),
        in_specs=vmem(2) + [anywhere] * 5 + vmem(5),
        out_specs=tuple(vmem(7)),
        scratch_shapes=[
            pltpu.VMEM((tokens, quarter), BF16),
            pltpu.VMEM((slots, width), BF16),
            pltpu.VMEM((width, 2 * hidden), BF16),
            pltpu.VMEM((hidden, width), BF16),
            pltpu.VMEM((slots, slots), BF16),
            pltpu.VMEM((DEPTH, CHUNK, hidden), BF16),
            pltpu.VMEM((DEPTH, CHUNK, hidden), F32),
            pltpu.VMEM((DEPTH, CHUNK, hidden), F32),
            pltpu.VMEM((DEPTH, CHUNK, 2 * hidden), BF16),
            pltpu.VMEM(rows, BF16),
            pltpu.VMEM(rows, BF16),
            pltpu.VMEM(rows, BF16),
            pltpu.VMEM((RING, *rows), BF16),
            pltpu.VMEM((DEPTH, RING, CHUNK, quarter), BF16),
            *[pltpu.VMEM(rows, BF16)] * 8,
            pltpu.VMEM((RING, tokens, quarter), BF16),
            pltpu.SemaphoreType.DMA((10, DEPTH)),
            pltpu.SemaphoreType.DMA((10, DEPTH)),
            pltpu.SemaphoreType.DMA((5,)),
            *Carry.scratch(),
        ],
        compiler_params=pltpu.CompilerParams(
            collective_id=0, has_side_effects=True, vmem_limit_bytes=60 * 2**20
        ),
        cost_estimate=pl.CostEstimate(
            flops=6 * 10**9, bytes_accessed=10 * 2**20, transcendentals=0
        ),
        name="experts",
    )(chosen, weight, layer_grad, slot_tokens, gate, up, down, q, k, v, fd, bd)


def attention_backward(stream, out_proj, q, k, v, fd, bd, o, entry):
    tokens = q.shape[0]
    return pl.pallas_call(
        backward_kernel,
        out_shape=(
            jax.ShapeDtypeStruct((tokens, 128), BF16),
            jax.ShapeDtypeStruct((tokens, 128), BF16),
            jax.ShapeDtypeStruct((tokens, 2 * DV), BF16),
        ),
        in_specs=vmem(9),
        out_specs=tuple(vmem(3)),
        scratch_shapes=Carry.scratch(),
        compiler_params=pltpu.CompilerParams(collective_id=1, has_side_effects=True),
        cost_estimate=pl.CostEstimate(
            flops=10**9, bytes_accessed=2**21, transcendentals=0
        ),
        name="attention_backward",
    )(stream, out_proj, q, k, v, fd, bd, o, entry)


def slot_choice(routes, weights, experts, slots):
    tokens = routes.shape[0]
    ids = routes.reshape(-1)
    members = (ids[:, None] == jnp.arange(experts, dtype=jnp.int32)[None, :]).astype(BF16)
    earlier = jnp.tril(jnp.ones((2 * tokens, 2 * tokens), BF16), -1)
    before = jnp.dot(earlier, members, preferred_element_type=F32)
    ranks = jnp.sum(before * members.astype(F32), axis=1).astype(jnp.int32)
    target = jnp.where(ranks < CAP, ids * CAP + ranks, -1).reshape(tokens, 2)
    row = jnp.arange(slots, dtype=jnp.int32)
    expert = (row // CAP) % DEPTH * PLANES + row // CHUNK
    slot = (expert * CAP + row % CAP)[:, None]
    first = slot == target[:, 0][None, :]
    second = slot == target[:, 1][None, :]
    chosen = (first | second).astype(BF16)
    weight = jnp.sum(
        jnp.where(first, weights[:, 0][None, :], 0.0)
        + jnp.where(second, weights[:, 1][None, :], 0.0),
        axis=1,
        keepdims=True,
    )
    return chosen, weight


def on_device(
    layer_grad,
    routes,
    route_weight,
    slot_tokens,
    gate_proj,
    up_proj,
    down_proj,
    out_proj,
    queries,
    keys,
    values,
    fwd_decay,
    bwd_decay,
):
    devices = lax.axis_size(SP)
    slots = slot_tokens.shape[1]
    chosen, weight = slot_choice(routes, route_weight, devices, slots)
    stream_grad, grad_gate, grad_up, grad_down, o, mixed_rows, entry = experts(
        chosen,
        weight,
        layer_grad,
        slot_tokens,
        gate_proj,
        up_proj,
        down_proj,
        queries,
        keys,
        values,
        fwd_decay,
        bwd_decay,
    )
    terms = lax.dot_general(
        stream_grad, mixed_rows, (TN, ((), ())), preferred_element_type=F32
    ).astype(BF16)
    arrived_terms = lax.all_to_all(
        terms.reshape(devices, -1, terms.shape[1]), SP, split_axis=0, concat_axis=0, tiled=True
    )
    proj_grad = arrived_terms.astype(F32).sum(axis=0)
    query_grad, key_grad, value_grad = attention_backward(
        stream_grad, out_proj, queries, keys, values, fwd_decay, bwd_decay, o, entry
    )
    return (
        grad_gate[None],
        grad_up[None],
        grad_down[None],
        proj_grad,
        query_grad,
        key_grad,
        value_grad,
    )


def solution(mesh):
    torus = Mesh(mesh.devices.reshape(8, 4, 2, mesh.shape["tp"]), ("sp_0", "sp_1", "sp_2", "tp"))
    in_specs = (
        P(SP, None),
        P(SP, None),
        P(SP, None),
        P(SP, None, None),
        P(SP, None, "tp"),
        P(SP, None, "tp"),
        P(SP, "tp", None),
        P(None, "tp"),
        P(SP, "tp"),
        P(SP, "tp"),
        P(SP, "tp"),
        P(SP, "tp"),
        P(SP, "tp"),
    )
    out_specs = (
        P(SP, None, "tp"),
        P(SP, None, "tp"),
        P(SP, "tp", None),
        P(SP, "tp"),
        P(SP, "tp"),
        P(SP, "tp"),
        P(SP, "tp"),
    )
    return jax.shard_map(
        on_device, mesh=torus, in_specs=in_specs, out_specs=out_specs, check_vma=False
    )
```

```python
import jax
import jax.numpy as jnp
from jax import lax
from jax.experimental import pallas as pl
from jax.experimental.pallas import tpu as pltpu
from jax.sharding import Mesh
from jax.sharding import PartitionSpec as P

KEY_CHANNELS = 64
DV = 128
BLOCK = 64
SP = ("sp_0", "sp_1", "sp_2")
EPSILON = 1e-06
CAP = 9
F32 = jnp.float32
BF16 = jnp.bfloat16
PIECE = 16
ROWS = PIECE + 8


def dot(a, b, contract=((1,), (0,))):
    return lax.dot_general(
        a.astype(BF16), b.astype(BF16), (contract, ((), ())), preferred_element_type=F32
    )


def dot_exact(a, b):
    return lax.dot_general(
        a,
        b,
        (((1,), (0,)), ((), ())),
        precision=lax.Precision.HIGHEST,
        preferred_element_type=F32,
    )


NT = ((1,), (1,))
TN = ((0,), (0,))


def iota(shape, dim):
    return lax.broadcasted_iota(jnp.int32, shape, dim)


def stacked(x):
    low = iota(x.shape, 1) < KEY_CHANNELS
    zero = jnp.zeros_like(x)
    return jnp.concatenate([jnp.where(low, x, zero), jnp.where(low, zero, x)], axis=0)


def doubled(x):
    return jnp.concatenate([x, x], axis=0)


def folded(x):
    half = x.shape[0] // 2
    return x[:half] + x[half:]


def heads_on_rows(x):
    return jnp.concatenate([x[:, :DV], x[:, DV:]], axis=0)


def heads_on_lanes(x):
    half = x.shape[0] // 2
    return jnp.concatenate([x[:half], x[half:]], axis=1)


def masks():
    shape = (2 * BLOCK, 2 * BLOCK)
    i, j = iota(shape, 0), iota(shape, 1)
    same = (i // BLOCK) == (j // BLOCK)
    return same & (i >= j), same & (i < j)


class Piece:
    def __init__(self, b, q_ref, k_ref, v_ref, fd_ref, bd_ref):
        rows = pl.ds(b * BLOCK, BLOCK)
        shape = (BLOCK, BLOCK)
        lower = (iota(shape, 0) >= iota(shape, 1)).astype(F32)
        upper = (iota(shape, 0) <= iota(shape, 1)).astype(F32)
        self.q = q_ref[rows, :].astype(F32) * KEY_CHANNELS**-0.5
        self.k = k_ref[rows, :].astype(F32)
        self.vs = heads_on_rows(v_ref[rows, :])
        self.g = dot_exact(lower, fd_ref[rows, :])
        self.h = dot_exact(upper, bd_ref[rows, :])
        self.last = self.g[BLOCK - 1 :, :]
        self.first = self.h[:1, :]
        self.mid_g = self.g[BLOCK // 2 - 1 : BLOCK // 2, :]
        self.mid_h = self.h[BLOCK // 2 : BLOCK // 2 + 1, :]

    def ends(self):
        self.eg_end = jnp.exp(self.last - self.g)
        self.eh_end = jnp.exp(self.first - self.h)
        self.kg_end = stacked(self.k * self.eg_end).astype(BF16)
        self.kh_end = stacked(self.k * self.eh_end).astype(BF16)
        self.fresh_f = dot(self.vs, self.kg_end, TN)
        self.fresh_b = dot(self.vs, self.kh_end, TN)

    def entries(self):
        self.eg = jnp.exp(self.g)
        self.eh = jnp.exp(self.h)
        self.qg = stacked(self.q * self.eg).astype(BF16)
        self.qh = stacked(self.q * self.eh).astype(BF16)

    def scores(self, inclusive, strict):
        self.up_g = jnp.exp(self.g - self.mid_g)
        self.dn_g = jnp.exp(self.mid_g - self.g)
        self.up_h = jnp.exp(self.h - self.mid_h)
        self.dn_h = jnp.exp(self.mid_h - self.h)
        self.q_up_g = stacked(self.q * self.up_g).astype(BF16)
        self.k_dn_g = stacked(self.k * self.dn_g).astype(BF16)
        self.q_up_h = stacked(self.q * self.up_h).astype(BF16)
        self.k_dn_h = stacked(self.k * self.dn_h).astype(BF16)
        a_f = jnp.where(inclusive, dot(self.q_up_g, self.k_dn_g, NT), 0.0)
        a_b = jnp.where(strict, dot(self.q_up_h, self.k_dn_h, NT), 0.0)
        return (a_f + a_b).astype(BF16)


def both_states(pieces, forward_entry, backward_entry):
    s, before = forward_entry, []
    for piece in pieces:
        before.append(s)
        s = jnp.exp(piece.last) * s + piece.fresh_f
    r, after = backward_entry, [None] * len(pieces)
    for b in reversed(range(len(pieces))):
        after[b] = r
        r = jnp.exp(pieces[b].first) * r + pieces[b].fresh_b
    return before, after, s, r


def position():
    z, y, c = (lax.axis_index(a) for a in SP)
    return z, y, c, y * 2 + c


def plane_peer(p, d, planes):
    other = lax.rem(p + d, planes)
    return other, {"sp_1": other // 2, "sp_2": lax.rem(other, 2)}


def greet(planes, depth):
    z, _, _, p = position()
    barrier = pltpu.get_barrier_semaphore()
    for d in range(1, planes):
        _, device = plane_peer(p, d, planes)
        pl.semaphore_signal(barrier, 1, device_id=device, device_id_type=pl.DeviceIdType.MESH)
    for d in range(1, depth):
        device = {"sp_0": lax.rem(z + d, depth)}
        pl.semaphore_signal(barrier, 1, device_id=device, device_id_type=pl.DeviceIdType.MESH)
    return barrier, planes + depth - 2


class Carry:
    SCRATCH_PLANES, SCRATCH_DEPTH = 8, 8

    @classmethod
    def scratch(cls):
        n, m = cls.SCRATCH_PLANES, cls.SCRATCH_DEPTH
        return [
            pltpu.VMEM((n, 2, ROWS, 128), F32),
            pltpu.VMEM((n, 2, ROWS, 128), F32),
            pltpu.VMEM((2, ROWS, 128), F32),
            pltpu.VMEM((m, ROWS, 128), F32),
            pltpu.VMEM((n, 2, PIECE, 128), F32),
            pltpu.VMEM((n, 2, PIECE, 128), F32),
            pltpu.SemaphoreType.DMA((n,)),
            pltpu.SemaphoreType.DMA((n,)),
            pltpu.SemaphoreType.DMA((m,)),
            pltpu.SemaphoreType.DMA((m,)),
            pltpu.SemaphoreType.DMA((n,)),
            pltpu.SemaphoreType.DMA((n,)),
        ]

    def __init__(self, refs):
        (
            self.out1,
            self.in1,
            self.out2,
            self.in2,
            self.out3,
            self.in3,
            self.s1,
            self.r1,
            self.s2,
            self.r2,
            self.s3,
            self.r3,
        ) = refs
        self.n, self.m = self.SCRATCH_PLANES, self.SCRATCH_DEPTH
        self.z, _, _, self.p = position()

    def plane_copy(self, out, into, send, recv, d, arriving=False):
        other, device = plane_peer(self.p, d, self.n)
        at = other if arriving else self.p
        return pltpu.make_async_remote_copy(
            src_ref=out.at[other],
            dst_ref=into.at[at],
            send_sem=send.at[other],
            recv_sem=recv.at[at],
            device_id=device,
            device_id_type=pl.DeviceIdType.MESH,
        )

    def start(self, terms, logs):
        for dim in range(2):
            decay = jnp.broadcast_to(logs[dim], (8, 128))
            for j in range(self.n):
                self.out1[j, dim, :PIECE, :] = terms[dim][j * PIECE : (j + 1) * PIECE, :]
                self.out1[j, dim, PIECE:, :] = decay
        for d in range(1, self.n):
            self.plane_copy(self.out1, self.in1, self.s1, self.r1, d).start()
        self.in1[self.p] = self.out1[self.p]

    def middle(self):
        for d in range(1, self.n):
            self.plane_copy(self.out1, self.in1, self.s1, self.r1, d, True).wait_recv()
        zero = jnp.zeros((PIECE, 128), F32)
        none = jnp.zeros((1, 128), F32)
        self.before = [[None] * self.n, [None] * self.n]
        for dim in range(2):
            total, log = zero, none
            for i in range(self.n) if dim == 0 else reversed(range(self.n)):
                self.before[dim][i] = (total, log)
                step = self.in1[i, dim, PIECE : PIECE + 1, :]
                total = total * jnp.exp(step) + self.in1[i, dim, :PIECE, :]
                log = log + step
            self.out2[dim, :PIECE, :] = total
            self.out2[dim, PIECE:, :] = jnp.broadcast_to(log, (8, 128))
        for d in range(1, self.m):
            self.depth_copy(d).start()

    def depth_copy(self, d, arriving=False):
        other = lax.rem(self.z + d, self.m)
        dim = jnp.where(other > self.z, 0, 1)
        at = other if arriving else self.z
        return pltpu.make_async_remote_copy(
            src_ref=self.out2.at[dim],
            dst_ref=self.in2.at[at],
            send_sem=self.s2.at[other],
            recv_sem=self.r2.at[at],
            device_id={"sp_0": other},
            device_id_type=pl.DeviceIdType.MESH,
        )

    def last(self):
        self.in2[self.z] = jnp.zeros((ROWS, 128), F32)
        for d in range(1, self.m):
            self.depth_copy(d, True).wait_recv()
        entry = []
        for dim in range(2):
            total = jnp.zeros((PIECE, 128), F32)
            for i in range(self.m) if dim == 0 else reversed(range(self.m)):
                passed = (i < self.z) if dim == 0 else (i > self.z)
                step = self.in2[i, PIECE : PIECE + 1, :]
                total = jnp.where(passed, total * jnp.exp(step) + self.in2[i, :PIECE, :], total)
            entry.append(total)
        for i in range(self.n):
            for dim in range(2):
                inside, log = self.before[dim][i]
                self.out3[i, dim] = inside + jnp.exp(log) * entry[dim]
        for d in range(1, self.n):
            self.plane_copy(self.out3, self.in3, self.s3, self.r3, d).start()
        self.in3[self.p] = self.out3[self.p]

    def finish(self):
        for d in range(1, self.n):
            self.plane_copy(self.out3, self.in3, self.s3, self.r3, d, True).wait_recv()
        for d in range(1, self.n):
            self.plane_copy(self.out1, self.in1, self.s1, self.r1, d).wait_send()
            self.plane_copy(self.out3, self.in3, self.s3, self.r3, d).wait_send()
        for d in range(1, self.m):
            self.depth_copy(d).wait_send()
        return [self.in3[:, dim].reshape(128, 128) for dim in range(2)]


OFFSETS = (0, 1, 7, 2, 6, 3, 5, 4)
PLANE_ORDER = (2, 6, 3, 7, 4, 5, 1)
PLANES, DEPTH, RING = 8, 8, 4
CHUNK = PLANES * CAP
MESH = pl.DeviceIdType.MESH


def remote(src, dst, sems, device):
    return pltpu.make_async_remote_copy(
        src_ref=src,
        dst_ref=dst,
        send_sem=sems[0],
        recv_sem=sems[1],
        device_id=device,
        device_id_type=MESH,
    )


def swap_matrix(shape):
    i = iota((shape[0], 1), 0)
    a = (i * 911) >> 16
    rest = i - a * CHUNK
    b = (rest * 7282) >> 16
    source = b * CHUNK + a * CAP + (rest - b * CAP)
    return jnp.where(source == iota(shape, 1), 1.0, 0.0).astype(BF16)


def layer_kernel(
    routes,
    route_weight,
    layer_grad,
    slot_tokens,
    gate_proj,
    up_proj,
    down_proj,
    out_proj,
    q,
    k,
    v,
    fd,
    bd,
    gate_grad_ref,
    up_grad_ref,
    down_grad_ref,
    proj_ref,
    dq_ref,
    dk_ref,
    dv_ref,
    own,
    x,
    w_cat,
    w_down,
    w_out,
    choice,
    swap,
    act,
    silu,
    slope,
    delta,
    out_plane,
    in_plane,
    out_depth,
    inbound,
    part,
    hop,
    hopped,
    both,
    plain,
    ret_out,
    ret_in,
    back_out,
    back_in,
    stream,
    terms,
    core_in,
    core_sum,
    row_in,
    row_sum,
    depth_in,
    send,
    recv,
    load,
    *carry_refs,
):
    z, y, c, p = position()
    t = lax.axis_index("tp")
    right, left, across = lax.rem(t + 1, RING), lax.rem(t + 3, RING), lax.rem(t + 2, RING)
    quarter = own.shape[1]
    barrier, count = greet(PLANES, DEPTH)
    for other in (left, right):
        pl.semaphore_signal(barrier, 1, device_id={"tp": other}, device_id_type=MESH)

    columns = pl.ds(pl.multiple_of(t * quarter, quarter), quarter)
    hidden = w_down.shape[0]
    loads = [
        pltpu.make_async_copy(layer_grad.at[:, columns], own, load.at[0]),
        pltpu.make_async_copy(slot_tokens.at[0], x, load.at[1]),
        pltpu.make_async_copy(gate_proj.at[0], w_cat.at[:, pl.ds(0, hidden)], load.at[2]),
        pltpu.make_async_copy(up_proj.at[0], w_cat.at[:, pl.ds(hidden, hidden)], load.at[3]),
        pltpu.make_async_copy(down_proj.at[0], w_down, load.at[4]),
        pltpu.make_async_copy(out_proj, w_out, load.at[5]),
    ]
    for copy in loads:
        copy.start()

    def sems(kind, i):
        return send.at[kind, i], recv.at[kind, i]

    def plane_out(kind, out, into, d):
        other, device = plane_peer(p, d, PLANES)
        return remote(out.at[other], into.at[p], sems(kind, d), device)

    def plane_in(kind, out, into, d):
        other, device = plane_peer(p, PLANES - d, PLANES)
        return remote(out.at[other], into.at[other], sems(kind, d), device)

    tokens = own.shape[0]
    slots = x.shape[0]
    lanes = iota((tokens, 128), 1)
    first = (routes[:, 0:1] == lanes).astype(BF16)
    second = (routes[:, 1:2] == lanes).astype(BF16)
    shape = (tokens, tokens)
    earlier = (iota(shape, 0) > iota(shape, 1)).astype(BF16)
    before = dot(earlier, first + second)
    loads[0].wait()
    mine = own[...].astype(F32)
    weighted = []
    for j, members in enumerate((first, second)):
        named = members.astype(F32)
        rank = jnp.sum((before + first.astype(F32) * j) * named, axis=1, keepdims=True)
        rank = rank.astype(jnp.int32)
        expert = routes[:, j : j + 1]
        row = (expert & (PLANES - 1)) * CHUNK + (expert >> 3) * CAP + rank
        row = jnp.where(rank < CAP, row, -1)
        taken = (row == iota((tokens, slots), 1)).astype(BF16)
        choice[j * tokens : (j + 1) * tokens, :] = taken
        weighted.append((mine * route_weight[:, j : j + 1]).astype(BF16))
    picked = dot(choice[...], jnp.concatenate(weighted, axis=0), TN)
    out_plane[...] = picked.astype(BF16).reshape(out_plane.shape)
    pl.semaphore_wait(barrier, count + 2)
    for d in PLANE_ORDER:
        plane_out(0, out_plane, in_plane, d).start()
    in_plane[p] = out_plane[p]

    pieces = [Piece(b, q, k, v, fd, bd) for b in range(3)]
    for piece in pieces:
        piece.ends()
    zero = jnp.zeros((DV, 128), F32)
    _, _, forward_end, backward_end = both_states(pieces, zero, zero)
    log_f = sum(piece.last for piece in pieces)
    log_b = sum(piece.first for piece in pieces)
    carry = Carry(carry_refs[:12])
    carry.start((forward_end, backward_end), (log_f, log_b))
    swap[...] = swap_matrix(swap.shape)

    def chunk_of(i):
        return lax.rem(z + OFFSETS[i], DEPTH)

    def spread(i, arriving=False):
        at = chunk_of(i)
        a, b = (left, right) if arriving else (t, t)
        return (
            remote(inbound.at[a, at], inbound.at[a, at], sems(2, i), {"tp": right}),
            remote(inbound.at[b, at], inbound.at[b, at], sems(3, i), {"tp": left}),
        )

    def sides(i):
        return (left, right) if i % 2 == 0 else (right, left)

    def pass_on(i, arriving=False):
        source, to = sides(i)
        at, which = chunk_of(i), across if arriving else source
        return remote(inbound.at[which, at], inbound.at[which, at], sems(4, i), {"tp": to})

    def send_hop(i):
        _, to = sides(i)
        return remote(part.at[i, across], hop.at[i], sems(5, i), {"tp": to})

    def send_both(i):
        _, to = sides(i)
        return remote(hopped.at[i], both.at[i], sems(6, i), {"tp": to})

    def send_plain(i):
        to, _ = sides(i)
        return remote(part.at[i, to], plain.at[i], sems(7, i), {"tp": to})

    def send_back(i, arriving=False):
        at = lax.rem(z + DEPTH - OFFSETS[i], DEPTH) if arriving else z
        other = chunk_of(i)
        return remote(ret_out.at[other], ret_in.at[at], sems(8, i), {"sp_0": other})

    def stage_0(i):
        if i > 0:
            at = chunk_of(i)
            remote(out_depth.at[at], inbound.at[t, at], sems(1, i), {"sp_0": at}).wait_recv()
        for copy in spread(i):
            copy.start()

    def stage_1(i):
        for copy in spread(i, True):
            copy.wait_recv()
        pass_on(i).start()

    def stage_2(i):
        at = chunk_of(i)
        pass_on(i, True).wait_recv()
        total = jnp.zeros((CHUNK, hidden), F32)
        for n in range(RING):
            total = total + dot(inbound[n, at], w_down[:, n * quarter : (n + 1) * quarter], NT)
        up_delta = (total * silu[at]).astype(BF16)
        gate_delta = (total * slope[at]).astype(BF16)
        deltas = jnp.concatenate([gate_delta, up_delta], axis=1)
        delta[at] = deltas
        _, to = sides(i)
        for n, which in enumerate((across, sides(i)[0], to, t)):
            rows = pl.ds(pl.multiple_of(which * quarter, quarter), quarter)
            part[i, which] = dot(deltas, w_cat[rows, :], NT).astype(BF16)
            if n == 0:
                send_hop(i).start()
            if n == 1:
                send_plain(i).start()

    def stage_3(i):
        _, to = sides(i)
        send_hop(i).wait_recv()
        hopped[i] = (hop[i].astype(F32) + part[i, to].astype(F32)).astype(BF16)
        send_both(i).start()

    def stage_4(i):
        at = chunk_of(i)
        send_both(i).wait_recv()
        send_plain(i).wait_recv()
        total = part[i, t].astype(F32) + both[i].astype(F32) + plain[i].astype(F32)
        if i == 0:
            ret_in[z] = total.astype(BF16)
        else:
            ret_out[at] = total.astype(BF16)
            send_back(i).start()

    for d in PLANE_ORDER:
        plane_in(0, out_plane, in_plane, d).wait_recv()
    moved = dot(swap[...], in_plane[...].reshape(DEPTH * CHUNK, quarter)).astype(BF16)
    out_depth[...] = moved.reshape(out_depth.shape)

    def depth_out(i):
        other = lax.rem(z + DEPTH - OFFSETS[i], DEPTH)
        return remote(out_depth.at[other], inbound.at[t, z], sems(1, i), {"sp_0": other})

    inbound[t, z] = out_depth[z]
    stage_0(0)
    for i in range(1, DEPTH):
        depth_out(i).start()
    carry.middle()

    for copy in loads[1:4]:
        copy.wait()
    half = x.shape[0] // 2
    for j in range(2):
        rows = pl.ds(j * half, half)
        chunks = pl.ds(j * (DEPTH // 2), DEPTH // 2)
        both_up = jnp.dot(x[rows, :], w_cat[...], preferred_element_type=F32)
        gate, up = both_up[:, :hidden], both_up[:, hidden:]
        sigma = jax.nn.sigmoid(gate)
        s = gate * sigma
        shape = (DEPTH // 2, CHUNK, hidden)
        silu[chunks] = s.reshape(shape)
        act[chunks] = (s * up).astype(BF16).reshape(shape)
        slope[chunks] = (up * sigma * (1.0 + gate * (1.0 - sigma))).reshape(shape)
    loads[4].wait()

    stages = (stage_0, stage_1, stage_2, stage_3, stage_4)
    for n in range(DEPTH + len(stages) - 1):
        for lag, stage in enumerate(stages):
            if 0 <= n - lag < DEPTH and (n > 0 or lag > 0):
                stage(n - lag)
        if n == 2:
            inclusive, strict = masks()
            for piece in pieces:
                piece.a = piece.scores(inclusive, strict)
                piece.inner = dot(piece.a, piece.vs)
                piece.entries()
        if n == 5:
            carry.last()
        if n == 8:
            forward_entry, backward_entry = carry.finish()
            before, after, _, _ = both_states(pieces, forward_entry, backward_entry)
            for b, piece in enumerate(pieces):
                piece.states = jnp.concatenate([before[b], after[b]], axis=1).astype(BF16)
                o = piece.inner + dot(
                    jnp.concatenate([piece.qg, piece.qh], axis=1), piece.states, NT
                )
                piece.inv = lax.rsqrt(jnp.mean(o * o, axis=1, keepdims=True) + EPSILON)
                piece.mixed = o * piece.inv

    act_all = act[...].reshape(DEPTH * CHUNK, hidden)
    for n in range(RING):
        rows = inbound[n].reshape(DEPTH * CHUNK, quarter)
        down_grad_ref[:, n * quarter : (n + 1) * quarter] = dot(act_all, rows, TN).astype(BF16)

    for i in range(1, DEPTH):
        send_back(i, True).wait_recv()
    moved = dot(swap[...], ret_in[...].reshape(DEPTH * CHUNK, quarter)).astype(BF16)
    back_out[...] = moved.reshape(back_out.shape)
    for d in PLANE_ORDER:
        plane_out(9, back_out, back_in, d).start()
    back_in[p] = back_out[p]
    deltas = delta[...].reshape(DEPTH * CHUNK, 2 * hidden)
    for n in range(RING):
        both_grads = dot(x[:, n * quarter : (n + 1) * quarter], deltas, TN)
        rows = pl.ds(n * quarter, quarter)
        gate_grad_ref[rows, :] = both_grads[:, :hidden].astype(BF16)
        up_grad_ref[rows, :] = both_grads[:, hidden:].astype(BF16)
    for d in PLANE_ORDER:
        plane_in(9, back_out, back_in, d).wait_recv()
    taken = choice[:tokens, :] + choice[tokens:, :]
    moe_grad = dot(taken, back_in[...].reshape(DEPTH * CHUNK, quarter))
    stream[t] = (own[...].astype(F32) + moe_grad).astype(BF16)

    low, high = pl.ds(0, tokens // 2), pl.ds(tokens // 2, tokens // 2)

    def ring(kind, which, rows, to):
        return remote(stream.at[which, rows], stream.at[which, rows], sems(kind, 0), {"tp": to})

    def stream_spread():
        return (
            ring(0, t, low, right),
            ring(1, t, high, left),
            ring(2 + 6, t, high, right),
            ring(3 + 6, t, low, left),
        )

    def stream_arrived():
        return (
            ring(0, left, low, right),
            ring(1, right, high, left),
            ring(2 + 6, left, high, right),
            ring(3 + 6, right, low, left),
        )

    def stream_pass(which_low, which_high):
        return (
            remote(
                stream.at[which_low, low], stream.at[which_low, low], sems(10, 0), {"tp": right}
            ),
            remote(
                stream.at[which_high, high], stream.at[which_high, high], sems(11, 0), {"tp": left}
            ),
        )

    for copy in stream_spread():
        copy.start()
    loads[5].wait()

    def share(which):
        rows = pl.ds(pl.multiple_of(which * quarter, quarter), quarter)
        return jnp.dot(stream[which], w_out[rows, :], preferred_element_type=F32)

    mixed_grad = share(t)
    for n, copy in enumerate(stream_arrived()):
        copy.wait_recv()
        if n < 2:
            stream_pass(left, right)[n].start()
    mixed_grad = mixed_grad + share(left) + share(right)
    for copy in stream_pass(across, across):
        copy.wait_recv()
    mixed_grad = mixed_grad + share(across)

    back_c, back_d = jnp.zeros((DV, 128), F32), jnp.zeros((DV, 128), F32)
    for b, piece in enumerate(pieces):
        mg = heads_on_rows(mixed_grad[b * BLOCK : (b + 1) * BLOCK, :])
        mean = jnp.mean(mg * piece.mixed, axis=1, keepdims=True)
        piece.do = (piece.inv * (mg - piece.mixed * mean)).astype(BF16)
        piece.back_f = dot(piece.do, piece.qg, TN)
        piece.back_b = dot(piece.do, piece.qh, TN)
    for piece in pieces:
        back_c = back_c * jnp.exp(piece.first) + piece.back_b
    for piece in reversed(pieces):
        back_d = back_d * jnp.exp(piece.last) + piece.back_f
    carry = Carry(carry_refs[12:])
    carry.start((back_c, back_d), (log_b, log_f))

    rows_of_mixed = jnp.concatenate([heads_on_lanes(piece.mixed) for piece in pieces], axis=0)
    rows_of_mixed = rows_of_mixed.astype(BF16)
    piece_rows = proj_ref.shape[0]
    for n in range(RING):
        term = dot(stream[n], rows_of_mixed, TN).astype(BF16)
        per = term.shape[0] // (piece_rows * PLANES)
        term = term.reshape(per, 4, 2, piece_rows, term.shape[1])
        for cc in range(2):
            for zz in range(per):
                terms[cc, :, n * per + zz] = term[zz, :, cc]

    def core_copy():
        return remote(terms.at[1 - c], core_in, sems(12, 0), {"sp_2": 1 - c})

    def row_copy(d, arriving=False):
        other = lax.rem(y + (4 - d if arriving else d), 4)
        at = other if arriving else y
        return remote(core_sum.at[other], row_in.at[at], sems(12, d), {"sp_1": other})

    def last_copy(d, arriving=False):
        other = lax.rem(z + (DEPTH - d if arriving else d), DEPTH)
        at = other if arriving else z
        return remote(row_sum.at[other], depth_in.at[at], sems(13, d), {"sp_0": other})

    core_copy().start()

    inclusive, strict = masks()
    for piece in pieces:
        da = dot(piece.do, piece.vs, NT)
        da_f = jnp.where(inclusive, da, 0.0).astype(BF16)
        da_b = jnp.where(strict, da, 0.0).astype(BF16)
        piece.dv = dot(piece.a, piece.do, TN)
        piece.dq = dot(da_f, piece.k_dn_g) * doubled(piece.up_g) + dot(
            da_b, piece.k_dn_h
        ) * doubled(piece.up_h)
        piece.dk = dot(da_f, piece.q_up_g, TN) * doubled(piece.dn_g) + dot(
            da_b, piece.q_up_h, TN
        ) * doubled(piece.dn_h)
    carry.middle()
    core_copy().wait_recv()
    core_sum[...] = (terms[c].astype(F32) + core_in[...].astype(F32)).astype(BF16)
    for d in (2, 1, 3):
        row_copy(d).start()
    for b, piece in enumerate(pieces):
        dq = dot(piece.do, piece.states)
        dq = piece.dq + dq[:, :128] * stacked(piece.eg) + dq[:, 128:] * stacked(piece.eh)
        dq_ref[pl.ds(b * BLOCK, BLOCK), :] = (folded(dq) * KEY_CHANNELS**-0.5).astype(BF16)
    carry.last()
    for d in (1, 3, 2):
        row_copy(d, True).wait_recv()
    row_in[y] = core_sum[y]
    total = row_in[0].astype(F32)
    for n in range(1, 4):
        total = total + row_in[n].astype(F32)
    row_sum[...] = total
    for d in (4, 3, 5, 2, 6, 1, 7):
        last_copy(d).start()
    back_c, back_d = carry.finish()
    late, early = [None] * 3, [None] * 3
    for b, piece in enumerate(pieces):
        early[b] = back_c
        back_c = back_c * jnp.exp(piece.first) + piece.back_b
    for b in reversed(range(3)):
        late[b] = back_d
        back_d = back_d * jnp.exp(pieces[b].last) + pieces[b].back_f
    for b, piece in enumerate(pieces):
        states = jnp.concatenate([late[b], early[b]], axis=1).astype(BF16)
        dk = dot(piece.vs, states)
        dk = piece.dk + dk[:, :128] * stacked(piece.eg_end) + dk[:, 128:] * stacked(piece.eh_end)
        dv = piece.dv + dot(jnp.concatenate([piece.kg_end, piece.kh_end], axis=1), states, NT)
        rows = pl.ds(b * BLOCK, BLOCK)
        dk_ref[rows, :] = folded(dk).astype(BF16)
        dv_ref[rows, :] = heads_on_lanes(dv).astype(BF16)
    depth_in[z] = row_sum[z]
    for d in range(1, DEPTH):
        last_copy(d, True).wait_recv()
    total = depth_in[0]
    for n in range(1, DEPTH):
        total = total + depth_in[n]
    proj_ref[...] = total

    for d in PLANE_ORDER:
        plane_out(0, out_plane, in_plane, d).wait_send()
        plane_out(9, back_out, back_in, d).wait_send()
    for i in range(DEPTH):
        if i > 0:
            depth_out(i).wait_send()
            send_back(i).wait_send()
        for copy in (*spread(i), pass_on(i), send_hop(i), send_both(i), send_plain(i)):
            copy.wait_send()
    for copy in (*stream_spread(), *stream_pass(left, right), core_copy()):
        copy.wait_send()
    for d in (1, 2, 3):
        row_copy(d).wait_send()
    for d in range(1, DEPTH):
        last_copy(d).wait_send()


def vmem(n):
    return [pl.BlockSpec(memory_space=pltpu.VMEM)] * n


def layer(*arrays):
    layer_grad, slot_tokens, gate = arrays[2], arrays[3], arrays[4]
    tokens, width = layer_grad.shape
    slots = slot_tokens.shape[1]
    quarter = width // RING
    hidden = gate.shape[2]
    out_columns = arrays[7].shape[1]
    piece_rows = width // (DEPTH * PLANES)
    rows = (DEPTH, CHUNK, quarter)
    anywhere = pl.BlockSpec(memory_space=pl.ANY)
    return pl.pallas_call(
        layer_kernel,
        out_shape=(
            jax.ShapeDtypeStruct((width, hidden), BF16),
            jax.ShapeDtypeStruct((width, hidden), BF16),
            jax.ShapeDtypeStruct((hidden, width), BF16),
            jax.ShapeDtypeStruct((piece_rows, out_columns), F32),
            jax.ShapeDtypeStruct((tokens, 128), BF16),
            jax.ShapeDtypeStruct((tokens, 128), BF16),
            jax.ShapeDtypeStruct((tokens, 2 * DV), BF16),
        ),
        in_specs=vmem(2) + [anywhere] * 6 + vmem(5),
        out_specs=tuple(vmem(7)),
        scratch_shapes=[
            pltpu.VMEM((tokens, quarter), BF16),
            pltpu.VMEM((slots, width), BF16),
            pltpu.VMEM((width, 2 * hidden), BF16),
            pltpu.VMEM((hidden, width), BF16),
            pltpu.VMEM((width, out_columns), BF16),
            pltpu.VMEM((2 * tokens, slots), BF16),
            pltpu.VMEM((slots, slots), BF16),
            pltpu.VMEM((DEPTH, CHUNK, hidden), BF16),
            pltpu.VMEM((DEPTH, CHUNK, hidden), F32),
            pltpu.VMEM((DEPTH, CHUNK, hidden), F32),
            pltpu.VMEM((DEPTH, CHUNK, 2 * hidden), BF16),
            pltpu.VMEM(rows, BF16),
            pltpu.VMEM(rows, BF16),
            pltpu.VMEM(rows, BF16),
            pltpu.VMEM((RING, *rows), BF16),
            pltpu.VMEM((DEPTH, RING, CHUNK, quarter), BF16),
            *[pltpu.VMEM(rows, BF16)] * 8,
            pltpu.VMEM((RING, tokens, quarter), BF16),
            pltpu.VMEM((2, 4, DEPTH, piece_rows, out_columns), BF16),
            pltpu.VMEM((4, DEPTH, piece_rows, out_columns), BF16),
            pltpu.VMEM((4, DEPTH, piece_rows, out_columns), BF16),
            pltpu.VMEM((4, DEPTH, piece_rows, out_columns), BF16),
            pltpu.VMEM((DEPTH, piece_rows, out_columns), F32),
            pltpu.VMEM((DEPTH, piece_rows, out_columns), F32),
            pltpu.SemaphoreType.DMA((14, DEPTH)),
            pltpu.SemaphoreType.DMA((14, DEPTH)),
            pltpu.SemaphoreType.DMA((6,)),
            *Carry.scratch(),
            *Carry.scratch(),
        ],
        compiler_params=pltpu.CompilerParams(
            collective_id=0, has_side_effects=True, vmem_limit_bytes=60 * 2**20
        ),
        cost_estimate=pl.CostEstimate(
            flops=8 * 10**9, bytes_accessed=12 * 2**20, transcendentals=0
        ),
        name="layer",
    )(*arrays)


def on_device(layer_grad, routes, route_weight, *arrays):
    gate, up, down, proj, query, key, value = layer(routes, route_weight, layer_grad, *arrays)
    return gate[None], up[None], down[None], proj, query, key, value


def solution(mesh):
    torus = Mesh(mesh.devices.reshape(8, 4, 2, mesh.shape["tp"]), ("sp_0", "sp_1", "sp_2", "tp"))
    in_specs = (
        P(SP, None),
        P(SP, None),
        P(SP, None),
        P(SP, None, None),
        P(SP, None, "tp"),
        P(SP, None, "tp"),
        P(SP, "tp", None),
        P(None, "tp"),
        P(SP, "tp"),
        P(SP, "tp"),
        P(SP, "tp"),
        P(SP, "tp"),
        P(SP, "tp"),
    )
    out_specs = (
        P(SP, None, "tp"),
        P(SP, None, "tp"),
        P(SP, "tp", None),
        P(SP, "tp"),
        P(SP, "tp"),
        P(SP, "tp"),
        P(SP, "tp"),
    )
    return jax.shard_map(
        on_device, mesh=torus, in_specs=in_specs, out_specs=out_specs, check_vma=False
    )
```

```python
import jax
import jax.numpy as jnp
from jax import lax
from jax.experimental import pallas as pl
from jax.experimental.pallas import tpu as pltpu
from jax.sharding import Mesh
from jax.sharding import PartitionSpec as P

KEY_CHANNELS = 64
DV = 128
BLOCK = 64
SP = ("sp_0", "sp_1", "sp_2")
EPSILON = 1e-06
CAP = 9
F32 = jnp.float32
BF16 = jnp.bfloat16
PIECE = 16
ROWS = PIECE + 8


def dot(a, b, contract=((1,), (0,))):
    return lax.dot_general(
        a.astype(BF16), b.astype(BF16), (contract, ((), ())), preferred_element_type=F32
    )


def dot_exact(a, b):
    return lax.dot_general(
        a,
        b,
        (((1,), (0,)), ((), ())),
        precision=lax.Precision.HIGHEST,
        preferred_element_type=F32,
    )


NT = ((1,), (1,))
TN = ((0,), (0,))


def iota(shape, dim):
    return lax.broadcasted_iota(jnp.int32, shape, dim)


def stacked(x):
    low = iota(x.shape, 1) < KEY_CHANNELS
    zero = jnp.zeros_like(x)
    return jnp.concatenate([jnp.where(low, x, zero), jnp.where(low, zero, x)], axis=0)


def doubled(x):
    return jnp.concatenate([x, x], axis=0)


def folded(x):
    half = x.shape[0] // 2
    return x[:half] + x[half:]


def heads_on_rows(x):
    return jnp.concatenate([x[:, :DV], x[:, DV:]], axis=0)


def heads_on_lanes(x):
    half = x.shape[0] // 2
    return jnp.concatenate([x[:half], x[half:]], axis=1)


def masks():
    shape = (2 * BLOCK, 2 * BLOCK)
    i, j = iota(shape, 0), iota(shape, 1)
    same = (i // BLOCK) == (j // BLOCK)
    return same & (i >= j), same & (i < j)


class Piece:
    def __init__(self, b, q_ref, k_ref, v_ref, fd_ref, bd_ref):
        rows = pl.ds(b * BLOCK, BLOCK)
        shape = (BLOCK, BLOCK)
        lower = (iota(shape, 0) >= iota(shape, 1)).astype(F32)
        upper = (iota(shape, 0) <= iota(shape, 1)).astype(F32)
        self.q = q_ref[rows, :].astype(F32) * KEY_CHANNELS**-0.5
        self.k = k_ref[rows, :].astype(F32)
        self.vs = heads_on_rows(v_ref[rows, :])
        self.g = dot_exact(lower, fd_ref[rows, :])
        self.h = dot_exact(upper, bd_ref[rows, :])
        self.last = self.g[BLOCK - 1 :, :]
        self.first = self.h[:1, :]
        self.mid_g = self.g[BLOCK // 2 - 1 : BLOCK // 2, :]
        self.mid_h = self.h[BLOCK // 2 : BLOCK // 2 + 1, :]

    def ends(self):
        self.eg_end = jnp.exp(self.last - self.g)
        self.eh_end = jnp.exp(self.first - self.h)
        self.kg_end = stacked(self.k * self.eg_end).astype(BF16)
        self.kh_end = stacked(self.k * self.eh_end).astype(BF16)
        self.fresh_f = dot(self.vs, self.kg_end, TN)
        self.fresh_b = dot(self.vs, self.kh_end, TN)

    def entries(self):
        self.eg = jnp.exp(self.g)
        self.eh = jnp.exp(self.h)
        self.qg = stacked(self.q * self.eg).astype(BF16)
        self.qh = stacked(self.q * self.eh).astype(BF16)

    def scores(self, inclusive, strict):
        self.up_g = jnp.exp(self.g - self.mid_g)
        self.dn_g = jnp.exp(self.mid_g - self.g)
        self.up_h = jnp.exp(self.h - self.mid_h)
        self.dn_h = jnp.exp(self.mid_h - self.h)
        self.q_up_g = stacked(self.q * self.up_g).astype(BF16)
        self.k_dn_g = stacked(self.k * self.dn_g).astype(BF16)
        self.q_up_h = stacked(self.q * self.up_h).astype(BF16)
        self.k_dn_h = stacked(self.k * self.dn_h).astype(BF16)
        a_f = jnp.where(inclusive, dot(self.q_up_g, self.k_dn_g, NT), 0.0)
        a_b = jnp.where(strict, dot(self.q_up_h, self.k_dn_h, NT), 0.0)
        return (a_f + a_b).astype(BF16)


def both_states(pieces, forward_entry, backward_entry):
    s, before = forward_entry, []
    for piece in pieces:
        before.append(s)
        s = jnp.exp(piece.last) * s + piece.fresh_f
    r, after = backward_entry, [None] * len(pieces)
    for b in reversed(range(len(pieces))):
        after[b] = r
        r = jnp.exp(pieces[b].first) * r + pieces[b].fresh_b
    return before, after, s, r


def position():
    z, y, c = (lax.axis_index(a) for a in SP)
    return z, y, c, y * 2 + c


def plane_peer(p, d, planes):
    other = lax.rem(p + d, planes)
    return other, {"sp_1": other // 2, "sp_2": lax.rem(other, 2)}


def greet(planes, depth):
    z, _, _, p = position()
    barrier = pltpu.get_barrier_semaphore()
    for d in range(1, planes):
        _, device = plane_peer(p, d, planes)
        pl.semaphore_signal(barrier, 1, device_id=device, device_id_type=pl.DeviceIdType.MESH)
    for d in range(1, depth):
        device = {"sp_0": lax.rem(z + d, depth)}
        pl.semaphore_signal(barrier, 1, device_id=device, device_id_type=pl.DeviceIdType.MESH)
    return barrier, planes + depth - 2


class Carry:
    SCRATCH_PLANES, SCRATCH_DEPTH = 8, 8

    @classmethod
    def scratch(cls):
        n, m = cls.SCRATCH_PLANES, cls.SCRATCH_DEPTH
        return [
            pltpu.VMEM((n, 2, ROWS, 128), F32),
            pltpu.VMEM((n, 2, ROWS, 128), F32),
            pltpu.VMEM((2, ROWS, 128), F32),
            pltpu.VMEM((m, ROWS, 128), F32),
            pltpu.VMEM((n, 2, PIECE, 128), F32),
            pltpu.VMEM((n, 2, PIECE, 128), F32),
            pltpu.SemaphoreType.DMA((n,)),
            pltpu.SemaphoreType.DMA((n,)),
            pltpu.SemaphoreType.DMA((m,)),
            pltpu.SemaphoreType.DMA((m,)),
            pltpu.SemaphoreType.DMA((n,)),
            pltpu.SemaphoreType.DMA((n,)),
        ]

    def __init__(self, refs):
        (
            self.out1,
            self.in1,
            self.out2,
            self.in2,
            self.out3,
            self.in3,
            self.s1,
            self.r1,
            self.s2,
            self.r2,
            self.s3,
            self.r3,
        ) = refs
        self.n, self.m = self.SCRATCH_PLANES, self.SCRATCH_DEPTH
        self.z, _, _, self.p = position()

    def plane_copy(self, out, into, send, recv, d, arriving=False):
        other, device = plane_peer(self.p, d, self.n)
        at = other if arriving else self.p
        return pltpu.make_async_remote_copy(
            src_ref=out.at[other],
            dst_ref=into.at[at],
            send_sem=send.at[other],
            recv_sem=recv.at[at],
            device_id=device,
            device_id_type=pl.DeviceIdType.MESH,
        )

    def start(self, terms, logs):
        for dim in range(2):
            decay = jnp.broadcast_to(logs[dim], (8, 128))
            for j in range(self.n):
                self.out1[j, dim, :PIECE, :] = terms[dim][j * PIECE : (j + 1) * PIECE, :]
                self.out1[j, dim, PIECE:, :] = decay
        for d in range(1, self.n):
            self.plane_copy(self.out1, self.in1, self.s1, self.r1, d).start()
        self.in1[self.p] = self.out1[self.p]

    def middle(self):
        for d in range(1, self.n):
            self.plane_copy(self.out1, self.in1, self.s1, self.r1, d, True).wait_recv()
        zero = jnp.zeros((PIECE, 128), F32)
        none = jnp.zeros((1, 128), F32)
        self.before = [[None] * self.n, [None] * self.n]
        for dim in range(2):
            total, log = zero, none
            for i in range(self.n) if dim == 0 else reversed(range(self.n)):
                self.before[dim][i] = (total, log)
                step = self.in1[i, dim, PIECE : PIECE + 1, :]
                total = total * jnp.exp(step) + self.in1[i, dim, :PIECE, :]
                log = log + step
            self.out2[dim, :PIECE, :] = total
            self.out2[dim, PIECE:, :] = jnp.broadcast_to(log, (8, 128))
        for d in range(1, self.m):
            self.depth_copy(d).start()

    def depth_copy(self, d, arriving=False):
        other = lax.rem(self.z + d, self.m)
        dim = jnp.where(other > self.z, 0, 1)
        at = other if arriving else self.z
        return pltpu.make_async_remote_copy(
            src_ref=self.out2.at[dim],
            dst_ref=self.in2.at[at],
            send_sem=self.s2.at[other],
            recv_sem=self.r2.at[at],
            device_id={"sp_0": other},
            device_id_type=pl.DeviceIdType.MESH,
        )

    def last(self):
        self.in2[self.z] = jnp.zeros((ROWS, 128), F32)
        for d in range(1, self.m):
            self.depth_copy(d, True).wait_recv()
        entry = []
        for dim in range(2):
            total = jnp.zeros((PIECE, 128), F32)
            for i in range(self.m) if dim == 0 else reversed(range(self.m)):
                passed = (i < self.z) if dim == 0 else (i > self.z)
                step = self.in2[i, PIECE : PIECE + 1, :]
                total = jnp.where(passed, total * jnp.exp(step) + self.in2[i, :PIECE, :], total)
            entry.append(total)
        for i in range(self.n):
            for dim in range(2):
                inside, log = self.before[dim][i]
                self.out3[i, dim] = inside + jnp.exp(log) * entry[dim]
        for d in range(1, self.n):
            self.plane_copy(self.out3, self.in3, self.s3, self.r3, d).start()
        self.in3[self.p] = self.out3[self.p]

    def finish(self):
        for d in range(1, self.n):
            self.plane_copy(self.out3, self.in3, self.s3, self.r3, d, True).wait_recv()
        for d in range(1, self.n):
            self.plane_copy(self.out1, self.in1, self.s1, self.r1, d).wait_send()
            self.plane_copy(self.out3, self.in3, self.s3, self.r3, d).wait_send()
        for d in range(1, self.m):
            self.depth_copy(d).wait_send()
        return [self.in3[:, dim].reshape(128, 128) for dim in range(2)]


OFFSETS = (0, 1, 7, 2, 6, 3, 5, 4)
PLANE_ORDER = (2, 6, 3, 7, 4, 5, 1)
PLANES, DEPTH, RING = 8, 8, 4
CHUNK = PLANES * CAP
MESH = pl.DeviceIdType.MESH


def remote(src, dst, sems, device):
    return pltpu.make_async_remote_copy(
        src_ref=src,
        dst_ref=dst,
        send_sem=sems[0],
        recv_sem=sems[1],
        device_id=device,
        device_id_type=MESH,
    )


def swap_matrix(shape):
    i = iota((shape[0], 1), 0)
    a = (i * 911) >> 16
    rest = i - a * CHUNK
    b = (rest * 7282) >> 16
    source = b * CHUNK + a * CAP + (rest - b * CAP)
    return jnp.where(source == iota(shape, 1), 1.0, 0.0).astype(BF16)


def layer_kernel(
    routes,
    route_weight,
    layer_grad,
    slot_tokens,
    gate_proj,
    up_proj,
    down_proj,
    out_proj,
    q_hbm,
    k_hbm,
    v_hbm,
    fd_hbm,
    bd_hbm,
    gate_grad_ref,
    up_grad_ref,
    down_grad_ref,
    proj_ref,
    dq_ref,
    dk_ref,
    dv_ref,
    q,
    k,
    v,
    fd,
    bd,
    own,
    x,
    w_cat,
    w_down,
    w_out,
    choice,
    choice_t,
    swap,
    act,
    silu,
    slope,
    delta,
    out_plane,
    in_plane,
    out_depth,
    inbound,
    part,
    hop,
    hopped,
    both,
    plain,
    ret_out,
    ret_in,
    back_out,
    back_in,
    stream,
    terms,
    core_in,
    core_sum,
    row_in,
    row_sum,
    depth_in,
    send,
    recv,
    load,
    *carry_refs,
):
    z, y, c, p = position()
    t = lax.axis_index("tp")
    right, left, across = lax.rem(t + 1, RING), lax.rem(t + 3, RING), lax.rem(t + 2, RING)
    quarter = own.shape[1]
    barrier, count = greet(PLANES, DEPTH)
    for other in (left, right):
        pl.semaphore_signal(barrier, 1, device_id={"tp": other}, device_id_type=MESH)

    columns = pl.ds(pl.multiple_of(t * quarter, quarter), quarter)
    hidden = w_down.shape[0]
    loads = [
        pltpu.make_async_copy(layer_grad.at[:, columns], own, load.at[0]),
        pltpu.make_async_copy(slot_tokens.at[0], x, load.at[1]),
        pltpu.make_async_copy(gate_proj.at[0], w_cat.at[:, pl.ds(0, hidden)], load.at[2]),
        pltpu.make_async_copy(up_proj.at[0], w_cat.at[:, pl.ds(hidden, hidden)], load.at[3]),
        pltpu.make_async_copy(down_proj.at[0], w_down, load.at[4]),
        pltpu.make_async_copy(out_proj, w_out, load.at[5]),
    ]
    for n, (source, to) in enumerate(
        ((q_hbm, q), (k_hbm, k), (v_hbm, v), (fd_hbm, fd), (bd_hbm, bd))
    ):
        loads.append(pltpu.make_async_copy(source, to, load.at[6 + n]))
    for copy in (loads[0], *loads[6:], *loads[1:6]):
        copy.start()

    def sems(kind, i):
        return send.at[kind, i], recv.at[kind, i]

    def plane_out(kind, out, into, d):
        other, device = plane_peer(p, d, PLANES)
        return remote(out.at[other], into.at[p], sems(kind, d), device)

    def plane_in(kind, out, into, d):
        other, device = plane_peer(p, PLANES - d, PLANES)
        return remote(out.at[other], into.at[other], sems(kind, d), device)

    tokens = own.shape[0]
    slots = x.shape[0]
    names = iota((128, tokens), 0)
    members = [(routes[j : j + 1, :] == names).astype(F32) for j in range(2)]
    shape = (tokens, tokens)
    later = (iota(shape, 0) < iota(shape, 1)).astype(BF16)
    before = dot(members[0] + members[1], later)
    scale = jnp.zeros((slots, 1), F32)
    chosen = jnp.zeros((slots, tokens), F32)
    for j in range(2):
        rank = jnp.sum((before + members[0] * j) * members[j], axis=0, keepdims=True)
        rank = rank.astype(jnp.int32)
        expert = routes[j : j + 1, :]
        row = (expert & (PLANES - 1)) * CHUNK + (expert >> 3) * CAP + rank
        row = jnp.where(rank < CAP, row, -1)
        taken = row == iota((slots, tokens), 0)
        chosen = jnp.where(taken, 1.0, chosen)
        given = jnp.where(taken, route_weight[j : j + 1, :], 0.0)
        scale = scale + jnp.sum(given, axis=1, keepdims=True)
    choice[...] = chosen.astype(BF16)
    loads[0].wait()
    picked = dot(choice[...], own[...]) * scale
    out_plane[...] = picked.astype(BF16).reshape(out_plane.shape)
    pl.semaphore_wait(barrier, count + 2)
    for d in PLANE_ORDER:
        plane_out(0, out_plane, in_plane, d).start()
    in_plane[p] = out_plane[p]

    for copy in loads[6:]:
        copy.wait()
    pieces = [Piece(b, q, k, v, fd, bd) for b in range(3)]
    for piece in pieces:
        piece.ends()
    zero = jnp.zeros((DV, 128), F32)
    _, _, forward_end, backward_end = both_states(pieces, zero, zero)
    log_f = sum(piece.last for piece in pieces)
    log_b = sum(piece.first for piece in pieces)
    carry = Carry(carry_refs[:12])
    carry.start((forward_end, backward_end), (log_f, log_b))
    swap[...] = swap_matrix(swap.shape)
    choice_t[...] = choice[...].T

    def chunk_of(i):
        return lax.rem(z + OFFSETS[i], DEPTH)

    def spread(i, arriving=False):
        at = chunk_of(i)
        a, b = (left, right) if arriving else (t, t)
        return (
            remote(inbound.at[a, at], inbound.at[a, at], sems(2, i), {"tp": right}),
            remote(inbound.at[b, at], inbound.at[b, at], sems(3, i), {"tp": left}),
        )

    def sides(i):
        return (left, right) if i % 2 == 0 else (right, left)

    def pass_on(i, arriving=False):
        source, to = sides(i)
        at, which = chunk_of(i), across if arriving else source
        return remote(inbound.at[which, at], inbound.at[which, at], sems(4, i), {"tp": to})

    def send_hop(i):
        _, to = sides(i)
        return remote(part.at[i, across], hop.at[i], sems(5, i), {"tp": to})

    def send_both(i):
        _, to = sides(i)
        return remote(hopped.at[i], both.at[i], sems(6, i), {"tp": to})

    def send_plain(i):
        to, _ = sides(i)
        return remote(part.at[i, to], plain.at[i], sems(7, i), {"tp": to})

    def send_back(i, arriving=False):
        at = lax.rem(z + DEPTH - OFFSETS[i], DEPTH) if arriving else z
        other = chunk_of(i)
        return remote(ret_out.at[other], ret_in.at[at], sems(8, i), {"sp_0": other})

    def stage_0(i):
        if i > 0:
            at = chunk_of(i)
            remote(out_depth.at[at], inbound.at[t, at], sems(1, i), {"sp_0": at}).wait_recv()
        for copy in spread(i):
            copy.start()

    def stage_1(i):
        for copy in spread(i, True):
            copy.wait_recv()
        pass_on(i).start()

    def stage_2(i):
        at = chunk_of(i)
        pass_on(i, True).wait_recv()
        total = jnp.zeros((CHUNK, hidden), F32)
        for n in range(RING):
            total = total + dot(inbound[n, at], w_down[:, n * quarter : (n + 1) * quarter], NT)
        up_delta = (total * silu[at]).astype(BF16)
        gate_delta = (total * slope[at]).astype(BF16)
        deltas = jnp.concatenate([gate_delta, up_delta], axis=1)
        delta[at] = deltas
        _, to = sides(i)
        for n, which in enumerate((across, sides(i)[0], to, t)):
            rows = pl.ds(pl.multiple_of(which * quarter, quarter), quarter)
            part[i, which] = dot(deltas, w_cat[rows, :], NT).astype(BF16)
            if n == 0:
                send_hop(i).start()
            if n == 1:
                send_plain(i).start()

    def stage_3(i):
        _, to = sides(i)
        send_hop(i).wait_recv()
        hopped[i] = (hop[i].astype(F32) + part[i, to].astype(F32)).astype(BF16)
        send_both(i).start()

    def stage_4(i):
        at = chunk_of(i)
        send_both(i).wait_recv()
        send_plain(i).wait_recv()
        total = part[i, t].astype(F32) + both[i].astype(F32) + plain[i].astype(F32)
        if i == 0:
            ret_in[z] = total.astype(BF16)
        else:
            ret_out[at] = total.astype(BF16)
            send_back(i).start()

    for d in PLANE_ORDER:
        plane_in(0, out_plane, in_plane, d).wait_recv()
    moved = dot(swap[...], in_plane[...].reshape(DEPTH * CHUNK, quarter)).astype(BF16)
    out_depth[...] = moved.reshape(out_depth.shape)

    def depth_out(i):
        other = lax.rem(z + DEPTH - OFFSETS[i], DEPTH)
        return remote(out_depth.at[other], inbound.at[t, z], sems(1, i), {"sp_0": other})

    inbound[t, z] = out_depth[z]
    stage_0(0)
    for i in range(1, DEPTH):
        depth_out(i).start()
    carry.middle()

    for copy in loads[1:4]:
        copy.wait()
    half = x.shape[0] // 2
    for j in range(2):
        rows = pl.ds(j * half, half)
        chunks = pl.ds(j * (DEPTH // 2), DEPTH // 2)
        both_up = jnp.dot(x[rows, :], w_cat[...], preferred_element_type=F32)
        gate, up = both_up[:, :hidden], both_up[:, hidden:]
        sigma = jax.nn.sigmoid(gate)
        s = gate * sigma
        shape = (DEPTH // 2, CHUNK, hidden)
        silu[chunks] = s.reshape(shape)
        act[chunks] = (s * up).astype(BF16).reshape(shape)
        slope[chunks] = (up * sigma * (1.0 + gate * (1.0 - sigma))).reshape(shape)
    loads[4].wait()

    stages = (stage_0, stage_1, stage_2, stage_3, stage_4)
    for n in range(DEPTH + len(stages) - 1):
        for lag, stage in enumerate(stages):
            if 0 <= n - lag < DEPTH and (n > 0 or lag > 0):
                stage(n - lag)
        if n == 2:
            inclusive, strict = masks()
            for piece in pieces:
                piece.a = piece.scores(inclusive, strict)
                piece.inner = dot(piece.a, piece.vs)
                piece.entries()
        if n == 5:
            carry.last()
        if n == 8:
            forward_entry, backward_entry = carry.finish()
            before, after, _, _ = both_states(pieces, forward_entry, backward_entry)
            for b, piece in enumerate(pieces):
                piece.states = jnp.concatenate([before[b], after[b]], axis=1).astype(BF16)
                o = piece.inner + dot(
                    jnp.concatenate([piece.qg, piece.qh], axis=1), piece.states, NT
                )
                piece.inv = lax.rsqrt(jnp.mean(o * o, axis=1, keepdims=True) + EPSILON)
                piece.mixed = o * piece.inv

    act_all = act[...].reshape(DEPTH * CHUNK, hidden)
    for n in range(RING):
        rows = inbound[n].reshape(DEPTH * CHUNK, quarter)
        down_grad_ref[:, n * quarter : (n + 1) * quarter] = dot(act_all, rows, TN).astype(BF16)

    for i in range(1, DEPTH):
        send_back(i, True).wait_recv()
    moved = dot(swap[...], ret_in[...].reshape(DEPTH * CHUNK, quarter)).astype(BF16)
    back_out[...] = moved.reshape(back_out.shape)
    for d in PLANE_ORDER:
        plane_out(9, back_out, back_in, d).start()
    back_in[p] = back_out[p]
    deltas = delta[...].reshape(DEPTH * CHUNK, 2 * hidden)
    for n in range(RING):
        both_grads = dot(x[:, n * quarter : (n + 1) * quarter], deltas, TN)
        rows = pl.ds(n * quarter, quarter)
        gate_grad_ref[rows, :] = both_grads[:, :hidden].astype(BF16)
        up_grad_ref[rows, :] = both_grads[:, hidden:].astype(BF16)
    for d in PLANE_ORDER:
        plane_in(9, back_out, back_in, d).wait_recv()
    moe_grad = dot(choice_t[...], back_in[...].reshape(DEPTH * CHUNK, quarter))
    stream[t] = (own[...].astype(F32) + moe_grad).astype(BF16)

    low, high = pl.ds(0, tokens // 2), pl.ds(tokens // 2, tokens // 2)

    def ring(kind, which, rows, to):
        return remote(stream.at[which, rows], stream.at[which, rows], sems(kind, 0), {"tp": to})

    def stream_spread():
        return (
            ring(0, t, low, right),
            ring(1, t, high, left),
            ring(2 + 6, t, high, right),
            ring(3 + 6, t, low, left),
        )

    def stream_arrived():
        return (
            ring(0, left, low, right),
            ring(1, right, high, left),
            ring(2 + 6, left, high, right),
            ring(3 + 6, right, low, left),
        )

    def stream_pass(which_low, which_high):
        return (
            remote(
                stream.at[which_low, low], stream.at[which_low, low], sems(10, 0), {"tp": right}
            ),
            remote(
                stream.at[which_high, high], stream.at[which_high, high], sems(11, 0), {"tp": left}
            ),
        )

    for copy in stream_spread():
        copy.start()
    loads[5].wait()

    def share(which):
        rows = pl.ds(pl.multiple_of(which * quarter, quarter), quarter)
        return jnp.dot(stream[which], w_out[rows, :], preferred_element_type=F32)

    mixed_grad = share(t)
    onward = stream_pass(left, right)
    for n, copy in enumerate(stream_arrived()):
        copy.wait_recv()
        if n < 2:
            onward[n].start()
    mixed_grad = mixed_grad + share(left) + share(right)
    for copy in stream_pass(across, across):
        copy.wait_recv()
    mixed_grad = mixed_grad + share(across)

    back_c, back_d = jnp.zeros((DV, 128), F32), jnp.zeros((DV, 128), F32)
    for b, piece in enumerate(pieces):
        mg = heads_on_rows(mixed_grad[b * BLOCK : (b + 1) * BLOCK, :])
        mean = jnp.mean(mg * piece.mixed, axis=1, keepdims=True)
        piece.do = (piece.inv * (mg - piece.mixed * mean)).astype(BF16)
        piece.back_f = dot(piece.do, piece.qg, TN)
        piece.back_b = dot(piece.do, piece.qh, TN)
    for piece in pieces:
        back_c = back_c * jnp.exp(piece.first) + piece.back_b
    for piece in reversed(pieces):
        back_d = back_d * jnp.exp(piece.last) + piece.back_f
    carry = Carry(carry_refs[12:])
    carry.start((back_c, back_d), (log_b, log_f))

    rows_of_mixed = jnp.concatenate([heads_on_lanes(piece.mixed) for piece in pieces], axis=0)
    rows_of_mixed = rows_of_mixed.astype(BF16)
    piece_rows = proj_ref.shape[0]
    for n in range(RING):
        term = dot(stream[n], rows_of_mixed, TN).astype(BF16)
        per = term.shape[0] // (piece_rows * PLANES)
        term = term.reshape(per, 4, 2, piece_rows, term.shape[1])
        for cc in range(2):
            for zz in range(per):
                terms[cc, :, n * per + zz] = term[zz, :, cc]

    def core_copy():
        return remote(terms.at[1 - c], core_in, sems(12, 0), {"sp_2": 1 - c})

    def row_copy(d, arriving=False):
        other = lax.rem(y + (4 - d if arriving else d), 4)
        at = other if arriving else y
        return remote(core_sum.at[other], row_in.at[at], sems(12, d), {"sp_1": other})

    def last_copy(d, arriving=False):
        other = lax.rem(z + (DEPTH - d if arriving else d), DEPTH)
        at = other if arriving else z
        return remote(row_sum.at[other], depth_in.at[at], sems(13, d), {"sp_0": other})

    core_copy().start()

    inclusive, strict = masks()
    for piece in pieces:
        da = dot(piece.do, piece.vs, NT)
        da_f = jnp.where(inclusive, da, 0.0).astype(BF16)
        da_b = jnp.where(strict, da, 0.0).astype(BF16)
        piece.dv = dot(piece.a, piece.do, TN)
        piece.dq = dot(da_f, piece.k_dn_g) * doubled(piece.up_g) + dot(
            da_b, piece.k_dn_h
        ) * doubled(piece.up_h)
        piece.dk = dot(da_f, piece.q_up_g, TN) * doubled(piece.dn_g) + dot(
            da_b, piece.q_up_h, TN
        ) * doubled(piece.dn_h)
    carry.middle()
    core_copy().wait_recv()
    core_sum[...] = (terms[c].astype(F32) + core_in[...].astype(F32)).astype(BF16)
    for d in (2, 1, 3):
        row_copy(d).start()
    for b, piece in enumerate(pieces):
        dq = dot(piece.do, piece.states)
        dq = piece.dq + dq[:, :128] * stacked(piece.eg) + dq[:, 128:] * stacked(piece.eh)
        dq_ref[pl.ds(b * BLOCK, BLOCK), :] = (folded(dq) * KEY_CHANNELS**-0.5).astype(BF16)
    carry.last()
    for d in (1, 3, 2):
        row_copy(d, True).wait_recv()
    row_in[y] = core_sum[y]
    total = row_in[0].astype(F32)
    for n in range(1, 4):
        total = total + row_in[n].astype(F32)
    row_sum[...] = total
    for d in (4, 3, 5, 2, 6, 1, 7):
        last_copy(d).start()
    back_c, back_d = carry.finish()
    late, early = [None] * 3, [None] * 3
    for b, piece in enumerate(pieces):
        early[b] = back_c
        back_c = back_c * jnp.exp(piece.first) + piece.back_b
    for b in reversed(range(3)):
        late[b] = back_d
        back_d = back_d * jnp.exp(pieces[b].last) + pieces[b].back_f
    for b, piece in enumerate(pieces):
        states = jnp.concatenate([late[b], early[b]], axis=1).astype(BF16)
        dk = dot(piece.vs, states)
        dk = piece.dk + dk[:, :128] * stacked(piece.eg_end) + dk[:, 128:] * stacked(piece.eh_end)
        dv = piece.dv + dot(jnp.concatenate([piece.kg_end, piece.kh_end], axis=1), states, NT)
        rows = pl.ds(b * BLOCK, BLOCK)
        dk_ref[rows, :] = folded(dk).astype(BF16)
        dv_ref[rows, :] = heads_on_lanes(dv).astype(BF16)
    depth_in[z] = row_sum[z]
    for d in range(1, DEPTH):
        last_copy(d, True).wait_recv()
    total = depth_in[0]
    for n in range(1, DEPTH):
        total = total + depth_in[n]
    proj_ref[...] = total

    for d in PLANE_ORDER:
        plane_out(0, out_plane, in_plane, d).wait_send()
        plane_out(9, back_out, back_in, d).wait_send()
    for i in range(DEPTH):
        if i > 0:
            depth_out(i).wait_send()
            send_back(i).wait_send()
        for copy in (*spread(i), pass_on(i), send_hop(i), send_both(i), send_plain(i)):
            copy.wait_send()
    for copy in (*stream_spread(), *stream_pass(left, right), core_copy()):
        copy.wait_send()
    for d in (1, 2, 3):
        row_copy(d).wait_send()
    for d in range(1, DEPTH):
        last_copy(d).wait_send()


def vmem(n):
    return [pl.BlockSpec(memory_space=pltpu.VMEM)] * n


def layer(*arrays):
    layer_grad, slot_tokens, gate = arrays[2], arrays[3], arrays[4]
    tokens, width = layer_grad.shape
    slots = slot_tokens.shape[1]
    quarter = width // RING
    hidden = gate.shape[2]
    out_columns = arrays[7].shape[1]
    piece_rows = width // (DEPTH * PLANES)
    rows = (DEPTH, CHUNK, quarter)
    anywhere = pl.BlockSpec(memory_space=pl.ANY)
    return pl.pallas_call(
        layer_kernel,
        out_shape=(
            pltpu.VMEM((width, hidden), BF16),
            pltpu.VMEM((width, hidden), BF16),
            pltpu.VMEM((hidden, width), BF16),
            pltpu.VMEM((piece_rows, out_columns), F32),
            pltpu.VMEM((tokens, 128), BF16),
            pltpu.VMEM((tokens, 128), BF16),
            pltpu.VMEM((tokens, 2 * DV), BF16),
        ),
        in_specs=vmem(2) + [anywhere] * 11,
        out_specs=tuple(vmem(7)),
        scratch_shapes=[
            *[pltpu.VMEM(a.shape, a.dtype) for a in arrays[8:]],
            pltpu.VMEM((tokens, quarter), BF16),
            pltpu.VMEM((slots, width), BF16),
            pltpu.VMEM((width, 2 * hidden), BF16),
            pltpu.VMEM((hidden, width), BF16),
            pltpu.VMEM((width, out_columns), BF16),
            pltpu.VMEM((slots, tokens), BF16),
            pltpu.VMEM((tokens, slots), BF16),
            pltpu.VMEM((slots, slots), BF16),
            pltpu.VMEM((DEPTH, CHUNK, hidden), BF16),
            pltpu.VMEM((DEPTH, CHUNK, hidden), F32),
            pltpu.VMEM((DEPTH, CHUNK, hidden), F32),
            pltpu.VMEM((DEPTH, CHUNK, 2 * hidden), BF16),
            pltpu.VMEM(rows, BF16),
            pltpu.VMEM(rows, BF16),
            pltpu.VMEM(rows, BF16),
            pltpu.VMEM((RING, *rows), BF16),
            pltpu.VMEM((DEPTH, RING, CHUNK, quarter), BF16),
            *[pltpu.VMEM(rows, BF16)] * 8,
            pltpu.VMEM((RING, tokens, quarter), BF16),
            pltpu.VMEM((2, 4, DEPTH, piece_rows, out_columns), BF16),
            pltpu.VMEM((4, DEPTH, piece_rows, out_columns), BF16),
            pltpu.VMEM((4, DEPTH, piece_rows, out_columns), BF16),
            pltpu.VMEM((4, DEPTH, piece_rows, out_columns), BF16),
            pltpu.VMEM((DEPTH, piece_rows, out_columns), F32),
            pltpu.VMEM((DEPTH, piece_rows, out_columns), F32),
            pltpu.SemaphoreType.DMA((14, DEPTH)),
            pltpu.SemaphoreType.DMA((14, DEPTH)),
            pltpu.SemaphoreType.DMA((11,)),
            *Carry.scratch(),
            *Carry.scratch(),
        ],
        compiler_params=pltpu.CompilerParams(
            collective_id=0, has_side_effects=True, vmem_limit_bytes=56 * 2**20
        ),
        cost_estimate=pl.CostEstimate(
            flops=8 * 10**9, bytes_accessed=12 * 2**20, transcendentals=0
        ),
        name="layer",
    )(*arrays)


def write_kernel(*refs):
    n = len(refs) // 2
    done = refs[-1]
    copies = [pltpu.make_async_copy(refs[i], refs[n + i], done.at[i]) for i in range(n)]
    for copy in copies:
        copy.start()
    for copy in copies:
        copy.wait()


def written(arrays):
    n = len(arrays)
    arrays = [pltpu.with_memory_space_constraint(a, pltpu.VMEM) for a in arrays]
    return pl.pallas_call(
        write_kernel,
        out_shape=tuple(jax.ShapeDtypeStruct(a.shape, a.dtype) for a in arrays),
        in_specs=vmem(n),
        out_specs=(pl.BlockSpec(memory_space=pl.ANY),) * n,
        scratch_shapes=[pltpu.SemaphoreType.DMA((n,))],
        compiler_params=pltpu.CompilerParams(vmem_limit_bytes=2**20),
        name="write",
    )(*arrays)


def on_device(layer_grad, routes, route_weight, *arrays):
    results = written(layer(routes.T, route_weight.T, layer_grad, *arrays))
    gate, up, down, proj, query, key, value = results
    return gate[None], up[None], down[None], proj, query, key, value


def solution(mesh):
    torus = Mesh(mesh.devices.reshape(8, 4, 2, mesh.shape["tp"]), ("sp_0", "sp_1", "sp_2", "tp"))
    in_specs = (
        P(SP, None),
        P(SP, None),
        P(SP, None),
        P(SP, None, None),
        P(SP, None, "tp"),
        P(SP, None, "tp"),
        P(SP, "tp", None),
        P(None, "tp"),
        P(SP, "tp"),
        P(SP, "tp"),
        P(SP, "tp"),
        P(SP, "tp"),
        P(SP, "tp"),
    )
    out_specs = (
        P(SP, None, "tp"),
        P(SP, None, "tp"),
        P(SP, "tp", None),
        P(SP, "tp"),
        P(SP, "tp"),
        P(SP, "tp"),
        P(SP, "tp"),
    )
    return jax.shard_map(
        on_device, mesh=torus, in_specs=in_specs, out_specs=out_specs, check_vma=False
    )
```

```python
import jax
import jax.numpy as jnp
from jax import lax
from jax.experimental import pallas as pl
from jax.experimental.pallas import tpu as pltpu
from jax.sharding import Mesh
from jax.sharding import PartitionSpec as P

KEY_CHANNELS = 64
DV = 128
BLOCK = 64
SP = ("sp_0", "sp_1", "sp_2")
EPSILON = 1e-06
CAP = 9
F32 = jnp.float32
BF16 = jnp.bfloat16
PIECE = 16
ROWS = PIECE + 8


def dot(a, b, contract=((1,), (0,))):
    return lax.dot_general(
        a.astype(BF16), b.astype(BF16), (contract, ((), ())), preferred_element_type=F32
    )


def dot_exact(a, b):
    return lax.dot_general(
        a,
        b,
        (((1,), (0,)), ((), ())),
        precision=lax.Precision.HIGHEST,
        preferred_element_type=F32,
    )


NT = ((1,), (1,))
TN = ((0,), (0,))


def iota(shape, dim):
    return lax.broadcasted_iota(jnp.int32, shape, dim)


def stacked(x):
    low = iota(x.shape, 1) < KEY_CHANNELS
    zero = jnp.zeros_like(x)
    return jnp.concatenate([jnp.where(low, x, zero), jnp.where(low, zero, x)], axis=0)


def doubled(x):
    return jnp.concatenate([x, x], axis=0)


def folded(x):
    half = x.shape[0] // 2
    return x[:half] + x[half:]


def heads_on_rows(x):
    return jnp.concatenate([x[:, :DV], x[:, DV:]], axis=0)


def heads_on_lanes(x):
    half = x.shape[0] // 2
    return jnp.concatenate([x[:half], x[half:]], axis=1)


def masks():
    shape = (2 * BLOCK, 2 * BLOCK)
    i, j = iota(shape, 0), iota(shape, 1)
    same = (i // BLOCK) == (j // BLOCK)
    return same & (i >= j), same & (i < j)


class Piece:
    def __init__(self, b, q_ref, k_ref, v_ref, fd_ref, bd_ref):
        rows = pl.ds(b * BLOCK, BLOCK)
        shape = (BLOCK, BLOCK)
        lower = (iota(shape, 0) >= iota(shape, 1)).astype(F32)
        upper = (iota(shape, 0) <= iota(shape, 1)).astype(F32)
        self.q = q_ref[rows, :].astype(F32) * KEY_CHANNELS**-0.5
        self.k = k_ref[rows, :].astype(F32)
        self.vs = heads_on_rows(v_ref[rows, :])
        self.g = dot_exact(lower, fd_ref[rows, :])
        self.h = dot_exact(upper, bd_ref[rows, :])
        self.last = self.g[BLOCK - 1 :, :]
        self.first = self.h[:1, :]
        self.mid_g = self.g[BLOCK // 2 - 1 : BLOCK // 2, :]
        self.mid_h = self.h[BLOCK // 2 : BLOCK // 2 + 1, :]

    def ends(self):
        self.eg_end = jnp.exp(self.last - self.g)
        self.eh_end = jnp.exp(self.first - self.h)
        self.kg_end = stacked(self.k * self.eg_end).astype(BF16)
        self.kh_end = stacked(self.k * self.eh_end).astype(BF16)
        self.fresh_f = dot(self.vs, self.kg_end, TN)
        self.fresh_b = dot(self.vs, self.kh_end, TN)

    def entries(self):
        self.eg = jnp.exp(self.g)
        self.eh = jnp.exp(self.h)
        self.qg = stacked(self.q * self.eg).astype(BF16)
        self.qh = stacked(self.q * self.eh).astype(BF16)

    def scores(self, inclusive, strict):
        self.up_g = jnp.exp(self.g - self.mid_g)
        self.dn_g = jnp.exp(self.mid_g - self.g)
        self.up_h = jnp.exp(self.h - self.mid_h)
        self.dn_h = jnp.exp(self.mid_h - self.h)
        self.q_up_g = stacked(self.q * self.up_g).astype(BF16)
        self.k_dn_g = stacked(self.k * self.dn_g).astype(BF16)
        self.q_up_h = stacked(self.q * self.up_h).astype(BF16)
        self.k_dn_h = stacked(self.k * self.dn_h).astype(BF16)
        a_f = jnp.where(inclusive, dot(self.q_up_g, self.k_dn_g, NT), 0.0)
        a_b = jnp.where(strict, dot(self.q_up_h, self.k_dn_h, NT), 0.0)
        return (a_f + a_b).astype(BF16)


def both_states(pieces, forward_entry, backward_entry):
    s, before = forward_entry, []
    for piece in pieces:
        before.append(s)
        s = jnp.exp(piece.last) * s + piece.fresh_f
    r, after = backward_entry, [None] * len(pieces)
    for b in reversed(range(len(pieces))):
        after[b] = r
        r = jnp.exp(pieces[b].first) * r + pieces[b].fresh_b
    return before, after, s, r


def position():
    z, y, c = (lax.axis_index(a) for a in SP)
    return z, y, c, y * 2 + c


def plane_peer(p, d, planes):
    other = lax.rem(p + d, planes)
    return other, {"sp_1": other // 2, "sp_2": lax.rem(other, 2)}


def greet(planes, depth):
    z, _, _, p = position()
    barrier = pltpu.get_barrier_semaphore()
    for d in range(1, planes):
        _, device = plane_peer(p, d, planes)
        pl.semaphore_signal(barrier, 1, device_id=device, device_id_type=pl.DeviceIdType.MESH)
    for d in range(1, depth):
        device = {"sp_0": lax.rem(z + d, depth)}
        pl.semaphore_signal(barrier, 1, device_id=device, device_id_type=pl.DeviceIdType.MESH)
    return barrier, planes + depth - 2


class Carry:
    SCRATCH_PLANES, SCRATCH_DEPTH = 8, 8

    @classmethod
    def scratch(cls):
        n, m = cls.SCRATCH_PLANES, cls.SCRATCH_DEPTH
        return [
            pltpu.VMEM((n, 2, ROWS, 128), F32),
            pltpu.VMEM((n, 2, ROWS, 128), F32),
            pltpu.VMEM((2, ROWS, 128), F32),
            pltpu.VMEM((m, ROWS, 128), F32),
            pltpu.VMEM((n, 2, PIECE, 128), F32),
            pltpu.VMEM((n, 2, PIECE, 128), F32),
            pltpu.SemaphoreType.DMA((n,)),
            pltpu.SemaphoreType.DMA((n,)),
            pltpu.SemaphoreType.DMA((m,)),
            pltpu.SemaphoreType.DMA((m,)),
            pltpu.SemaphoreType.DMA((n,)),
            pltpu.SemaphoreType.DMA((n,)),
        ]

    def __init__(self, refs):
        (
            self.out1,
            self.in1,
            self.out2,
            self.in2,
            self.out3,
            self.in3,
            self.s1,
            self.r1,
            self.s2,
            self.r2,
            self.s3,
            self.r3,
        ) = refs
        self.n, self.m = self.SCRATCH_PLANES, self.SCRATCH_DEPTH
        self.z, _, _, self.p = position()

    def plane_copy(self, out, into, send, recv, d, arriving=False):
        other, device = plane_peer(self.p, d, self.n)
        at = other if arriving else self.p
        return pltpu.make_async_remote_copy(
            src_ref=out.at[other],
            dst_ref=into.at[at],
            send_sem=send.at[other],
            recv_sem=recv.at[at],
            device_id=device,
            device_id_type=pl.DeviceIdType.MESH,
        )

    def start(self, terms, logs):
        for dim in range(2):
            decay = jnp.broadcast_to(logs[dim], (8, 128))
            for j in range(self.n):
                self.out1[j, dim, :PIECE, :] = terms[dim][j * PIECE : (j + 1) * PIECE, :]
                self.out1[j, dim, PIECE:, :] = decay
        for d in range(1, self.n):
            self.plane_copy(self.out1, self.in1, self.s1, self.r1, d).start()
        self.in1[self.p] = self.out1[self.p]

    def middle(self):
        for d in range(1, self.n):
            self.plane_copy(self.out1, self.in1, self.s1, self.r1, d, True).wait_recv()
        zero = jnp.zeros((PIECE, 128), F32)
        none = jnp.zeros((1, 128), F32)
        self.before = [[None] * self.n, [None] * self.n]
        for dim in range(2):
            total, log = zero, none
            for i in range(self.n) if dim == 0 else reversed(range(self.n)):
                self.before[dim][i] = (total, log)
                step = self.in1[i, dim, PIECE : PIECE + 1, :]
                total = total * jnp.exp(step) + self.in1[i, dim, :PIECE, :]
                log = log + step
            self.out2[dim, :PIECE, :] = total
            self.out2[dim, PIECE:, :] = jnp.broadcast_to(log, (8, 128))
        for d in range(1, self.m):
            self.depth_copy(d).start()

    def depth_copy(self, d, arriving=False):
        other = lax.rem(self.z + d, self.m)
        dim = jnp.where(other > self.z, 0, 1)
        at = other if arriving else self.z
        return pltpu.make_async_remote_copy(
            src_ref=self.out2.at[dim],
            dst_ref=self.in2.at[at],
            send_sem=self.s2.at[other],
            recv_sem=self.r2.at[at],
            device_id={"sp_0": other},
            device_id_type=pl.DeviceIdType.MESH,
        )

    def last(self):
        self.in2[self.z] = jnp.zeros((ROWS, 128), F32)
        for d in range(1, self.m):
            self.depth_copy(d, True).wait_recv()
        entry = []
        for dim in range(2):
            total = jnp.zeros((PIECE, 128), F32)
            for i in range(self.m) if dim == 0 else reversed(range(self.m)):
                passed = (i < self.z) if dim == 0 else (i > self.z)
                step = self.in2[i, PIECE : PIECE + 1, :]
                total = jnp.where(passed, total * jnp.exp(step) + self.in2[i, :PIECE, :], total)
            entry.append(total)
        for i in range(self.n):
            for dim in range(2):
                inside, log = self.before[dim][i]
                self.out3[i, dim] = inside + jnp.exp(log) * entry[dim]
        for d in range(1, self.n):
            self.plane_copy(self.out3, self.in3, self.s3, self.r3, d).start()
        self.in3[self.p] = self.out3[self.p]

    def finish(self):
        for d in range(1, self.n):
            self.plane_copy(self.out3, self.in3, self.s3, self.r3, d, True).wait_recv()
        for d in range(1, self.n):
            self.plane_copy(self.out1, self.in1, self.s1, self.r1, d).wait_send()
            self.plane_copy(self.out3, self.in3, self.s3, self.r3, d).wait_send()
        for d in range(1, self.m):
            self.depth_copy(d).wait_send()
        return [self.in3[:, dim].reshape(128, 128) for dim in range(2)]


OFFSETS = (0, 1, 7, 2, 6, 3, 5, 4)
PLANE_ORDER = (2, 6, 3, 7, 4, 5, 1)
PLANES, DEPTH, RING = 8, 8, 4
CHUNK = PLANES * CAP
MESH = pl.DeviceIdType.MESH


def remote(src, dst, sems, device):
    return pltpu.make_async_remote_copy(
        src_ref=src,
        dst_ref=dst,
        send_sem=sems[0],
        recv_sem=sems[1],
        device_id=device,
        device_id_type=MESH,
    )


def swap_matrix(shape):
    i = iota((shape[0], 1), 0)
    a = (i * 911) >> 16
    rest = i - a * CHUNK
    b = (rest * 7282) >> 16
    source = b * CHUNK + a * CAP + (rest - b * CAP)
    return jnp.where(source == iota(shape, 1), 1.0, 0.0).astype(BF16)


def layer_kernel(
    routes,
    route_weight,
    layer_grad,
    slot_tokens,
    gate_proj,
    up_proj,
    down_proj,
    out_proj,
    q_hbm,
    k_hbm,
    v_hbm,
    fd_hbm,
    bd_hbm,
    gate_grad_ref,
    up_grad_ref,
    down_grad_ref,
    proj_ref,
    dq_ref,
    dk_ref,
    dv_ref,
    q,
    k,
    v,
    fd,
    bd,
    own,
    x,
    w_cat,
    down_out,
    down_in,
    w_out,
    choice,
    choice_t,
    swap,
    act,
    silu,
    slope,
    delta,
    out_plane,
    in_plane,
    out_depth,
    inbound,
    first_part,
    first_hop,
    first_hopped,
    first_both,
    first_plain,
    part,
    hop,
    hopped,
    both,
    plain,
    ret_out,
    ret_in,
    back_out,
    back_in,
    stream,
    terms,
    core_in,
    core_sum,
    row_in,
    row_sum,
    depth_in,
    send,
    recv,
    load,
    *carry_refs,
):
    z, y, c, p = position()
    t = lax.axis_index("tp")
    right, left, across = lax.rem(t + 1, RING), lax.rem(t + 3, RING), lax.rem(t + 2, RING)
    quarter = own.shape[1]
    barrier, count = greet(PLANES, DEPTH)
    for other in (left, right, across):
        pl.semaphore_signal(barrier, 1, device_id={"tp": other}, device_id_type=MESH)

    columns = pl.ds(pl.multiple_of(t * quarter, quarter), quarter)
    hidden = down_in.shape[1]
    loads = [
        pltpu.make_async_copy(layer_grad.at[:, columns], own, load.at[0]),
        pltpu.make_async_copy(slot_tokens.at[0], x, load.at[1]),
        pltpu.make_async_copy(gate_proj.at[0], w_cat.at[:, pl.ds(0, hidden)], load.at[2]),
        pltpu.make_async_copy(up_proj.at[0], w_cat.at[:, pl.ds(hidden, hidden)], load.at[3]),
        pltpu.make_async_copy(down_proj.at[0, :, columns], down_in.at[t], load.at[4]),
        pltpu.make_async_copy(out_proj, w_out, load.at[5]),
    ]
    for n, (source, to) in enumerate(
        ((q_hbm, q), (k_hbm, k), (v_hbm, v), (fd_hbm, fd), (bd_hbm, bd))
    ):
        loads.append(pltpu.make_async_copy(source, to, load.at[6 + n]))
    for n in range(1, RING):
        other = lax.rem(t + n, RING)
        there = pl.ds(pl.multiple_of(other * quarter, quarter), quarter)
        loads.append(
            pltpu.make_async_copy(
                down_proj.at[0, :, there], down_out.at[other], load.at[10 + n]
            )
        )
    for copy in (loads[0], *loads[11:], *loads[6:11], *loads[1:6]):
        copy.start()

    def sems(kind, i):
        return send.at[kind, i], recv.at[kind, i]

    def plane_out(kind, out, into, d):
        other, device = plane_peer(p, d, PLANES)
        return remote(out.at[other], into.at[p], sems(kind, d), device)

    def plane_in(kind, out, into, d):
        other, device = plane_peer(p, PLANES - d, PLANES)
        return remote(out.at[other], into.at[other], sems(kind, d), device)

    tokens = own.shape[0]
    slots = x.shape[0]
    names = iota((128, tokens), 0)
    members = [(routes[j : j + 1, :] == names).astype(F32) for j in range(2)]
    shape = (tokens, tokens)
    later = (iota(shape, 0) < iota(shape, 1)).astype(BF16)
    before = dot(members[0] + members[1], later)
    scale = jnp.zeros((slots, 1), F32)
    chosen = jnp.zeros((slots, tokens), F32)
    for j in range(2):
        rank = jnp.sum((before + members[0] * j) * members[j], axis=0, keepdims=True)
        rank = rank.astype(jnp.int32)
        expert = routes[j : j + 1, :]
        row = (expert & (PLANES - 1)) * CHUNK + (expert >> 3) * CAP + rank
        row = jnp.where(rank < CAP, row, -1)
        taken = row == iota((slots, tokens), 0)
        chosen = jnp.where(taken, 1.0, chosen)
        given = jnp.where(taken, route_weight[j : j + 1, :], 0.0)
        scale = scale + jnp.sum(given, axis=1, keepdims=True)
    choice[...] = chosen.astype(BF16)
    loads[0].wait()
    picked = dot(choice[...], own[...]) * scale
    out_plane[...] = picked.astype(BF16).reshape(out_plane.shape)
    pl.semaphore_wait(barrier, count + 3)
    for d in PLANE_ORDER:
        plane_out(0, out_plane, in_plane, d).start()
    in_plane[p] = out_plane[p]

    def down_copy(n, arriving=False):
        other = lax.rem(t + (RING - n if arriving else n), RING)
        at = other if arriving else t
        return remote(down_out.at[other], down_in.at[at], sems(14, n), {"tp": other})

    for copy in loads[11:]:
        copy.wait()
    for n in (2, 1, 3):
        down_copy(n).start()

    for copy in loads[6:11]:
        copy.wait()
    pieces = [Piece(b, q, k, v, fd, bd) for b in range(3)]
    for piece in pieces:
        piece.ends()
    zero = jnp.zeros((DV, 128), F32)
    _, _, forward_end, backward_end = both_states(pieces, zero, zero)
    log_f = sum(piece.last for piece in pieces)
    log_b = sum(piece.first for piece in pieces)
    carry = Carry(carry_refs[:12])
    carry.start((forward_end, backward_end), (log_f, log_b))
    swap[...] = swap_matrix(swap.shape)
    choice_t[...] = choice[...].T

    def chunk_of(i):
        return lax.rem(z + OFFSETS[i], DEPTH)

    def spread(i, arriving=False):
        at = chunk_of(i)
        a, b = (left, right) if arriving else (t, t)
        return (
            remote(inbound.at[a, at], inbound.at[a, at], sems(2, i), {"tp": right}),
            remote(inbound.at[b, at], inbound.at[b, at], sems(3, i), {"tp": left}),
        )

    def sides(i):
        return (left, right) if i % 2 == 0 else (right, left)

    def pass_on(i, arriving=False):
        source, to = sides(i)
        at, which = chunk_of(i), across if arriving else source
        return remote(inbound.at[which, at], inbound.at[which, at], sems(4, i), {"tp": to})

    def send_hop(i):
        _, to = sides(i)
        return remote(part.at[i, across], hop.at[i], sems(5, i), {"tp": to})

    def send_both(i):
        _, to = sides(i)
        return remote(hopped.at[i], both.at[i], sems(6, i), {"tp": to})

    def send_plain(i):
        to, _ = sides(i)
        return remote(part.at[i, to], plain.at[i], sems(7, i), {"tp": to})

    def send_back(i, arriving=False):
        at = lax.rem(z + DEPTH - OFFSETS[i], DEPTH) if arriving else z
        other = chunk_of(i)
        return remote(ret_out.at[other], ret_in.at[at], sems(8, i), {"sp_0": other})

    def first_send_hop(i):
        _, to = sides(i)
        return remote(first_part.at[i, across], first_hop.at[i], sems(15, i), {"tp": to})

    def first_send_both(i):
        _, to = sides(i)
        return remote(first_hopped.at[i], first_both.at[i], sems(16, i), {"tp": to})

    def first_send_plain(i):
        to, _ = sides(i)
        return remote(first_part.at[i, to], first_plain.at[i], sems(17, i), {"tp": to})

    def stage_0(i):
        at = chunk_of(i)
        if i > 0:
            remote(out_depth.at[at], inbound.at[t, at], sems(1, i), {"sp_0": at}).wait_recv()
        partial = dot(inbound[t, at], down_in[...].reshape(RING * hidden, quarter), NT)
        for n in range(RING):
            first_part[i, n] = partial[:, n * hidden : (n + 1) * hidden].astype(BF16)
        first_send_hop(i).start()
        first_send_plain(i).start()

    def stage_1(i):
        _, to = sides(i)
        first_send_hop(i).wait_recv()
        total = first_hop[i].astype(F32) + first_part[i, to].astype(F32)
        first_hopped[i] = total.astype(BF16)
        first_send_both(i).start()

    def stage_2(i):
        at = chunk_of(i)
        first_send_both(i).wait_recv()
        first_send_plain(i).wait_recv()
        total = first_part[i, t].astype(F32) + first_both[i].astype(F32)
        total = total + first_plain[i].astype(F32)
        up_delta = (total * silu[at]).astype(BF16)
        gate_delta = (total * slope[at]).astype(BF16)
        deltas = jnp.concatenate([gate_delta, up_delta], axis=1)
        delta[at] = deltas
        _, to = sides(i)
        for n, which in enumerate((across, sides(i)[0], to, t)):
            rows = pl.ds(pl.multiple_of(which * quarter, quarter), quarter)
            part[i, which] = dot(deltas, w_cat[rows, :], NT).astype(BF16)
            if n == 0:
                send_hop(i).start()
            if n == 1:
                send_plain(i).start()

    def stage_3(i):
        _, to = sides(i)
        send_hop(i).wait_recv()
        hopped[i] = (hop[i].astype(F32) + part[i, to].astype(F32)).astype(BF16)
        send_both(i).start()

    def stage_4(i):
        at = chunk_of(i)
        send_both(i).wait_recv()
        send_plain(i).wait_recv()
        total = part[i, t].astype(F32) + both[i].astype(F32) + plain[i].astype(F32)
        if i == 0:
            ret_in[z] = total.astype(BF16)
        else:
            ret_out[at] = total.astype(BF16)
            send_back(i).start()

    for d in PLANE_ORDER:
        plane_in(0, out_plane, in_plane, d).wait_recv()
    moved = dot(swap[...], in_plane[...].reshape(DEPTH * CHUNK, quarter)).astype(BF16)
    out_depth[...] = moved.reshape(out_depth.shape)

    def depth_out(i):
        other = lax.rem(z + DEPTH - OFFSETS[i], DEPTH)
        return remote(out_depth.at[other], inbound.at[t, z], sems(1, i), {"sp_0": other})

    inbound[t, z] = out_depth[z]
    for i in range(1, DEPTH):
        depth_out(i).start()
    carry.middle()

    for copy in loads[1:4]:
        copy.wait()
    half = x.shape[0] // 2
    for j in range(2):
        rows = pl.ds(j * half, half)
        chunks = pl.ds(j * (DEPTH // 2), DEPTH // 2)
        both_up = jnp.dot(x[rows, :], w_cat[...], preferred_element_type=F32)
        gate, up = both_up[:, :hidden], both_up[:, hidden:]
        sigma = jax.nn.sigmoid(gate)
        s = gate * sigma
        shape = (DEPTH // 2, CHUNK, hidden)
        silu[chunks] = s.reshape(shape)
        act[chunks] = (s * up).astype(BF16).reshape(shape)
        slope[chunks] = (up * sigma * (1.0 + gate * (1.0 - sigma))).reshape(shape)
    loads[4].wait()
    for n in range(1, RING):
        down_copy(n, True).wait_recv()

    stages = (stage_0, stage_1, stage_2, stage_3, stage_4)
    for n in range(DEPTH + len(stages) - 1):
        for lag, stage in enumerate(stages):
            if 0 <= n - lag < DEPTH:
                stage(n - lag)
        if n == 2:
            inclusive, strict = masks()
            for piece in pieces:
                piece.a = piece.scores(inclusive, strict)
                piece.inner = dot(piece.a, piece.vs)
                piece.entries()
        if n == 5:
            carry.last()
        if n == 8:
            forward_entry, backward_entry = carry.finish()
            before, after, _, _ = both_states(pieces, forward_entry, backward_entry)
            for b, piece in enumerate(pieces):
                piece.states = jnp.concatenate([before[b], after[b]], axis=1).astype(BF16)
                o = piece.inner + dot(
                    jnp.concatenate([piece.qg, piece.qh], axis=1), piece.states, NT
                )
                piece.inv = lax.rsqrt(jnp.mean(o * o, axis=1, keepdims=True) + EPSILON)
                piece.mixed = o * piece.inv

    for i in range(DEPTH):
        for copy in spread(i):
            copy.start()

    for i in range(1, DEPTH):
        send_back(i, True).wait_recv()
    moved = dot(swap[...], ret_in[...].reshape(DEPTH * CHUNK, quarter)).astype(BF16)
    back_out[...] = moved.reshape(back_out.shape)
    for d in PLANE_ORDER:
        plane_out(9, back_out, back_in, d).start()
    back_in[p] = back_out[p]
    deltas = delta[...].reshape(DEPTH * CHUNK, 2 * hidden)
    for n in range(RING):
        both_grads = dot(x[:, n * quarter : (n + 1) * quarter], deltas, TN)
        rows = pl.ds(n * quarter, quarter)
        gate_grad_ref[rows, :] = both_grads[:, :hidden].astype(BF16)
        up_grad_ref[rows, :] = both_grads[:, hidden:].astype(BF16)
    for d in PLANE_ORDER:
        plane_in(9, back_out, back_in, d).wait_recv()
    moe_grad = dot(choice_t[...], back_in[...].reshape(DEPTH * CHUNK, quarter))
    stream[t] = (own[...].astype(F32) + moe_grad).astype(BF16)

    low, high = pl.ds(0, tokens // 2), pl.ds(tokens // 2, tokens // 2)

    def ring(kind, which, rows, to):
        return remote(stream.at[which, rows], stream.at[which, rows], sems(kind, 0), {"tp": to})

    def stream_spread():
        return (
            ring(0, t, low, right),
            ring(1, t, high, left),
            ring(2 + 6, t, high, right),
            ring(3 + 6, t, low, left),
        )

    def stream_arrived():
        return (
            ring(0, left, low, right),
            ring(1, right, high, left),
            ring(2 + 6, left, high, right),
            ring(3 + 6, right, low, left),
        )

    def stream_pass(which_low, which_high):
        return (
            remote(
                stream.at[which_low, low], stream.at[which_low, low], sems(10, 0), {"tp": right}
            ),
            remote(
                stream.at[which_high, high], stream.at[which_high, high], sems(11, 0), {"tp": left}
            ),
        )

    for copy in stream_spread():
        copy.start()
    loads[5].wait()

    def share(which):
        rows = pl.ds(pl.multiple_of(which * quarter, quarter), quarter)
        return jnp.dot(stream[which], w_out[rows, :], preferred_element_type=F32)

    mixed_grad = share(t)
    onward = stream_pass(left, right)
    for n, copy in enumerate(stream_arrived()):
        copy.wait_recv()
        if n < 2:
            onward[n].start()
    mixed_grad = mixed_grad + share(left) + share(right)
    for copy in stream_pass(across, across):
        copy.wait_recv()
    mixed_grad = mixed_grad + share(across)

    back_c, back_d = jnp.zeros((DV, 128), F32), jnp.zeros((DV, 128), F32)
    for b, piece in enumerate(pieces):
        mg = heads_on_rows(mixed_grad[b * BLOCK : (b + 1) * BLOCK, :])
        mean = jnp.mean(mg * piece.mixed, axis=1, keepdims=True)
        piece.do = (piece.inv * (mg - piece.mixed * mean)).astype(BF16)
        piece.back_f = dot(piece.do, piece.qg, TN)
        piece.back_b = dot(piece.do, piece.qh, TN)
    for piece in pieces:
        back_c = back_c * jnp.exp(piece.first) + piece.back_b
    for piece in reversed(pieces):
        back_d = back_d * jnp.exp(piece.last) + piece.back_f
    carry = Carry(carry_refs[12:])
    carry.start((back_c, back_d), (log_b, log_f))

    rows_of_mixed = jnp.concatenate([heads_on_lanes(piece.mixed) for piece in pieces], axis=0)
    rows_of_mixed = rows_of_mixed.astype(BF16)
    piece_rows = proj_ref.shape[0]
    for n in range(RING):
        term = dot(stream[n], rows_of_mixed, TN).astype(BF16)
        per = term.shape[0] // (piece_rows * PLANES)
        term = term.reshape(per, 4, 2, piece_rows, term.shape[1])
        for cc in range(2):
            for zz in range(per):
                terms[cc, :, n * per + zz] = term[zz, :, cc]

    def core_copy():
        return remote(terms.at[1 - c], core_in, sems(12, 0), {"sp_2": 1 - c})

    def row_copy(d, arriving=False):
        other = lax.rem(y + (4 - d if arriving else d), 4)
        at = other if arriving else y
        return remote(core_sum.at[other], row_in.at[at], sems(12, d), {"sp_1": other})

    def last_copy(d, arriving=False):
        other = lax.rem(z + (DEPTH - d if arriving else d), DEPTH)
        at = other if arriving else z
        return remote(row_sum.at[other], depth_in.at[at], sems(13, d), {"sp_0": other})

    core_copy().start()
    for i in range(DEPTH):
        for copy in spread(i, True):
            copy.wait_recv()
        pass_on(i).start()

    inclusive, strict = masks()
    for piece in pieces:
        da = dot(piece.do, piece.vs, NT)
        da_f = jnp.where(inclusive, da, 0.0).astype(BF16)
        da_b = jnp.where(strict, da, 0.0).astype(BF16)
        piece.dv = dot(piece.a, piece.do, TN)
        piece.dq = dot(da_f, piece.k_dn_g) * doubled(piece.up_g) + dot(
            da_b, piece.k_dn_h
        ) * doubled(piece.up_h)
        piece.dk = dot(da_f, piece.q_up_g, TN) * doubled(piece.dn_g) + dot(
            da_b, piece.q_up_h, TN
        ) * doubled(piece.dn_h)
    carry.middle()
    core_copy().wait_recv()
    core_sum[...] = (terms[c].astype(F32) + core_in[...].astype(F32)).astype(BF16)
    for d in (2, 1, 3):
        row_copy(d).start()
    for b, piece in enumerate(pieces):
        dq = dot(piece.do, piece.states)
        dq = piece.dq + dq[:, :128] * stacked(piece.eg) + dq[:, 128:] * stacked(piece.eh)
        dq_ref[pl.ds(b * BLOCK, BLOCK), :] = (folded(dq) * KEY_CHANNELS**-0.5).astype(BF16)
    carry.last()
    for i in range(DEPTH):
        pass_on(i, True).wait_recv()
    act_all = act[...].reshape(DEPTH * CHUNK, hidden)
    for n in range(RING):
        rows = inbound[n].reshape(DEPTH * CHUNK, quarter)
        down_grad_ref[:, n * quarter : (n + 1) * quarter] = dot(act_all, rows, TN).astype(BF16)
    for d in (1, 3, 2):
        row_copy(d, True).wait_recv()
    row_in[y] = core_sum[y]
    total = row_in[0].astype(F32)
    for n in range(1, 4):
        total = total + row_in[n].astype(F32)
    row_sum[...] = total.astype(BF16)
    for d in (4, 3, 5, 2, 6, 1, 7):
        last_copy(d).start()
    back_c, back_d = carry.finish()
    late, early = [None] * 3, [None] * 3
    for b, piece in enumerate(pieces):
        early[b] = back_c
        back_c = back_c * jnp.exp(piece.first) + piece.back_b
    for b in reversed(range(3)):
        late[b] = back_d
        back_d = back_d * jnp.exp(pieces[b].last) + pieces[b].back_f
    for b, piece in enumerate(pieces):
        states = jnp.concatenate([late[b], early[b]], axis=1).astype(BF16)
        dk = dot(piece.vs, states)
        dk = piece.dk + dk[:, :128] * stacked(piece.eg_end) + dk[:, 128:] * stacked(piece.eh_end)
        dv = piece.dv + dot(jnp.concatenate([piece.kg_end, piece.kh_end], axis=1), states, NT)
        rows = pl.ds(b * BLOCK, BLOCK)
        dk_ref[rows, :] = folded(dk).astype(BF16)
        dv_ref[rows, :] = heads_on_lanes(dv).astype(BF16)
    depth_in[z] = row_sum[z]
    for d in range(1, DEPTH):
        last_copy(d, True).wait_recv()
    total = depth_in[0].astype(F32)
    for n in range(1, DEPTH):
        total = total + depth_in[n].astype(F32)
    proj_ref[...] = total

    for d in PLANE_ORDER:
        plane_out(0, out_plane, in_plane, d).wait_send()
        plane_out(9, back_out, back_in, d).wait_send()
    for i in range(DEPTH):
        if i > 0:
            depth_out(i).wait_send()
            send_back(i).wait_send()
        for copy in (*spread(i), pass_on(i), send_hop(i), send_both(i), send_plain(i)):
            copy.wait_send()
        for copy in (first_send_hop(i), first_send_both(i), first_send_plain(i)):
            copy.wait_send()
    for n in range(1, RING):
        down_copy(n).wait_send()
    for copy in (*stream_spread(), *stream_pass(left, right), core_copy()):
        copy.wait_send()
    for d in (1, 2, 3):
        row_copy(d).wait_send()
    for d in range(1, DEPTH):
        last_copy(d).wait_send()


def vmem(n):
    return [pl.BlockSpec(memory_space=pltpu.VMEM)] * n


def layer(*arrays):
    layer_grad, slot_tokens, gate = arrays[2], arrays[3], arrays[4]
    tokens, width = layer_grad.shape
    slots = slot_tokens.shape[1]
    quarter = width // RING
    hidden = gate.shape[2]
    out_columns = arrays[7].shape[1]
    piece_rows = width // (DEPTH * PLANES)
    rows = (DEPTH, CHUNK, quarter)
    anywhere = pl.BlockSpec(memory_space=pl.ANY)
    return pl.pallas_call(
        layer_kernel,
        out_shape=(
            pltpu.VMEM((width, hidden), BF16),
            pltpu.VMEM((width, hidden), BF16),
            pltpu.VMEM((hidden, width), BF16),
            pltpu.VMEM((piece_rows, out_columns), F32),
            pltpu.VMEM((tokens, 128), BF16),
            pltpu.VMEM((tokens, 128), BF16),
            pltpu.VMEM((tokens, 2 * DV), BF16),
        ),
        in_specs=vmem(2) + [anywhere] * 11,
        out_specs=tuple(vmem(7)),
        scratch_shapes=[
            *[pltpu.VMEM(a.shape, a.dtype) for a in arrays[8:]],
            pltpu.VMEM((tokens, quarter), BF16),
            pltpu.VMEM((slots, width), BF16),
            pltpu.VMEM((width, 2 * hidden), BF16),
            pltpu.VMEM((RING, hidden, quarter), BF16),
            pltpu.VMEM((RING, hidden, quarter), BF16),
            pltpu.VMEM((width, out_columns), BF16),
            pltpu.VMEM((slots, tokens), BF16),
            pltpu.VMEM((tokens, slots), BF16),
            pltpu.VMEM((slots, slots), BF16),
            pltpu.VMEM((DEPTH, CHUNK, hidden), BF16),
            pltpu.VMEM((DEPTH, CHUNK, hidden), F32),
            pltpu.VMEM((DEPTH, CHUNK, hidden), F32),
            pltpu.VMEM((DEPTH, CHUNK, 2 * hidden), BF16),
            pltpu.VMEM(rows, BF16),
            pltpu.VMEM(rows, BF16),
            pltpu.VMEM(rows, BF16),
            pltpu.VMEM((RING, *rows), BF16),
            pltpu.VMEM((DEPTH, RING, CHUNK, hidden), BF16),
            *[pltpu.VMEM((DEPTH, CHUNK, hidden), BF16)] * 4,
            pltpu.VMEM((DEPTH, RING, CHUNK, quarter), BF16),
            *[pltpu.VMEM(rows, BF16)] * 8,
            pltpu.VMEM((RING, tokens, quarter), BF16),
            pltpu.VMEM((2, 4, DEPTH, piece_rows, out_columns), BF16),
            pltpu.VMEM((4, DEPTH, piece_rows, out_columns), BF16),
            pltpu.VMEM((4, DEPTH, piece_rows, out_columns), BF16),
            pltpu.VMEM((4, DEPTH, piece_rows, out_columns), BF16),
            pltpu.VMEM((DEPTH, piece_rows, out_columns), BF16),
            pltpu.VMEM((DEPTH, piece_rows, out_columns), BF16),
            pltpu.SemaphoreType.DMA((18, DEPTH)),
            pltpu.SemaphoreType.DMA((18, DEPTH)),
            pltpu.SemaphoreType.DMA((14,)),
            *Carry.scratch(),
            *Carry.scratch(),
        ],
        compiler_params=pltpu.CompilerParams(
            collective_id=0, has_side_effects=True, vmem_limit_bytes=56 * 2**20
        ),
        cost_estimate=pl.CostEstimate(
            flops=8 * 10**9, bytes_accessed=12 * 2**20, transcendentals=0
        ),
        name="layer",
    )(*arrays)


def write_kernel(*refs):
    n = len(refs) // 2
    done = refs[-1]
    copies = [pltpu.make_async_copy(refs[i], refs[n + i], done.at[i]) for i in range(n)]
    for copy in copies:
        copy.start()
    for copy in copies:
        copy.wait()


def written(arrays):
    n = len(arrays)
    arrays = [pltpu.with_memory_space_constraint(a, pltpu.VMEM) for a in arrays]
    return pl.pallas_call(
        write_kernel,
        out_shape=tuple(jax.ShapeDtypeStruct(a.shape, a.dtype) for a in arrays),
        in_specs=vmem(n),
        out_specs=(pl.BlockSpec(memory_space=pl.ANY),) * n,
        scratch_shapes=[pltpu.SemaphoreType.DMA((n,))],
        compiler_params=pltpu.CompilerParams(vmem_limit_bytes=2**20),
        name="write",
    )(*arrays)


def on_device(layer_grad, routes, route_weight, *arrays):
    results = written(layer(routes.T, route_weight.T, layer_grad, *arrays))
    gate, up, down, proj, query, key, value = results
    return gate[None], up[None], down[None], proj, query, key, value


def solution(mesh):
    torus = Mesh(mesh.devices.reshape(8, 4, 2, mesh.shape["tp"]), ("sp_0", "sp_1", "sp_2", "tp"))
    in_specs = (
        P(SP, None),
        P(SP, None),
        P(SP, None),
        P(SP, None, None),
        P(SP, None, "tp"),
        P(SP, None, "tp"),
        P(SP, "tp", None),
        P(None, "tp"),
        P(SP, "tp"),
        P(SP, "tp"),
        P(SP, "tp"),
        P(SP, "tp"),
        P(SP, "tp"),
    )
    out_specs = (
        P(SP, None, "tp"),
        P(SP, None, "tp"),
        P(SP, "tp", None),
        P(SP, "tp"),
        P(SP, "tp"),
        P(SP, "tp"),
        P(SP, "tp"),
    )
    return jax.shard_map(
        on_device, mesh=torus, in_specs=in_specs, out_specs=out_specs, check_vma=False
    )
```

```python
import jax
import jax.numpy as jnp
from jax import lax
from jax.experimental import pallas as pl
from jax.experimental.pallas import tpu as pltpu
from jax.sharding import Mesh
from jax.sharding import PartitionSpec as P

KEY_CHANNELS = 64
DV = 128
BLOCK = 64
SP = ("sp_0", "sp_1", "sp_2")
EPSILON = 1e-06
CAP = 9
F32 = jnp.float32
BF16 = jnp.bfloat16
PIECE = 16
ROWS = PIECE + 8


def dot(a, b, contract=((1,), (0,))):
    return lax.dot_general(
        a.astype(BF16), b.astype(BF16), (contract, ((), ())), preferred_element_type=F32
    )


def dot_exact(a, b):
    return lax.dot_general(
        a,
        b,
        (((1,), (0,)), ((), ())),
        precision=lax.Precision.HIGHEST,
        preferred_element_type=F32,
    )


NT = ((1,), (1,))
TN = ((0,), (0,))


def iota(shape, dim):
    return lax.broadcasted_iota(jnp.int32, shape, dim)


def stacked(x):
    low = iota(x.shape, 1) < KEY_CHANNELS
    zero = jnp.zeros_like(x)
    return jnp.concatenate([jnp.where(low, x, zero), jnp.where(low, zero, x)], axis=0)


def doubled(x):
    return jnp.concatenate([x, x], axis=0)


def folded(x):
    half = x.shape[0] // 2
    return x[:half] + x[half:]


def heads_on_rows(x):
    return jnp.concatenate([x[:, :DV], x[:, DV:]], axis=0)


def heads_on_lanes(x):
    half = x.shape[0] // 2
    return jnp.concatenate([x[:half], x[half:]], axis=1)


def masks():
    shape = (2 * BLOCK, 2 * BLOCK)
    i, j = iota(shape, 0), iota(shape, 1)
    same = (i // BLOCK) == (j // BLOCK)
    return same & (i >= j), same & (i < j)


class Piece:
    def __init__(self, b, q_ref, k_ref, v_ref, fd_ref, bd_ref):
        rows = pl.ds(b * BLOCK, BLOCK)
        shape = (BLOCK, BLOCK)
        lower = (iota(shape, 0) >= iota(shape, 1)).astype(F32)
        upper = (iota(shape, 0) <= iota(shape, 1)).astype(F32)
        self.q = q_ref[rows, :].astype(F32) * KEY_CHANNELS**-0.5
        self.k = k_ref[rows, :].astype(F32)
        self.vs = heads_on_rows(v_ref[rows, :])
        self.g = dot_exact(lower, fd_ref[rows, :])
        self.h = dot_exact(upper, bd_ref[rows, :])
        self.last = self.g[BLOCK - 1 :, :]
        self.first = self.h[:1, :]
        self.mid_g = self.g[BLOCK // 2 - 1 : BLOCK // 2, :]
        self.mid_h = self.h[BLOCK // 2 : BLOCK // 2 + 1, :]

    def ends(self):
        self.eg_end = jnp.exp(self.last - self.g)
        self.eh_end = jnp.exp(self.first - self.h)
        self.kg_end = stacked(self.k * self.eg_end).astype(BF16)
        self.kh_end = stacked(self.k * self.eh_end).astype(BF16)
        self.fresh_f = dot(self.vs, self.kg_end, TN)
        self.fresh_b = dot(self.vs, self.kh_end, TN)

    def entries(self):
        self.eg = jnp.exp(self.g)
        self.eh = jnp.exp(self.h)
        self.qg = stacked(self.q * self.eg).astype(BF16)
        self.qh = stacked(self.q * self.eh).astype(BF16)

    def scores(self, inclusive, strict):
        self.up_g = jnp.exp(self.g - self.mid_g)
        self.dn_g = jnp.exp(self.mid_g - self.g)
        self.up_h = jnp.exp(self.h - self.mid_h)
        self.dn_h = jnp.exp(self.mid_h - self.h)
        self.q_up_g = stacked(self.q * self.up_g).astype(BF16)
        self.k_dn_g = stacked(self.k * self.dn_g).astype(BF16)
        self.q_up_h = stacked(self.q * self.up_h).astype(BF16)
        self.k_dn_h = stacked(self.k * self.dn_h).astype(BF16)
        a_f = jnp.where(inclusive, dot(self.q_up_g, self.k_dn_g, NT), 0.0)
        a_b = jnp.where(strict, dot(self.q_up_h, self.k_dn_h, NT), 0.0)
        return (a_f + a_b).astype(BF16)


def both_states(pieces, forward_entry, backward_entry):
    s, before = forward_entry, []
    for piece in pieces:
        before.append(s)
        s = jnp.exp(piece.last) * s + piece.fresh_f
    r, after = backward_entry, [None] * len(pieces)
    for b in reversed(range(len(pieces))):
        after[b] = r
        r = jnp.exp(pieces[b].first) * r + pieces[b].fresh_b
    return before, after, s, r


def position():
    z, y, c = (lax.axis_index(a) for a in SP)
    return z, y, c, y * 2 + c


def plane_peer(p, d, planes):
    other = lax.rem(p + d, planes)
    return other, {"sp_1": other // 2, "sp_2": lax.rem(other, 2)}


def greet(planes, depth):
    z, _, _, p = position()
    barrier = pltpu.get_barrier_semaphore()
    for d in range(1, planes):
        _, device = plane_peer(p, d, planes)
        pl.semaphore_signal(barrier, 1, device_id=device, device_id_type=pl.DeviceIdType.MESH)
    for d in range(1, depth):
        device = {"sp_0": lax.rem(z + d, depth)}
        pl.semaphore_signal(barrier, 1, device_id=device, device_id_type=pl.DeviceIdType.MESH)
    return barrier, planes + depth - 2


class Carry:
    SCRATCH_PLANES, SCRATCH_DEPTH = 8, 8

    @classmethod
    def scratch(cls):
        n, m = cls.SCRATCH_PLANES, cls.SCRATCH_DEPTH
        return [
            pltpu.VMEM((n, 2, ROWS, 128), F32),
            pltpu.VMEM((n, 2, ROWS, 128), F32),
            pltpu.VMEM((2, ROWS, 128), F32),
            pltpu.VMEM((m, ROWS, 128), F32),
            pltpu.VMEM((n, 2, PIECE, 128), F32),
            pltpu.VMEM((n, 2, PIECE, 128), F32),
            pltpu.SemaphoreType.DMA((n,)),
            pltpu.SemaphoreType.DMA((n,)),
            pltpu.SemaphoreType.DMA((m,)),
            pltpu.SemaphoreType.DMA((m,)),
            pltpu.SemaphoreType.DMA((n,)),
            pltpu.SemaphoreType.DMA((n,)),
        ]

    def __init__(self, refs):
        (
            self.out1,
            self.in1,
            self.out2,
            self.in2,
            self.out3,
            self.in3,
            self.s1,
            self.r1,
            self.s2,
            self.r2,
            self.s3,
            self.r3,
        ) = refs
        self.n, self.m = self.SCRATCH_PLANES, self.SCRATCH_DEPTH
        self.z, _, _, self.p = position()

    def plane_copy(self, out, into, send, recv, d, arriving=False):
        other, device = plane_peer(self.p, d, self.n)
        at = other if arriving else self.p
        return pltpu.make_async_remote_copy(
            src_ref=out.at[other],
            dst_ref=into.at[at],
            send_sem=send.at[other],
            recv_sem=recv.at[at],
            device_id=device,
            device_id_type=pl.DeviceIdType.MESH,
        )

    def start(self, terms, logs):
        for dim in range(2):
            decay = jnp.broadcast_to(logs[dim], (8, 128))
            for j in range(self.n):
                self.out1[j, dim, :PIECE, :] = terms[dim][j * PIECE : (j + 1) * PIECE, :]
                self.out1[j, dim, PIECE:, :] = decay
        for d in range(1, self.n):
            self.plane_copy(self.out1, self.in1, self.s1, self.r1, d).start()
        self.in1[self.p] = self.out1[self.p]

    def middle(self):
        for d in range(1, self.n):
            self.plane_copy(self.out1, self.in1, self.s1, self.r1, d, True).wait_recv()
        zero = jnp.zeros((PIECE, 128), F32)
        none = jnp.zeros((1, 128), F32)
        self.before = [[None] * self.n, [None] * self.n]
        for dim in range(2):
            total, log = zero, none
            for i in range(self.n) if dim == 0 else reversed(range(self.n)):
                self.before[dim][i] = (total, log)
                step = self.in1[i, dim, PIECE : PIECE + 1, :]
                total = total * jnp.exp(step) + self.in1[i, dim, :PIECE, :]
                log = log + step
            self.out2[dim, :PIECE, :] = total
            self.out2[dim, PIECE:, :] = jnp.broadcast_to(log, (8, 128))
        for d in range(1, self.m):
            self.depth_copy(d).start()

    def depth_copy(self, d, arriving=False):
        other = lax.rem(self.z + d, self.m)
        dim = jnp.where(other > self.z, 0, 1)
        at = other if arriving else self.z
        return pltpu.make_async_remote_copy(
            src_ref=self.out2.at[dim],
            dst_ref=self.in2.at[at],
            send_sem=self.s2.at[other],
            recv_sem=self.r2.at[at],
            device_id={"sp_0": other},
            device_id_type=pl.DeviceIdType.MESH,
        )

    def last(self):
        self.in2[self.z] = jnp.zeros((ROWS, 128), F32)
        for d in range(1, self.m):
            self.depth_copy(d, True).wait_recv()
        entry = []
        for dim in range(2):
            total = jnp.zeros((PIECE, 128), F32)
            for i in range(self.m) if dim == 0 else reversed(range(self.m)):
                passed = (i < self.z) if dim == 0 else (i > self.z)
                step = self.in2[i, PIECE : PIECE + 1, :]
                total = jnp.where(passed, total * jnp.exp(step) + self.in2[i, :PIECE, :], total)
            entry.append(total)
        for i in range(self.n):
            for dim in range(2):
                inside, log = self.before[dim][i]
                self.out3[i, dim] = inside + jnp.exp(log) * entry[dim]
        for d in range(1, self.n):
            self.plane_copy(self.out3, self.in3, self.s3, self.r3, d).start()
        self.in3[self.p] = self.out3[self.p]

    def finish(self):
        for d in range(1, self.n):
            self.plane_copy(self.out3, self.in3, self.s3, self.r3, d, True).wait_recv()
        for d in range(1, self.n):
            self.plane_copy(self.out1, self.in1, self.s1, self.r1, d).wait_send()
            self.plane_copy(self.out3, self.in3, self.s3, self.r3, d).wait_send()
        for d in range(1, self.m):
            self.depth_copy(d).wait_send()
        return [self.in3[:, dim].reshape(128, 128) for dim in range(2)]


OFFSETS = (0, 7, 3, 4, 5, 2, 6, 1)
AWAY = tuple(i for i, offset in enumerate(OFFSETS) if offset)
OWN = OFFSETS.index(0)
SCHEDULE = (
    ((0, 0), (0, 1), (1, 0), (1, 1), (0, 2), (2, 0), (2, 1), (0, 3), (0, 4), (1, 2), (0, 8))
    + ((0, 7), (0, 6), (1, 3), (0, 5), (1, 4), (2, 2), (1, 6), (2, 3), (1, 5), (3, 1), (2, 4))
    + ((3, 2), (3, 3), (1, 7), (2, 5), (1, 8), (4, 1), (3, 4), (2, 6), (4, 2), (2, 8), (4, 3))
    + ((2, 7), (4, 4), (3, 5), (3, 6), (3, 0), (3, 7), (4, 5), (4, 6), (4, 0), (4, 7))
)
PLANE_ORDER = (2, 6, 3, 7, 4, 5, 1)
PLANES, DEPTH, RING = 8, 8, 4
CHUNK = PLANES * CAP
MESH = pl.DeviceIdType.MESH


def remote(src, dst, sems, device):
    return pltpu.make_async_remote_copy(
        src_ref=src,
        dst_ref=dst,
        send_sem=sems[0],
        recv_sem=sems[1],
        device_id=device,
        device_id_type=MESH,
    )


def swap_matrix(shape):
    i = iota((shape[0], 1), 0)
    a = (i * 911) >> 16
    rest = i - a * CHUNK
    b = (rest * 7282) >> 16
    source = b * CHUNK + a * CAP + (rest - b * CAP)
    return jnp.where(source == iota(shape, 1), 1.0, 0.0).astype(BF16)


def layer_kernel(
    routes,
    route_weight,
    layer_grad,
    slot_tokens,
    gate_proj,
    up_proj,
    down_proj,
    out_proj,
    q_hbm,
    k_hbm,
    v_hbm,
    fd_hbm,
    bd_hbm,
    gate_grad_ref,
    up_grad_ref,
    down_grad_ref,
    proj_ref,
    dq_ref,
    dk_ref,
    dv_ref,
    q,
    k,
    v,
    fd,
    bd,
    own,
    x,
    w_cat,
    down_out,
    down_in,
    w_out,
    choice,
    choice_t,
    swap,
    act,
    silu,
    slope,
    delta,
    out_plane,
    in_plane,
    out_depth,
    inbound,
    first_part,
    first_hop,
    first_hopped,
    first_both,
    first_plain,
    part,
    hop,
    hopped,
    both,
    plain,
    ret_out,
    ret_in,
    back_out,
    back_in,
    stream,
    terms,
    core_in,
    core_sum,
    row_in,
    row_sum,
    depth_in,
    send,
    recv,
    load,
    *carry_refs,
):
    z, y, c, p = position()
    t = lax.axis_index("tp")
    right, left, across = lax.rem(t + 1, RING), lax.rem(t + 3, RING), lax.rem(t + 2, RING)
    quarter = own.shape[1]
    barrier, count = greet(PLANES, DEPTH)
    for other in (left, right, across):
        pl.semaphore_signal(barrier, 1, device_id={"tp": other}, device_id_type=MESH)

    columns = pl.ds(pl.multiple_of(t * quarter, quarter), quarter)
    hidden = down_in.shape[1]
    loads = [
        pltpu.make_async_copy(layer_grad.at[:, columns], own, load.at[0]),
        pltpu.make_async_copy(slot_tokens.at[0], x, load.at[1]),
        pltpu.make_async_copy(gate_proj.at[0], w_cat.at[:, pl.ds(0, hidden)], load.at[2]),
        pltpu.make_async_copy(up_proj.at[0], w_cat.at[:, pl.ds(hidden, hidden)], load.at[3]),
        pltpu.make_async_copy(down_proj.at[0, :, columns], down_in.at[t], load.at[4]),
        pltpu.make_async_copy(out_proj, w_out, load.at[5]),
    ]
    for n, (source, to) in enumerate(
        ((q_hbm, q), (k_hbm, k), (v_hbm, v), (fd_hbm, fd), (bd_hbm, bd))
    ):
        loads.append(pltpu.make_async_copy(source, to, load.at[6 + n]))
    for n in range(1, RING):
        other = lax.rem(t + n, RING)
        there = pl.ds(pl.multiple_of(other * quarter, quarter), quarter)
        loads.append(
            pltpu.make_async_copy(
                down_proj.at[0, :, there], down_out.at[other], load.at[10 + n]
            )
        )
    for copy in (loads[0], *loads[11:], *loads[6:11], *loads[1:6]):
        copy.start()

    def sems(kind, i):
        return send.at[kind, i], recv.at[kind, i]

    def plane_out(kind, out, into, d):
        other, device = plane_peer(p, d, PLANES)
        return remote(out.at[other], into.at[p], sems(kind, d), device)

    def plane_in(kind, out, into, d):
        other, device = plane_peer(p, PLANES - d, PLANES)
        return remote(out.at[other], into.at[other], sems(kind, d), device)

    tokens = own.shape[0]
    slots = x.shape[0]
    names = iota((128, tokens), 0)
    members = [(routes[j : j + 1, :] == names).astype(F32) for j in range(2)]
    shape = (tokens, tokens)
    later = (iota(shape, 0) < iota(shape, 1)).astype(BF16)
    before = dot(members[0] + members[1], later)
    scale = jnp.zeros((slots, 1), F32)
    chosen = jnp.zeros((slots, tokens), F32)
    for j in range(2):
        rank = jnp.sum((before + members[0] * j) * members[j], axis=0, keepdims=True)
        rank = rank.astype(jnp.int32)
        expert = routes[j : j + 1, :]
        row = (expert & (PLANES - 1)) * CHUNK + (expert >> 3) * CAP + rank
        row = jnp.where(rank < CAP, row, -1)
        taken = row == iota((slots, tokens), 0)
        chosen = jnp.where(taken, 1.0, chosen)
        given = jnp.where(taken, route_weight[j : j + 1, :], 0.0)
        scale = scale + jnp.sum(given, axis=1, keepdims=True)
    choice[...] = chosen.astype(BF16)
    loads[0].wait()
    picked = dot(choice[...], own[...]) * scale
    out_plane[...] = picked.astype(BF16).reshape(out_plane.shape)
    pl.semaphore_wait(barrier, count + 3)
    for d in PLANE_ORDER:
        plane_out(0, out_plane, in_plane, d).start()
    in_plane[p] = out_plane[p]

    def down_copy(n, arriving=False):
        other = lax.rem(t + (RING - n if arriving else n), RING)
        at = other if arriving else t
        return remote(down_out.at[other], down_in.at[at], sems(14, n), {"tp": other})

    for copy in loads[11:]:
        copy.wait()
    for n in (2, 1, 3):
        down_copy(n).start()

    for copy in loads[6:11]:
        copy.wait()
    pieces = [Piece(b, q, k, v, fd, bd) for b in range(3)]
    for piece in pieces:
        piece.ends()
    zero = jnp.zeros((DV, 128), F32)
    _, _, forward_end, backward_end = both_states(pieces, zero, zero)
    log_f = sum(piece.last for piece in pieces)
    log_b = sum(piece.first for piece in pieces)
    carry = Carry(carry_refs[:12])
    carry.start((forward_end, backward_end), (log_f, log_b))
    swap[...] = swap_matrix(swap.shape)
    choice_t[...] = choice[...].T

    def chunk_of(i):
        return lax.rem(z + OFFSETS[i], DEPTH)

    def spread(i, arriving=False):
        at = chunk_of(i)
        a, b = (left, right) if arriving else (t, t)
        return (
            remote(inbound.at[a, at], inbound.at[a, at], sems(2, i), {"tp": right}),
            remote(inbound.at[b, at], inbound.at[b, at], sems(3, i), {"tp": left}),
        )

    def sides(i):
        return (left, right) if i % 2 == 0 else (right, left)

    def pass_on(i, arriving=False):
        source, to = sides(i)
        at, which = chunk_of(i), across if arriving else source
        return remote(inbound.at[which, at], inbound.at[which, at], sems(4, i), {"tp": to})

    def send_hop(i):
        _, to = sides(i)
        return remote(part.at[i, across], hop.at[i], sems(5, i), {"tp": to})

    def send_both(i):
        _, to = sides(i)
        return remote(hopped.at[i], both.at[i], sems(6, i), {"tp": to})

    def send_plain(i):
        to, _ = sides(i)
        return remote(part.at[i, to], plain.at[i], sems(7, i), {"tp": to})

    def send_back(i, arriving=False):
        at = lax.rem(z + DEPTH - OFFSETS[i], DEPTH) if arriving else z
        other = chunk_of(i)
        return remote(ret_out.at[other], ret_in.at[at], sems(8, i), {"sp_0": other})

    def first_send_hop(i):
        _, to = sides(i)
        return remote(first_part.at[i, across], first_hop.at[i], sems(15, i), {"tp": to})

    def first_send_both(i):
        _, to = sides(i)
        return remote(first_hopped.at[i], first_both.at[i], sems(16, i), {"tp": to})

    def first_send_plain(i):
        to, _ = sides(i)
        return remote(first_part.at[i, to], first_plain.at[i], sems(17, i), {"tp": to})

    def stage_0(i):
        at = chunk_of(i)
        if i != OWN:
            remote(out_depth.at[at], inbound.at[t, at], sems(1, i), {"sp_0": at}).wait_recv()
        partial = dot(inbound[t, at], down_in[...].reshape(RING * hidden, quarter), NT)
        for n in range(RING):
            first_part[i, n] = partial[:, n * hidden : (n + 1) * hidden].astype(BF16)
        first_send_hop(i).start()
        first_send_plain(i).start()

    def stage_1(i):
        _, to = sides(i)
        first_send_hop(i).wait_recv()
        total = first_hop[i].astype(F32) + first_part[i, to].astype(F32)
        first_hopped[i] = total.astype(BF16)
        first_send_both(i).start()

    def stage_2(i):
        at = chunk_of(i)
        first_send_both(i).wait_recv()
        first_send_plain(i).wait_recv()
        total = first_part[i, t].astype(F32) + first_both[i].astype(F32)
        total = total + first_plain[i].astype(F32)
        up_delta = (total * silu[at]).astype(BF16)
        gate_delta = (total * slope[at]).astype(BF16)
        deltas = jnp.concatenate([gate_delta, up_delta], axis=1)
        delta[at] = deltas
        _, to = sides(i)
        for n, which in enumerate((across, sides(i)[0], to, t)):
            rows = pl.ds(pl.multiple_of(which * quarter, quarter), quarter)
            part[i, which] = dot(deltas, w_cat[rows, :], NT).astype(BF16)
            if n == 0:
                send_hop(i).start()
            if n == 1:
                send_plain(i).start()

    def stage_3(i):
        _, to = sides(i)
        send_hop(i).wait_recv()
        hopped[i] = (hop[i].astype(F32) + part[i, to].astype(F32)).astype(BF16)
        send_both(i).start()

    def stage_4(i):
        at = chunk_of(i)
        send_both(i).wait_recv()
        send_plain(i).wait_recv()
        total = part[i, t].astype(F32) + both[i].astype(F32) + plain[i].astype(F32)
        if i == OWN:
            ret_in[z] = total.astype(BF16)
        else:
            ret_out[at] = total.astype(BF16)
            send_back(i).start()

    for d in PLANE_ORDER:
        plane_in(0, out_plane, in_plane, d).wait_recv()
    moved = dot(swap[...], in_plane[...].reshape(DEPTH * CHUNK, quarter)).astype(BF16)
    out_depth[...] = moved.reshape(out_depth.shape)

    def depth_out(i):
        other = lax.rem(z + DEPTH - OFFSETS[i], DEPTH)
        return remote(out_depth.at[other], inbound.at[t, z], sems(1, i), {"sp_0": other})

    inbound[t, z] = out_depth[z]
    for i in AWAY:
        depth_out(i).start()

    for copy in loads[1:4]:
        copy.wait()
    half = x.shape[0] // 2
    for j in range(2):
        rows = pl.ds(j * half, half)
        chunks = pl.ds(j * (DEPTH // 2), DEPTH // 2)
        both_up = jnp.dot(x[rows, :], w_cat[...], preferred_element_type=F32)
        gate, up = both_up[:, :hidden], both_up[:, hidden:]
        sigma = jax.nn.sigmoid(gate)
        s = gate * sigma
        shape = (DEPTH // 2, CHUNK, hidden)
        silu[chunks] = s.reshape(shape)
        act[chunks] = (s * up).astype(BF16).reshape(shape)
        slope[chunks] = (up * sigma * (1.0 + gate * (1.0 - sigma))).reshape(shape)
    loads[4].wait()
    for n in range(1, RING):
        down_copy(n, True).wait_recv()

    def attend(step):
        if step == 0:
            carry.middle()
        elif step == 1:
            inclusive, strict = masks()
            for piece in pieces:
                piece.a = piece.scores(inclusive, strict)
                piece.inner = dot(piece.a, piece.vs)
                piece.entries()
        else:
            carry.last()

    stages = (stage_0, stage_1, stage_2, stage_3, stage_4)
    for stage, i in SCHEDULE:
        if i == DEPTH:
            attend(stage)
        else:
            stages[stage](i)

    for i in range(DEPTH):
        for copy in spread(i):
            copy.start()

    forward_entry, backward_entry = carry.finish()
    before, after, _, _ = both_states(pieces, forward_entry, backward_entry)
    for b, piece in enumerate(pieces):
        piece.states = jnp.concatenate([before[b], after[b]], axis=1).astype(BF16)
        o = piece.inner + dot(jnp.concatenate([piece.qg, piece.qh], axis=1), piece.states, NT)
        piece.inv = lax.rsqrt(jnp.mean(o * o, axis=1, keepdims=True) + EPSILON)
        piece.mixed = o * piece.inv

    for i in AWAY:
        send_back(i, True).wait_recv()
    moved = dot(swap[...], ret_in[...].reshape(DEPTH * CHUNK, quarter)).astype(BF16)
    back_out[...] = moved.reshape(back_out.shape)
    for d in PLANE_ORDER:
        plane_out(9, back_out, back_in, d).start()
    back_in[p] = back_out[p]
    deltas = delta[...].reshape(DEPTH * CHUNK, 2 * hidden)
    for n in range(RING):
        both_grads = dot(x[:, n * quarter : (n + 1) * quarter], deltas, TN)
        rows = pl.ds(n * quarter, quarter)
        gate_grad_ref[rows, :] = both_grads[:, :hidden].astype(BF16)
        up_grad_ref[rows, :] = both_grads[:, hidden:].astype(BF16)
    for d in PLANE_ORDER:
        plane_in(9, back_out, back_in, d).wait_recv()
    moe_grad = dot(choice_t[...], back_in[...].reshape(DEPTH * CHUNK, quarter))
    stream[t] = (own[...].astype(F32) + moe_grad).astype(BF16)

    low, high = pl.ds(0, tokens // 2), pl.ds(tokens // 2, tokens // 2)

    def ring(kind, which, rows, to):
        pair = sems(kind, 0 if kind in (0, 9) else OWN)
        return remote(stream.at[which, rows], stream.at[which, rows], pair, {"tp": to})

    def stream_spread():
        return (
            ring(0, t, low, right),
            ring(1, t, high, left),
            ring(8, t, high, right),
            ring(9, t, low, left),
        )

    def stream_arrived():
        return (
            ring(0, left, low, right),
            ring(1, right, high, left),
            ring(8, left, high, right),
            ring(9, right, low, left),
        )

    def stream_pass(which_low, which_high):
        return (
            remote(
                stream.at[which_low, low], stream.at[which_low, low], sems(10, 0), {"tp": right}
            ),
            remote(
                stream.at[which_high, high], stream.at[which_high, high], sems(11, 0), {"tp": left}
            ),
        )

    for copy in stream_spread():
        copy.start()
    loads[5].wait()

    def share(which):
        rows = pl.ds(pl.multiple_of(which * quarter, quarter), quarter)
        return jnp.dot(stream[which], w_out[rows, :], preferred_element_type=F32)

    mixed_grad = share(t)
    onward = stream_pass(left, right)
    for n, copy in enumerate(stream_arrived()):
        copy.wait_recv()
        if n < 2:
            onward[n].start()
    mixed_grad = mixed_grad + share(left) + share(right)
    for copy in stream_pass(across, across):
        copy.wait_recv()
    mixed_grad = mixed_grad + share(across)

    back_c, back_d = jnp.zeros((DV, 128), F32), jnp.zeros((DV, 128), F32)
    for b, piece in enumerate(pieces):
        mg = heads_on_rows(mixed_grad[b * BLOCK : (b + 1) * BLOCK, :])
        mean = jnp.mean(mg * piece.mixed, axis=1, keepdims=True)
        piece.do = (piece.inv * (mg - piece.mixed * mean)).astype(BF16)
        piece.back_f = dot(piece.do, piece.qg, TN)
        piece.back_b = dot(piece.do, piece.qh, TN)
    for piece in pieces:
        back_c = back_c * jnp.exp(piece.first) + piece.back_b
    for piece in reversed(pieces):
        back_d = back_d * jnp.exp(piece.last) + piece.back_f
    carry = Carry(carry_refs[12:])
    carry.start((back_c, back_d), (log_b, log_f))

    rows_of_mixed = jnp.concatenate([heads_on_lanes(piece.mixed) for piece in pieces], axis=0)
    rows_of_mixed = rows_of_mixed.astype(BF16)
    piece_rows = proj_ref.shape[0]
    for n in range(RING):
        term = dot(stream[n], rows_of_mixed, TN).astype(BF16)
        per = term.shape[0] // (piece_rows * PLANES)
        term = term.reshape(per, 4, 2, piece_rows, term.shape[1])
        for cc in range(2):
            for zz in range(per):
                terms[cc, :, n * per + zz] = term[zz, :, cc]

    def core_copy():
        return remote(terms.at[1 - c], core_in, sems(12, 0), {"sp_2": 1 - c})

    def row_copy(d, arriving=False):
        other = lax.rem(y + (4 - d if arriving else d), 4)
        at = other if arriving else y
        return remote(core_sum.at[other], row_in.at[at], sems(12, d), {"sp_1": other})

    def last_copy(d, arriving=False):
        other = lax.rem(z + (DEPTH - d if arriving else d), DEPTH)
        at = other if arriving else z
        return remote(row_sum.at[other], depth_in.at[at], sems(13, d), {"sp_0": other})

    core_copy().start()
    core_copy().wait_recv()
    core_sum[...] = (terms[c].astype(F32) + core_in[...].astype(F32)).astype(BF16)
    for d in (2, 1, 3):
        row_copy(d).start()
    for i in range(DEPTH):
        for copy in spread(i, True):
            copy.wait_recv()
        pass_on(i).start()

    inclusive, strict = masks()
    for piece in pieces:
        da = dot(piece.do, piece.vs, NT)
        da_f = jnp.where(inclusive, da, 0.0).astype(BF16)
        da_b = jnp.where(strict, da, 0.0).astype(BF16)
        piece.dv = dot(piece.a, piece.do, TN)
        piece.dq = dot(da_f, piece.k_dn_g) * doubled(piece.up_g) + dot(
            da_b, piece.k_dn_h
        ) * doubled(piece.up_h)
        piece.dk = dot(da_f, piece.q_up_g, TN) * doubled(piece.dn_g) + dot(
            da_b, piece.q_up_h, TN
        ) * doubled(piece.dn_h)
    carry.middle()
    for b, piece in enumerate(pieces):
        dq = dot(piece.do, piece.states)
        dq = piece.dq + dq[:, :128] * stacked(piece.eg) + dq[:, 128:] * stacked(piece.eh)
        dq_ref[pl.ds(b * BLOCK, BLOCK), :] = (folded(dq) * KEY_CHANNELS**-0.5).astype(BF16)
    carry.last()
    for d in (1, 3, 2):
        row_copy(d, True).wait_recv()
    row_in[y] = core_sum[y]
    total = row_in[0].astype(F32)
    for n in range(1, 4):
        total = total + row_in[n].astype(F32)
    row_sum[...] = total.astype(BF16)
    for d in (4, 3, 5, 2, 6, 1, 7):
        last_copy(d).start()
    for i in range(DEPTH):
        pass_on(i, True).wait_recv()
    act_all = act[...].reshape(DEPTH * CHUNK, hidden)
    for n in range(RING):
        rows = inbound[n].reshape(DEPTH * CHUNK, quarter)
        down_grad_ref[:, n * quarter : (n + 1) * quarter] = dot(act_all, rows, TN).astype(BF16)
    back_c, back_d = carry.finish()
    late, early = [None] * 3, [None] * 3
    for b, piece in enumerate(pieces):
        early[b] = back_c
        back_c = back_c * jnp.exp(piece.first) + piece.back_b
    for b in reversed(range(3)):
        late[b] = back_d
        back_d = back_d * jnp.exp(pieces[b].last) + pieces[b].back_f
    for b, piece in enumerate(pieces):
        states = jnp.concatenate([late[b], early[b]], axis=1).astype(BF16)
        dk = dot(piece.vs, states)
        dk = piece.dk + dk[:, :128] * stacked(piece.eg_end) + dk[:, 128:] * stacked(piece.eh_end)
        dv = piece.dv + dot(jnp.concatenate([piece.kg_end, piece.kh_end], axis=1), states, NT)
        rows = pl.ds(b * BLOCK, BLOCK)
        dk_ref[rows, :] = folded(dk).astype(BF16)
        dv_ref[rows, :] = heads_on_lanes(dv).astype(BF16)
    depth_in[z] = row_sum[z]
    for d in range(1, DEPTH):
        last_copy(d, True).wait_recv()
    total = depth_in[0].astype(F32)
    for n in range(1, DEPTH):
        total = total + depth_in[n].astype(F32)
    proj_ref[...] = total

    for d in PLANE_ORDER:
        plane_out(0, out_plane, in_plane, d).wait_send()
        plane_out(9, back_out, back_in, d).wait_send()
    for i in range(DEPTH):
        if i != OWN:
            depth_out(i).wait_send()
            send_back(i).wait_send()
        for copy in (*spread(i), pass_on(i), send_hop(i), send_both(i), send_plain(i)):
            copy.wait_send()
        for copy in (first_send_hop(i), first_send_both(i), first_send_plain(i)):
            copy.wait_send()
    for n in range(1, RING):
        down_copy(n).wait_send()
    for copy in (*stream_spread(), *stream_pass(left, right), core_copy()):
        copy.wait_send()
    for d in (1, 2, 3):
        row_copy(d).wait_send()
    for d in range(1, DEPTH):
        last_copy(d).wait_send()


def vmem(n):
    return [pl.BlockSpec(memory_space=pltpu.VMEM)] * n


def layer(*arrays):
    layer_grad, slot_tokens, gate = arrays[2], arrays[3], arrays[4]
    tokens, width = layer_grad.shape
    slots = slot_tokens.shape[1]
    quarter = width // RING
    hidden = gate.shape[2]
    out_columns = arrays[7].shape[1]
    piece_rows = width // (DEPTH * PLANES)
    rows = (DEPTH, CHUNK, quarter)
    anywhere = pl.BlockSpec(memory_space=pl.ANY)
    return pl.pallas_call(
        layer_kernel,
        out_shape=(
            pltpu.VMEM((width, hidden), BF16),
            pltpu.VMEM((width, hidden), BF16),
            pltpu.VMEM((hidden, width), BF16),
            pltpu.VMEM((piece_rows, out_columns), F32),
            pltpu.VMEM((tokens, 128), BF16),
            pltpu.VMEM((tokens, 128), BF16),
            pltpu.VMEM((tokens, 2 * DV), BF16),
        ),
        in_specs=vmem(2) + [anywhere] * 11,
        out_specs=tuple(vmem(7)),
        scratch_shapes=[
            *[pltpu.VMEM(a.shape, a.dtype) for a in arrays[8:]],
            pltpu.VMEM((tokens, quarter), BF16),
            pltpu.VMEM((slots, width), BF16),
            pltpu.VMEM((width, 2 * hidden), BF16),
            pltpu.VMEM((RING, hidden, quarter), BF16),
            pltpu.VMEM((RING, hidden, quarter), BF16),
            pltpu.VMEM((width, out_columns), BF16),
            pltpu.VMEM((slots, tokens), BF16),
            pltpu.VMEM((tokens, slots), BF16),
            pltpu.VMEM((slots, slots), BF16),
            pltpu.VMEM((DEPTH, CHUNK, hidden), BF16),
            pltpu.VMEM((DEPTH, CHUNK, hidden), F32),
            pltpu.VMEM((DEPTH, CHUNK, hidden), F32),
            pltpu.VMEM((DEPTH, CHUNK, 2 * hidden), BF16),
            pltpu.VMEM(rows, BF16),
            pltpu.VMEM(rows, BF16),
            pltpu.VMEM(rows, BF16),
            pltpu.VMEM((RING, *rows), BF16),
            pltpu.VMEM((DEPTH, RING, CHUNK, hidden), BF16),
            *[pltpu.VMEM((DEPTH, CHUNK, hidden), BF16)] * 4,
            pltpu.VMEM((DEPTH, RING, CHUNK, quarter), BF16),
            *[pltpu.VMEM(rows, BF16)] * 8,
            pltpu.VMEM((RING, tokens, quarter), BF16),
            pltpu.VMEM((2, 4, DEPTH, piece_rows, out_columns), BF16),
            pltpu.VMEM((4, DEPTH, piece_rows, out_columns), BF16),
            pltpu.VMEM((4, DEPTH, piece_rows, out_columns), BF16),
            pltpu.VMEM((4, DEPTH, piece_rows, out_columns), BF16),
            pltpu.VMEM((DEPTH, piece_rows, out_columns), BF16),
            pltpu.VMEM((DEPTH, piece_rows, out_columns), BF16),
            pltpu.SemaphoreType.DMA((18, DEPTH)),
            pltpu.SemaphoreType.DMA((18, DEPTH)),
            pltpu.SemaphoreType.DMA((14,)),
            *Carry.scratch(),
            *Carry.scratch(),
        ],
        compiler_params=pltpu.CompilerParams(
            collective_id=0, has_side_effects=True, vmem_limit_bytes=56 * 2**20
        ),
        cost_estimate=pl.CostEstimate(
            flops=8 * 10**9, bytes_accessed=12 * 2**20, transcendentals=0
        ),
        name="layer",
    )(*arrays)


def write_kernel(*refs):
    n = len(refs) // 2
    done = refs[-1]
    copies = [pltpu.make_async_copy(refs[i], refs[n + i], done.at[i]) for i in range(n)]
    for copy in copies:
        copy.start()
    for copy in copies:
        copy.wait()


def written(arrays):
    n = len(arrays)
    arrays = [pltpu.with_memory_space_constraint(a, pltpu.VMEM) for a in arrays]
    return pl.pallas_call(
        write_kernel,
        out_shape=tuple(jax.ShapeDtypeStruct(a.shape, a.dtype) for a in arrays),
        in_specs=vmem(n),
        out_specs=(pl.BlockSpec(memory_space=pl.ANY),) * n,
        scratch_shapes=[pltpu.SemaphoreType.DMA((n,))],
        compiler_params=pltpu.CompilerParams(vmem_limit_bytes=2**20),
        name="write",
    )(*arrays)


def on_device(layer_grad, routes, route_weight, *arrays):
    results = written(layer(routes.T, route_weight.T, layer_grad, *arrays))
    gate, up, down, proj, query, key, value = results
    return gate[None], up[None], down[None], proj, query, key, value


def solution(mesh):
    torus = Mesh(mesh.devices.reshape(8, 4, 2, mesh.shape["tp"]), ("sp_0", "sp_1", "sp_2", "tp"))
    in_specs = (
        P(SP, None),
        P(SP, None),
        P(SP, None),
        P(SP, None, None),
        P(SP, None, "tp"),
        P(SP, None, "tp"),
        P(SP, "tp", None),
        P(None, "tp"),
        P(SP, "tp"),
        P(SP, "tp"),
        P(SP, "tp"),
        P(SP, "tp"),
        P(SP, "tp"),
    )
    out_specs = (
        P(SP, None, "tp"),
        P(SP, None, "tp"),
        P(SP, "tp", None),
        P(SP, "tp"),
        P(SP, "tp"),
        P(SP, "tp"),
        P(SP, "tp"),
    )
    return jax.shard_map(
        on_device, mesh=torus, in_specs=in_specs, out_specs=out_specs, check_vma=False
    )
```

```python
import jax
import jax.numpy as jnp
from jax import lax
from jax.experimental import pallas as pl
from jax.experimental.pallas import tpu as pltpu
from jax.sharding import Mesh
from jax.sharding import PartitionSpec as P

KEY_CHANNELS = 64
DV = 128
BLOCK = 64
SP = ("sp_0", "sp_1", "sp_2")
EPSILON = 1e-06
CAP = 9
F32 = jnp.float32
BF16 = jnp.bfloat16
PIECE = 16
ROWS = PIECE + 8


def dot(a, b, contract=((1,), (0,))):
    return lax.dot_general(
        a.astype(BF16), b.astype(BF16), (contract, ((), ())), preferred_element_type=F32
    )


def dot_exact(a, b):
    return lax.dot_general(
        a,
        b,
        (((1,), (0,)), ((), ())),
        precision=lax.Precision.HIGHEST,
        preferred_element_type=F32,
    )


NT = ((1,), (1,))
TN = ((0,), (0,))


def iota(shape, dim):
    return lax.broadcasted_iota(jnp.int32, shape, dim)


def stacked(x):
    low = iota(x.shape, 1) < KEY_CHANNELS
    zero = jnp.zeros_like(x)
    return jnp.concatenate([jnp.where(low, x, zero), jnp.where(low, zero, x)], axis=0)


def doubled(x):
    return jnp.concatenate([x, x], axis=0)


def folded(x):
    half = x.shape[0] // 2
    return x[:half] + x[half:]


def heads_on_rows(x):
    return jnp.concatenate([x[:, :DV], x[:, DV:]], axis=0)


def heads_on_lanes(x):
    half = x.shape[0] // 2
    return jnp.concatenate([x[:half], x[half:]], axis=1)


def masks():
    shape = (2 * BLOCK, 2 * BLOCK)
    i, j = iota(shape, 0), iota(shape, 1)
    same = (i // BLOCK) == (j // BLOCK)
    return same & (i >= j), same & (i < j)


class Piece:
    def __init__(self, b, q_ref, k_ref, v_ref, fd_ref, bd_ref):
        rows = pl.ds(b * BLOCK, BLOCK)
        shape = (BLOCK, BLOCK)
        lower = (iota(shape, 0) >= iota(shape, 1)).astype(F32)
        upper = (iota(shape, 0) <= iota(shape, 1)).astype(F32)
        self.q = q_ref[rows, :].astype(F32) * KEY_CHANNELS**-0.5
        self.k = k_ref[rows, :].astype(F32)
        self.vs = heads_on_rows(v_ref[rows, :])
        self.g = dot_exact(lower, fd_ref[rows, :])
        self.h = dot_exact(upper, bd_ref[rows, :])
        self.last = self.g[BLOCK - 1 :, :]
        self.first = self.h[:1, :]
        self.mid_g = self.g[BLOCK // 2 - 1 : BLOCK // 2, :]
        self.mid_h = self.h[BLOCK // 2 : BLOCK // 2 + 1, :]

    def ends(self):
        self.eg_end = jnp.exp(self.last - self.g)
        self.eh_end = jnp.exp(self.first - self.h)
        self.kg_end = stacked(self.k * self.eg_end).astype(BF16)
        self.kh_end = stacked(self.k * self.eh_end).astype(BF16)
        self.fresh_f = dot(self.vs, self.kg_end, TN)
        self.fresh_b = dot(self.vs, self.kh_end, TN)

    def entries(self):
        self.eg = jnp.exp(self.g)
        self.eh = jnp.exp(self.h)
        self.qg = stacked(self.q * self.eg).astype(BF16)
        self.qh = stacked(self.q * self.eh).astype(BF16)

    def scores(self, inclusive, strict):
        self.up_g = jnp.exp(self.g - self.mid_g)
        self.dn_g = jnp.exp(self.mid_g - self.g)
        self.up_h = jnp.exp(self.h - self.mid_h)
        self.dn_h = jnp.exp(self.mid_h - self.h)
        self.q_up_g = stacked(self.q * self.up_g).astype(BF16)
        self.k_dn_g = stacked(self.k * self.dn_g).astype(BF16)
        self.q_up_h = stacked(self.q * self.up_h).astype(BF16)
        self.k_dn_h = stacked(self.k * self.dn_h).astype(BF16)
        a_f = jnp.where(inclusive, dot(self.q_up_g, self.k_dn_g, NT), 0.0)
        a_b = jnp.where(strict, dot(self.q_up_h, self.k_dn_h, NT), 0.0)
        return (a_f + a_b).astype(BF16)


def both_states(pieces, forward_entry, backward_entry):
    s, before = forward_entry, []
    for piece in pieces:
        before.append(s)
        s = jnp.exp(piece.last) * s + piece.fresh_f
    r, after = backward_entry, [None] * len(pieces)
    for b in reversed(range(len(pieces))):
        after[b] = r
        r = jnp.exp(pieces[b].first) * r + pieces[b].fresh_b
    return before, after, s, r


def position():
    z, y, c = (lax.axis_index(a) for a in SP)
    return z, y, c, y * 2 + c


def plane_peer(p, d, planes):
    other = lax.rem(p + d, planes)
    return other, {"sp_1": other // 2, "sp_2": lax.rem(other, 2)}


def greet(planes, depth):
    z, _, _, p = position()
    barrier = pltpu.get_barrier_semaphore()
    for d in range(1, planes):
        _, device = plane_peer(p, d, planes)
        pl.semaphore_signal(barrier, 1, device_id=device, device_id_type=pl.DeviceIdType.MESH)
    for d in range(1, depth):
        device = {"sp_0": lax.rem(z + d, depth)}
        pl.semaphore_signal(barrier, 1, device_id=device, device_id_type=pl.DeviceIdType.MESH)
    return barrier, planes + depth - 2


class Carry:
    SCRATCH_PLANES, SCRATCH_DEPTH = 8, 8

    @classmethod
    def scratch(cls):
        n, m = cls.SCRATCH_PLANES, cls.SCRATCH_DEPTH
        return [
            pltpu.VMEM((n, 2, ROWS, 128), F32),
            pltpu.VMEM((n, 2, ROWS, 128), F32),
            pltpu.VMEM((2, ROWS, 128), F32),
            pltpu.VMEM((m, ROWS, 128), F32),
            pltpu.VMEM((n, 2, PIECE, 128), F32),
            pltpu.VMEM((n, 2, PIECE, 128), F32),
            pltpu.SemaphoreType.DMA((n,)),
            pltpu.SemaphoreType.DMA((n,)),
            pltpu.SemaphoreType.DMA((m,)),
            pltpu.SemaphoreType.DMA((m,)),
            pltpu.SemaphoreType.DMA((n,)),
            pltpu.SemaphoreType.DMA((n,)),
        ]

    def __init__(self, refs):
        (
            self.out1,
            self.in1,
            self.out2,
            self.in2,
            self.out3,
            self.in3,
            self.s1,
            self.r1,
            self.s2,
            self.r2,
            self.s3,
            self.r3,
        ) = refs
        self.n, self.m = self.SCRATCH_PLANES, self.SCRATCH_DEPTH
        self.z, _, _, self.p = position()

    def plane_copy(self, out, into, send, recv, d, arriving=False):
        other, device = plane_peer(self.p, d, self.n)
        at = other if arriving else self.p
        return pltpu.make_async_remote_copy(
            src_ref=out.at[other],
            dst_ref=into.at[at],
            send_sem=send.at[other],
            recv_sem=recv.at[at],
            device_id=device,
            device_id_type=pl.DeviceIdType.MESH,
        )

    def start(self, terms, logs):
        for dim in range(2):
            decay = jnp.broadcast_to(logs[dim], (8, 128))
            for j in range(self.n):
                self.out1[j, dim, :PIECE, :] = terms[dim][j * PIECE : (j + 1) * PIECE, :]
                self.out1[j, dim, PIECE:, :] = decay
        for d in PLANE_ORDER:
            self.plane_copy(self.out1, self.in1, self.s1, self.r1, d).start()
        self.in1[self.p] = self.out1[self.p]

    def middle(self):
        for d in range(1, self.n):
            self.plane_copy(self.out1, self.in1, self.s1, self.r1, d, True).wait_recv()
        zero = jnp.zeros((PIECE, 128), F32)
        none = jnp.zeros((1, 128), F32)
        self.before = [[None] * self.n, [None] * self.n]
        for dim in range(2):
            total, log = zero, none
            for i in range(self.n) if dim == 0 else reversed(range(self.n)):
                self.before[dim][i] = (total, log)
                step = self.in1[i, dim, PIECE : PIECE + 1, :]
                total = total * jnp.exp(step) + self.in1[i, dim, :PIECE, :]
                log = log + step
            self.out2[dim, :PIECE, :] = total
            self.out2[dim, PIECE:, :] = jnp.broadcast_to(log, (8, 128))
        for d in DEPTH_ORDER:
            self.depth_copy(d).start()

    def depth_copy(self, d, arriving=False):
        other = lax.rem(self.z + d, self.m)
        dim = jnp.where(other > self.z, 0, 1)
        at = other if arriving else self.z
        return pltpu.make_async_remote_copy(
            src_ref=self.out2.at[dim],
            dst_ref=self.in2.at[at],
            send_sem=self.s2.at[other],
            recv_sem=self.r2.at[at],
            device_id={"sp_0": other},
            device_id_type=pl.DeviceIdType.MESH,
        )

    def last(self):
        self.in2[self.z] = jnp.zeros((ROWS, 128), F32)
        for d in range(1, self.m):
            self.depth_copy(d, True).wait_recv()
        entry = []
        for dim in range(2):
            total = jnp.zeros((PIECE, 128), F32)
            for i in range(self.m) if dim == 0 else reversed(range(self.m)):
                passed = (i < self.z) if dim == 0 else (i > self.z)
                step = self.in2[i, PIECE : PIECE + 1, :]
                total = jnp.where(passed, total * jnp.exp(step) + self.in2[i, :PIECE, :], total)
            entry.append(total)
        for i in range(self.n):
            for dim in range(2):
                inside, log = self.before[dim][i]
                self.out3[i, dim] = inside + jnp.exp(log) * entry[dim]
        for d in PLANE_ORDER:
            self.plane_copy(self.out3, self.in3, self.s3, self.r3, d).start()
        self.in3[self.p] = self.out3[self.p]

    def finish(self):
        for d in range(1, self.n):
            self.plane_copy(self.out3, self.in3, self.s3, self.r3, d, True).wait_recv()
        for d in range(1, self.n):
            self.plane_copy(self.out1, self.in1, self.s1, self.r1, d).wait_send()
            self.plane_copy(self.out3, self.in3, self.s3, self.r3, d).wait_send()
        for d in range(1, self.m):
            self.depth_copy(d).wait_send()
        return [self.in3[:, dim].reshape(128, 128) for dim in range(2)]


OFFSETS = (0, 7, 3, 4, 5, 2, 6, 1)
AWAY = tuple(i for i, offset in enumerate(OFFSETS) if offset)
OWN = OFFSETS.index(0)
SCHEDULE = (
    ((0, 0), (0, 1), (1, 0), (1, 1), (0, 2), (2, 0), (2, 1), (0, 3), (0, 4), (1, 2), (0, 8))
    + ((0, 7), (0, 6), (1, 3), (0, 5), (1, 4), (2, 2), (1, 6), (2, 3), (1, 5), (3, 1), (2, 4))
    + ((3, 2), (3, 3), (1, 7), (2, 5), (1, 8), (4, 1), (3, 4), (2, 6), (4, 2), (2, 8), (4, 3))
    + ((2, 7), (4, 4), (3, 5), (3, 6), (3, 0), (3, 7), (4, 5), (4, 6), (4, 0), (4, 7))
)
PLANE_ORDER = (4, 5, 2, 6, 3, 7, 1)
DEPTH_ORDER = (4, 3, 5, 2, 6, 1, 7)
PLANES, DEPTH, RING = 8, 8, 4
CHUNK = PLANES * CAP
MESH = pl.DeviceIdType.MESH


def remote(src, dst, sems, device):
    return pltpu.make_async_remote_copy(
        src_ref=src,
        dst_ref=dst,
        send_sem=sems[0],
        recv_sem=sems[1],
        device_id=device,
        device_id_type=MESH,
    )


def swap_matrix(shape):
    i = iota((shape[0], 1), 0)
    a = (i * 911) >> 16
    rest = i - a * CHUNK
    b = (rest * 7282) >> 16
    source = b * CHUNK + a * CAP + (rest - b * CAP)
    return jnp.where(source == iota(shape, 1), 1.0, 0.0).astype(BF16)


def layer_kernel(
    routes,
    route_weight,
    layer_grad,
    slot_tokens,
    gate_proj,
    up_proj,
    down_proj,
    out_proj,
    q_hbm,
    k_hbm,
    v_hbm,
    fd_hbm,
    bd_hbm,
    gate_grad_ref,
    up_grad_ref,
    down_grad_ref,
    proj_ref,
    dq_ref,
    dk_ref,
    dv_ref,
    q,
    k,
    v,
    fd,
    bd,
    own,
    x,
    w_cat,
    down_out,
    down_in,
    w_out,
    choice,
    choice_t,
    swap,
    act,
    silu,
    slope,
    delta,
    out_plane,
    in_plane,
    out_depth,
    inbound,
    first_part,
    first_hop,
    first_hopped,
    first_both,
    first_plain,
    part,
    hop,
    hopped,
    both,
    plain,
    ret_out,
    ret_in,
    back_out,
    back_in,
    stream,
    terms,
    core_in,
    core_sum,
    row_in,
    row_sum,
    depth_in,
    send,
    recv,
    load,
    *carry_refs,
):
    z, y, c, p = position()
    t = lax.axis_index("tp")
    right, left, across = lax.rem(t + 1, RING), lax.rem(t + 3, RING), lax.rem(t + 2, RING)
    quarter = own.shape[1]
    barrier, count = greet(PLANES, DEPTH)
    for other in (left, right, across):
        pl.semaphore_signal(barrier, 1, device_id={"tp": other}, device_id_type=MESH)

    columns = pl.ds(pl.multiple_of(t * quarter, quarter), quarter)
    hidden = down_in.shape[1]
    loads = [
        pltpu.make_async_copy(layer_grad.at[:, columns], own, load.at[0]),
        pltpu.make_async_copy(slot_tokens.at[0], x, load.at[1]),
        pltpu.make_async_copy(gate_proj.at[0], w_cat.at[:, pl.ds(0, hidden)], load.at[2]),
        pltpu.make_async_copy(up_proj.at[0], w_cat.at[:, pl.ds(hidden, hidden)], load.at[3]),
        pltpu.make_async_copy(down_proj.at[0, :, columns], down_in.at[t], load.at[4]),
        pltpu.make_async_copy(out_proj, w_out, load.at[5]),
    ]
    for n, (source, to) in enumerate(
        ((q_hbm, q), (k_hbm, k), (v_hbm, v), (fd_hbm, fd), (bd_hbm, bd))
    ):
        loads.append(pltpu.make_async_copy(source, to, load.at[6 + n]))
    for n in range(1, RING):
        other = lax.rem(t + n, RING)
        there = pl.ds(pl.multiple_of(other * quarter, quarter), quarter)
        loads.append(
            pltpu.make_async_copy(
                down_proj.at[0, :, there], down_out.at[other], load.at[10 + n]
            )
        )
    for copy in (loads[0], *loads[11:], *loads[6:11], *loads[1:6]):
        copy.start()

    def sems(kind, i):
        return send.at[kind, i], recv.at[kind, i]

    def plane_out(kind, out, into, d):
        other, device = plane_peer(p, d, PLANES)
        return remote(out.at[other], into.at[p], sems(kind, d), device)

    def plane_in(kind, out, into, d):
        other, device = plane_peer(p, PLANES - d, PLANES)
        return remote(out.at[other], into.at[other], sems(kind, d), device)

    tokens = own.shape[0]
    slots = x.shape[0]
    names = iota((128, tokens), 0)
    members = [(routes[j : j + 1, :] == names).astype(F32) for j in range(2)]
    shape = (tokens, tokens)
    later = (iota(shape, 0) < iota(shape, 1)).astype(BF16)
    before = dot(members[0] + members[1], later)
    scale = jnp.zeros((slots, 1), F32)
    chosen = jnp.zeros((slots, tokens), F32)
    for j in range(2):
        rank = jnp.sum((before + members[0] * j) * members[j], axis=0, keepdims=True)
        rank = rank.astype(jnp.int32)
        expert = routes[j : j + 1, :]
        row = (expert & (PLANES - 1)) * CHUNK + (expert >> 3) * CAP + rank
        row = jnp.where(rank < CAP, row, -1)
        taken = row == iota((slots, tokens), 0)
        chosen = jnp.where(taken, 1.0, chosen)
        given = jnp.where(taken, route_weight[j : j + 1, :], 0.0)
        scale = scale + jnp.sum(given, axis=1, keepdims=True)
    choice[...] = chosen.astype(BF16)
    loads[0].wait()
    picked = dot(choice[...], own[...]) * scale
    out_plane[...] = picked.astype(BF16).reshape(out_plane.shape)
    pl.semaphore_wait(barrier, count + 3)
    for d in PLANE_ORDER:
        plane_out(0, out_plane, in_plane, d).start()
    in_plane[p] = out_plane[p]

    def down_copy(n, arriving=False):
        other = lax.rem(t + (RING - n if arriving else n), RING)
        at = other if arriving else t
        return remote(down_out.at[other], down_in.at[at], sems(14, n), {"tp": other})

    for copy in loads[11:]:
        copy.wait()
    for n in (2, 1, 3):
        down_copy(n).start()

    for copy in loads[6:11]:
        copy.wait()
    pieces = [Piece(b, q, k, v, fd, bd) for b in range(3)]
    for piece in pieces:
        piece.ends()
    zero = jnp.zeros((DV, 128), F32)
    _, _, forward_end, backward_end = both_states(pieces, zero, zero)
    log_f = sum(piece.last for piece in pieces)
    log_b = sum(piece.first for piece in pieces)
    carry = Carry(carry_refs[:12])
    carry.start((forward_end, backward_end), (log_f, log_b))
    swap[...] = swap_matrix(swap.shape)
    choice_t[...] = choice[...].T

    def chunk_of(i):
        return lax.rem(z + OFFSETS[i], DEPTH)

    def spread(i, arriving=False):
        at = chunk_of(i)
        a, b = (left, right) if arriving else (t, t)
        return (
            remote(inbound.at[a, at], inbound.at[a, at], sems(2, i), {"tp": right}),
            remote(inbound.at[b, at], inbound.at[b, at], sems(3, i), {"tp": left}),
        )

    def sides(i):
        return (left, right) if i % 2 == 0 else (right, left)

    def pass_on(i, arriving=False):
        source, to = sides(i)
        at, which = chunk_of(i), across if arriving else source
        return remote(inbound.at[which, at], inbound.at[which, at], sems(4, i), {"tp": to})

    def send_hop(i):
        _, to = sides(i)
        return remote(part.at[i, across], hop.at[i], sems(5, i), {"tp": to})

    def send_both(i):
        _, to = sides(i)
        return remote(hopped.at[i], both.at[i], sems(6, i), {"tp": to})

    def send_plain(i):
        to, _ = sides(i)
        return remote(part.at[i, to], plain.at[i], sems(7, i), {"tp": to})

    def send_back(i, arriving=False):
        at = lax.rem(z + DEPTH - OFFSETS[i], DEPTH) if arriving else z
        other = chunk_of(i)
        return remote(ret_out.at[other], ret_in.at[at], sems(8, i), {"sp_0": other})

    def first_send_hop(i):
        _, to = sides(i)
        return remote(first_part.at[i, across], first_hop.at[i], sems(15, i), {"tp": to})

    def first_send_both(i):
        _, to = sides(i)
        return remote(first_hopped.at[i], first_both.at[i], sems(16, i), {"tp": to})

    def first_send_plain(i):
        to, _ = sides(i)
        return remote(first_part.at[i, to], first_plain.at[i], sems(17, i), {"tp": to})

    def stage_0(i):
        at = chunk_of(i)
        if i != OWN:
            remote(out_depth.at[at], inbound.at[t, at], sems(1, i), {"sp_0": at}).wait_recv()
        partial = dot(inbound[t, at], down_in[...].reshape(RING * hidden, quarter), NT)
        for n in range(RING):
            first_part[i, n] = partial[:, n * hidden : (n + 1) * hidden].astype(BF16)
        first_send_hop(i).start()
        first_send_plain(i).start()

    def stage_1(i):
        _, to = sides(i)
        first_send_hop(i).wait_recv()
        total = first_hop[i].astype(F32) + first_part[i, to].astype(F32)
        first_hopped[i] = total.astype(BF16)
        first_send_both(i).start()

    def stage_2(i):
        at = chunk_of(i)
        first_send_both(i).wait_recv()
        first_send_plain(i).wait_recv()
        total = first_part[i, t].astype(F32) + first_both[i].astype(F32)
        total = total + first_plain[i].astype(F32)
        up_delta = (total * silu[at]).astype(BF16)
        gate_delta = (total * slope[at]).astype(BF16)
        deltas = jnp.concatenate([gate_delta, up_delta], axis=1)
        delta[at] = deltas
        _, to = sides(i)
        for n, which in enumerate((across, sides(i)[0], to, t)):
            rows = pl.ds(pl.multiple_of(which * quarter, quarter), quarter)
            part[i, which] = dot(deltas, w_cat[rows, :], NT).astype(BF16)
            if n == 0:
                send_hop(i).start()
            if n == 1:
                send_plain(i).start()

    def stage_3(i):
        _, to = sides(i)
        send_hop(i).wait_recv()
        hopped[i] = (hop[i].astype(F32) + part[i, to].astype(F32)).astype(BF16)
        send_both(i).start()

    def stage_4(i):
        at = chunk_of(i)
        send_both(i).wait_recv()
        send_plain(i).wait_recv()
        total = part[i, t].astype(F32) + both[i].astype(F32) + plain[i].astype(F32)
        if i == OWN:
            ret_in[z] = total.astype(BF16)
        else:
            ret_out[at] = total.astype(BF16)
            send_back(i).start()

    for d in PLANE_ORDER:
        plane_in(0, out_plane, in_plane, d).wait_recv()
    moved = dot(swap[...], in_plane[...].reshape(DEPTH * CHUNK, quarter)).astype(BF16)
    out_depth[...] = moved.reshape(out_depth.shape)

    def depth_out(i):
        other = lax.rem(z + DEPTH - OFFSETS[i], DEPTH)
        return remote(out_depth.at[other], inbound.at[t, z], sems(1, i), {"sp_0": other})

    inbound[t, z] = out_depth[z]
    for i in AWAY:
        depth_out(i).start()

    for copy in loads[1:4]:
        copy.wait()
    half = x.shape[0] // 2
    for j in range(2):
        rows = pl.ds(j * half, half)
        chunks = pl.ds(j * (DEPTH // 2), DEPTH // 2)
        both_up = jnp.dot(x[rows, :], w_cat[...], preferred_element_type=F32)
        gate, up = both_up[:, :hidden], both_up[:, hidden:]
        sigma = jax.nn.sigmoid(gate)
        s = gate * sigma
        shape = (DEPTH // 2, CHUNK, hidden)
        silu[chunks] = s.reshape(shape)
        act[chunks] = (s * up).astype(BF16).reshape(shape)
        slope[chunks] = (up * sigma * (1.0 + gate * (1.0 - sigma))).reshape(shape)
    loads[4].wait()
    for n in range(1, RING):
        down_copy(n, True).wait_recv()

    def attend(step):
        if step == 0:
            carry.middle()
        elif step == 1:
            inclusive, strict = masks()
            for piece in pieces:
                piece.a = piece.scores(inclusive, strict)
                piece.inner = dot(piece.a, piece.vs)
                piece.entries()
        else:
            carry.last()

    stages = (stage_0, stage_1, stage_2, stage_3, stage_4)
    for stage, i in SCHEDULE:
        if i == DEPTH:
            attend(stage)
        else:
            stages[stage](i)

    for i in range(DEPTH):
        for copy in spread(i):
            copy.start()

    forward_entry, backward_entry = carry.finish()
    before, after, _, _ = both_states(pieces, forward_entry, backward_entry)
    for b, piece in enumerate(pieces):
        piece.states = jnp.concatenate([before[b], after[b]], axis=1).astype(BF16)
        o = piece.inner + dot(jnp.concatenate([piece.qg, piece.qh], axis=1), piece.states, NT)
        piece.inv = lax.rsqrt(jnp.mean(o * o, axis=1, keepdims=True) + EPSILON)
        piece.mixed = o * piece.inv

    for i in AWAY:
        send_back(i, True).wait_recv()
    moved = dot(swap[...], ret_in[...].reshape(DEPTH * CHUNK, quarter)).astype(BF16)
    back_out[...] = moved.reshape(back_out.shape)
    for d in PLANE_ORDER:
        plane_out(9, back_out, back_in, d).start()
    back_in[p] = back_out[p]
    deltas = delta[...].reshape(DEPTH * CHUNK, 2 * hidden)
    for n in range(RING):
        both_grads = dot(x[:, n * quarter : (n + 1) * quarter], deltas, TN)
        rows = pl.ds(n * quarter, quarter)
        gate_grad_ref[rows, :] = both_grads[:, :hidden].astype(BF16)
        up_grad_ref[rows, :] = both_grads[:, hidden:].astype(BF16)
    for d in PLANE_ORDER:
        plane_in(9, back_out, back_in, d).wait_recv()
    moe_grad = dot(choice_t[...], back_in[...].reshape(DEPTH * CHUNK, quarter))
    stream[t] = (own[...].astype(F32) + moe_grad).astype(BF16)

    low, high = pl.ds(0, tokens // 2), pl.ds(tokens // 2, tokens // 2)

    def ring(kind, which, rows, to):
        pair = sems(kind, 0 if kind in (0, 9) else OWN)
        return remote(stream.at[which, rows], stream.at[which, rows], pair, {"tp": to})

    def stream_spread():
        return (
            ring(0, t, low, right),
            ring(1, t, high, left),
            ring(8, t, high, right),
            ring(9, t, low, left),
        )

    def stream_arrived():
        return (
            ring(0, left, low, right),
            ring(1, right, high, left),
            ring(8, left, high, right),
            ring(9, right, low, left),
        )

    def stream_pass(which_low, which_high):
        return (
            remote(
                stream.at[which_low, low], stream.at[which_low, low], sems(10, 0), {"tp": right}
            ),
            remote(
                stream.at[which_high, high], stream.at[which_high, high], sems(11, 0), {"tp": left}
            ),
        )

    rows_of_mixed = jnp.concatenate([heads_on_lanes(piece.mixed) for piece in pieces], axis=0)
    rows_of_mixed = rows_of_mixed.astype(BF16)
    piece_rows = proj_ref.shape[0]
    per = quarter // (piece_rows * PLANES)
    turns = (t, left, right, across)

    def span(n):
        return pl.ds(turns[n] * per, per)

    def make_terms(n):
        term = dot(stream[turns[n]], rows_of_mixed, TN).astype(BF16)
        term = term.reshape(per, 4, 2, piece_rows, term.shape[1])
        for cc in range(2):
            for zz in range(per):
                terms[cc, :, turns[n] * per + zz] = term[zz, :, cc]
        core_copy(n).start()

    def core_copy(n):
        src, dst = terms.at[1 - c, :, span(n)], core_in.at[:, span(n)]
        return remote(src, dst, sems(12, n), {"sp_2": 1 - c})

    def row_copy(n, d, arriving=False):
        other = lax.rem(y + (4 - d if arriving else d), 4)
        at = other if arriving else y
        src, dst = core_sum.at[other, span(n)], row_in.at[at, span(n)]
        return remote(src, dst, sems(18 + n, d), {"sp_1": other})

    def send_terms(n):
        core_copy(n).wait_recv()
        mine = terms[c, :, span(n)].astype(F32)
        core_sum[:, span(n)] = (mine + core_in[:, span(n)].astype(F32)).astype(BF16)
        for d in (2, 1, 3):
            row_copy(n, d).start()

    for copy in stream_spread():
        copy.start()
    make_terms(0)
    loads[5].wait()

    def share(which):
        rows = pl.ds(pl.multiple_of(which * quarter, quarter), quarter)
        return jnp.dot(stream[which], w_out[rows, :], preferred_element_type=F32)

    mixed_grad = share(t)
    onward = stream_pass(left, right)
    for n, copy in enumerate(stream_arrived()):
        copy.wait_recv()
        if n < 2:
            onward[n].start()
    make_terms(1)
    make_terms(2)
    mixed_grad = mixed_grad + share(left) + share(right)
    send_terms(0)
    for copy in stream_pass(across, across):
        copy.wait_recv()
    mixed_grad = mixed_grad + share(across)

    back_c, back_d = jnp.zeros((DV, 128), F32), jnp.zeros((DV, 128), F32)
    for b, piece in enumerate(pieces):
        mg = heads_on_rows(mixed_grad[b * BLOCK : (b + 1) * BLOCK, :])
        mean = jnp.mean(mg * piece.mixed, axis=1, keepdims=True)
        piece.do = (piece.inv * (mg - piece.mixed * mean)).astype(BF16)
        piece.back_f = dot(piece.do, piece.qg, TN)
        piece.back_b = dot(piece.do, piece.qh, TN)
    for piece in pieces:
        back_c = back_c * jnp.exp(piece.first) + piece.back_b
    for piece in reversed(pieces):
        back_d = back_d * jnp.exp(piece.last) + piece.back_f
    carry = Carry(carry_refs[12:])
    carry.start((back_c, back_d), (log_b, log_f))
    make_terms(3)
    send_terms(1)
    send_terms(2)

    def last_copy(d, arriving=False):
        other = lax.rem(z + (DEPTH - d if arriving else d), DEPTH)
        at = other if arriving else z
        return remote(row_sum.at[other], depth_in.at[at], sems(13, d), {"sp_0": other})

    inclusive, strict = masks()
    for piece in pieces:
        da = dot(piece.do, piece.vs, NT)
        da_f = jnp.where(inclusive, da, 0.0).astype(BF16)
        da_b = jnp.where(strict, da, 0.0).astype(BF16)
        piece.dv = dot(piece.a, piece.do, TN)
        piece.dq = dot(da_f, piece.k_dn_g) * doubled(piece.up_g) + dot(
            da_b, piece.k_dn_h
        ) * doubled(piece.up_h)
        piece.dk = dot(da_f, piece.q_up_g, TN) * doubled(piece.dn_g) + dot(
            da_b, piece.q_up_h, TN
        ) * doubled(piece.dn_h)
    send_terms(3)
    for i in range(DEPTH):
        for copy in spread(i, True):
            copy.wait_recv()
        pass_on(i).start()

    carry.middle()
    for b, piece in enumerate(pieces):
        dq = dot(piece.do, piece.states)
        dq = piece.dq + dq[:, :128] * stacked(piece.eg) + dq[:, 128:] * stacked(piece.eh)
        dq_ref[pl.ds(b * BLOCK, BLOCK), :] = (folded(dq) * KEY_CHANNELS**-0.5).astype(BF16)
    for n in range(4):
        for d in (1, 3, 2):
            row_copy(n, d, True).wait_recv()
    row_in[y] = core_sum[y]
    total = row_in[0].astype(F32)
    for n in range(1, 4):
        total = total + row_in[n].astype(F32)
    row_sum[...] = total.astype(BF16)
    for d in DEPTH_ORDER:
        last_copy(d).start()
    carry.last()
    for i in range(DEPTH):
        pass_on(i, True).wait_recv()
    act_all = act[...].reshape(DEPTH * CHUNK, hidden)
    for n in range(RING):
        rows = inbound[n].reshape(DEPTH * CHUNK, quarter)
        down_grad_ref[:, n * quarter : (n + 1) * quarter] = dot(act_all, rows, TN).astype(BF16)
    back_c, back_d = carry.finish()
    late, early = [None] * 3, [None] * 3
    for b, piece in enumerate(pieces):
        early[b] = back_c
        back_c = back_c * jnp.exp(piece.first) + piece.back_b
    for b in reversed(range(3)):
        late[b] = back_d
        back_d = back_d * jnp.exp(pieces[b].last) + pieces[b].back_f
    for b, piece in enumerate(pieces):
        states = jnp.concatenate([late[b], early[b]], axis=1).astype(BF16)
        dk = dot(piece.vs, states)
        dk = piece.dk + dk[:, :128] * stacked(piece.eg_end) + dk[:, 128:] * stacked(piece.eh_end)
        dv = piece.dv + dot(jnp.concatenate([piece.kg_end, piece.kh_end], axis=1), states, NT)
        rows = pl.ds(b * BLOCK, BLOCK)
        dk_ref[rows, :] = folded(dk).astype(BF16)
        dv_ref[rows, :] = heads_on_lanes(dv).astype(BF16)
    depth_in[z] = row_sum[z]
    for d in range(1, DEPTH):
        last_copy(d, True).wait_recv()
    total = depth_in[0].astype(F32)
    for n in range(1, DEPTH):
        total = total + depth_in[n].astype(F32)
    proj_ref[...] = total

    for d in PLANE_ORDER:
        plane_out(0, out_plane, in_plane, d).wait_send()
        plane_out(9, back_out, back_in, d).wait_send()
    for i in range(DEPTH):
        if i != OWN:
            depth_out(i).wait_send()
            send_back(i).wait_send()
        for copy in (*spread(i), pass_on(i), send_hop(i), send_both(i), send_plain(i)):
            copy.wait_send()
        for copy in (first_send_hop(i), first_send_both(i), first_send_plain(i)):
            copy.wait_send()
    for n in range(1, RING):
        down_copy(n).wait_send()
    for copy in (*stream_spread(), *stream_pass(left, right)):
        copy.wait_send()
    for n in range(4):
        core_copy(n).wait_send()
        for d in (1, 2, 3):
            row_copy(n, d).wait_send()
    for d in range(1, DEPTH):
        last_copy(d).wait_send()


def vmem(n):
    return [pl.BlockSpec(memory_space=pltpu.VMEM)] * n


def layer(*arrays):
    layer_grad, slot_tokens, gate = arrays[2], arrays[3], arrays[4]
    tokens, width = layer_grad.shape
    slots = slot_tokens.shape[1]
    quarter = width // RING
    hidden = gate.shape[2]
    out_columns = arrays[7].shape[1]
    piece_rows = width // (DEPTH * PLANES)
    rows = (DEPTH, CHUNK, quarter)
    anywhere = pl.BlockSpec(memory_space=pl.ANY)
    return pl.pallas_call(
        layer_kernel,
        out_shape=(
            pltpu.VMEM((width, hidden), BF16),
            pltpu.VMEM((width, hidden), BF16),
            pltpu.VMEM((hidden, width), BF16),
            pltpu.VMEM((piece_rows, out_columns), F32),
            pltpu.VMEM((tokens, 128), BF16),
            pltpu.VMEM((tokens, 128), BF16),
            pltpu.VMEM((tokens, 2 * DV), BF16),
        ),
        in_specs=vmem(2) + [anywhere] * 11,
        out_specs=tuple(vmem(7)),
        scratch_shapes=[
            *[pltpu.VMEM(a.shape, a.dtype) for a in arrays[8:]],
            pltpu.VMEM((tokens, quarter), BF16),
            pltpu.VMEM((slots, width), BF16),
            pltpu.VMEM((width, 2 * hidden), BF16),
            pltpu.VMEM((RING, hidden, quarter), BF16),
            pltpu.VMEM((RING, hidden, quarter), BF16),
            pltpu.VMEM((width, out_columns), BF16),
            pltpu.VMEM((slots, tokens), BF16),
            pltpu.VMEM((tokens, slots), BF16),
            pltpu.VMEM((slots, slots), BF16),
            pltpu.VMEM((DEPTH, CHUNK, hidden), BF16),
            pltpu.VMEM((DEPTH, CHUNK, hidden), F32),
            pltpu.VMEM((DEPTH, CHUNK, hidden), F32),
            pltpu.VMEM((DEPTH, CHUNK, 2 * hidden), BF16),
            pltpu.VMEM(rows, BF16),
            pltpu.VMEM(rows, BF16),
            pltpu.VMEM(rows, BF16),
            pltpu.VMEM((RING, *rows), BF16),
            pltpu.VMEM((DEPTH, RING, CHUNK, hidden), BF16),
            *[pltpu.VMEM((DEPTH, CHUNK, hidden), BF16)] * 4,
            pltpu.VMEM((DEPTH, RING, CHUNK, quarter), BF16),
            *[pltpu.VMEM(rows, BF16)] * 8,
            pltpu.VMEM((RING, tokens, quarter), BF16),
            pltpu.VMEM((2, 4, DEPTH, piece_rows, out_columns), BF16),
            pltpu.VMEM((4, DEPTH, piece_rows, out_columns), BF16),
            pltpu.VMEM((4, DEPTH, piece_rows, out_columns), BF16),
            pltpu.VMEM((4, DEPTH, piece_rows, out_columns), BF16),
            pltpu.VMEM((DEPTH, piece_rows, out_columns), BF16),
            pltpu.VMEM((DEPTH, piece_rows, out_columns), BF16),
            pltpu.SemaphoreType.DMA((22, DEPTH)),
            pltpu.SemaphoreType.DMA((22, DEPTH)),
            pltpu.SemaphoreType.DMA((14,)),
            *Carry.scratch(),
            *Carry.scratch(),
        ],
        compiler_params=pltpu.CompilerParams(
            collective_id=0, has_side_effects=True, vmem_limit_bytes=56 * 2**20
        ),
        cost_estimate=pl.CostEstimate(
            flops=8 * 10**9, bytes_accessed=12 * 2**20, transcendentals=0
        ),
        name="layer",
    )(*arrays)


def write_kernel(*refs):
    n = len(refs) // 2
    done = refs[-1]
    copies = [pltpu.make_async_copy(refs[i], refs[n + i], done.at[i]) for i in range(n)]
    for copy in copies:
        copy.start()
    for copy in copies:
        copy.wait()


def written(arrays):
    n = len(arrays)
    arrays = [pltpu.with_memory_space_constraint(a, pltpu.VMEM) for a in arrays]
    return pl.pallas_call(
        write_kernel,
        out_shape=tuple(jax.ShapeDtypeStruct(a.shape, a.dtype) for a in arrays),
        in_specs=vmem(n),
        out_specs=(pl.BlockSpec(memory_space=pl.ANY),) * n,
        scratch_shapes=[pltpu.SemaphoreType.DMA((n,))],
        compiler_params=pltpu.CompilerParams(vmem_limit_bytes=2**20),
        name="write",
    )(*arrays)


def on_device(layer_grad, routes, route_weight, *arrays):
    results = written(layer(routes.T, route_weight.T, layer_grad, *arrays))
    gate, up, down, proj, query, key, value = results
    return gate[None], up[None], down[None], proj, query, key, value


def solution(mesh):
    torus = Mesh(mesh.devices.reshape(8, 4, 2, mesh.shape["tp"]), ("sp_0", "sp_1", "sp_2", "tp"))
    in_specs = (
        P(SP, None),
        P(SP, None),
        P(SP, None),
        P(SP, None, None),
        P(SP, None, "tp"),
        P(SP, None, "tp"),
        P(SP, "tp", None),
        P(None, "tp"),
        P(SP, "tp"),
        P(SP, "tp"),
        P(SP, "tp"),
        P(SP, "tp"),
        P(SP, "tp"),
    )
    out_specs = (
        P(SP, None, "tp"),
        P(SP, None, "tp"),
        P(SP, "tp", None),
        P(SP, "tp"),
        P(SP, "tp"),
        P(SP, "tp"),
        P(SP, "tp"),
    )
    return jax.shard_map(
        on_device, mesh=torus, in_specs=in_specs, out_specs=out_specs, check_vma=False
    )
```
